32 devices in a mesh: sp: 16 (over z, y, x), tp: 2 (over core).
Axes of the slice: x: 2, y: 2, z: 4, core: 2. Of those that a mesh axis runs over, the one named last changes fastest.
Arguments:
- tokens: bfloat16 [8192, 2048], P('sp', 'tp'), may hold values from -6 to 6
- norm_gain: float32 [2048], replicated, may hold values from 0.1 to 1.9
- outer_gate: bfloat16 [2048, 1024], P('sp', 'tp'), may hold values from -0.125 to 0.125
- inner_gate: bfloat16 [2048, 1024], P('sp', 'tp'), may hold values from -0.125 to 0.125
- conv_input: bfloat16 [2048, 1024], P('sp', 'tp'), may hold values from -0.125 to 0.125
- query_proj: bfloat16 [2048, 1024], P('sp', 'tp'), may hold values from -0.125 to 0.125
- key_proj: bfloat16 [2048, 1024], P('sp', 'tp'), may hold values from -0.125 to 0.125
- value_proj: bfloat16 [2048, 1024], P('sp', 'tp'), may hold values from -0.125 to 0.125
- out_gate: bfloat16 [2048, 1024], P('sp', 'tp'), may hold values from -0.125 to 0.125
- conv_taps: float32 [3, 1024], P(None, 'tp'), may hold values from -3.5 to 3.5
- log_decay: float32 [2, 16, 8192], P(None, 'tp', 'sp'), may hold values from -1.2 to 0, as said below
- head_gain: float32 [1024], P('tp'), may hold values from 0.1 to 1.9
- conv_output: bfloat16 [1024, 2048], P('tp', 'sp'), may hold values from -0.1875 to 0.1875
- retention_output: bfloat16 [1024, 2048], P('tp', 'sp'), may hold values from -0.1875 to 0.1875
Outputs:
- mixed: bfloat16 [8192, 2048], P(('sp', 'tp'))
The draws below stay inside these ranges and needn't reach their ends.
Inputs may be any that keep to these rules, and one draw needn't show every extreme that they name: `log_decay`: logarithms of per-position decays, below zero.
All inputs are finite; a program needn't handle non-finite values.
Results may differ from the reference program's by a relative error of at most 0.02.
Values may be sent and summed in bfloat16 or wider, within the bound.
A program may use at most 128 MiB of HBM per device.

```python
import math
import jax
import jax.numpy as jnp
from jax import lax

D = 2048
CONV_CH = 1024
HEAD_NUMBER = 16
HEAD_DIM = 64
TOK_DEV = 512
TOKEN_NUMBER = 8192
N_SP = 16
N_TP = 2


def draw_log_decay(key, part):
    key_sequence = jax.random.split(jax.random.fold_in(key, 17), 6)
    span_count = TOKEN_NUMBER // TOK_DEV
    is_fast = jax.random.uniform(key_sequence[0], (2, HEAD_NUMBER, 1), jnp.float32) < 0.5
    fast_rate = jax.random.uniform(key_sequence[1], (2, HEAD_NUMBER, 1), jnp.float32, 0.01, 0.02)
    slow_rate = jax.random.uniform(key_sequence[2], (2, HEAD_NUMBER, 1), jnp.float32, 0.1, 0.3) / TOKEN_NUMBER
    selected_rate = jnp.where(is_fast, fast_rate, slow_rate)
    multiplier = jnp.exp(jax.random.uniform(key_sequence[3], (2, HEAD_NUMBER, span_count), jnp.float32, 0.0, math.log(4.0)))
    multiplier = jnp.repeat(multiplier, TOK_DEV, axis=2)
    flurry_location = jax.random.randint(key_sequence[4], (2, HEAD_NUMBER, 2, 1), 0, TOKEN_NUMBER)
    flurry_depth = jax.random.uniform(key_sequence[5], (2, HEAD_NUMBER, 2, 1), jnp.float32, 0.22, 0.51)
    position_list = jnp.arange(TOKEN_NUMBER, dtype=jnp.int32)
    flurry_list = jnp.sum(jnp.where(position_list == flurry_location, flurry_depth, 0.0), axis=2)
    return (-(selected_rate * multiplier) - flurry_list).astype(jnp.float32)


def shard_levels(stream_key, dims, pieces, least, largest):
    gain, own = 1.0, jax.random.fold_in(stream_key, 6)
    for axis_at, blocks in pieces:
        steps = jnp.exp(jax.random.uniform(jax.random.fold_in(own, axis_at), (blocks,), jnp.float32, least / len(pieces), largest / len(pieces)))
        gain = gain * jnp.repeat(steps, dims[axis_at] // blocks).reshape([-1 if axis == axis_at else 1 for axis in range(len(dims))])
    return gain


def centred(stream_key, dims, width, reach, cuts=(), held_as=jnp.bfloat16):
    gain = shard_levels(stream_key, dims, cuts, -0.22, 0.18) if cuts else 1.0
    entries = jax.random.normal(stream_key, dims, jnp.float32) * width * gain
    return jnp.minimum(jnp.maximum(entries, -reach), reach).astype(held_as)


def setup_inputs(seed: int = 0) -> dict:
    seeds = jax.random.split(jax.random.key(seed), 15)
    tokens = centred(seeds[0], (TOKEN_NUMBER, D), 1.0, 6.0, ((0, 16), (1, 2)))
    norm_gain = jnp.clip(1.0 + 0.18 * jax.random.normal(seeds[1], (D,), jnp.float32), 0.1, 1.9)
    outer_gate = centred(seeds[2], (D, CONV_CH), D ** -0.5, 0.125, ((0, 16), (1, 2)))
    inner_gate = centred(seeds[3], (D, CONV_CH), D ** -0.5, 0.125, ((0, 16), (1, 2)))
    conv_input = centred(seeds[4], (D, CONV_CH), D ** -0.5, 0.125, ((0, 16), (1, 2)))
    query_proj = centred(seeds[5], (D, HEAD_NUMBER * HEAD_DIM), D ** -0.5, 0.125, ((0, 16), (1, 2)))
    key_proj = centred(seeds[6], (D, HEAD_NUMBER * HEAD_DIM), D ** -0.5, 0.125, ((0, 16), (1, 2)))
    value_proj = centred(seeds[7], (D, HEAD_NUMBER * HEAD_DIM), D ** -0.5, 0.125, ((0, 16), (1, 2)))
    out_gate = centred(seeds[8], (D, HEAD_NUMBER * HEAD_DIM), D ** -0.5, 0.125, ((0, 16), (1, 2)))
    conv_taps = centred(seeds[9], (3, CONV_CH), 3 ** -0.5, 3.5, ((1, 2),), jnp.float32)
    log_decay = draw_log_decay(jax.random.fold_in(seeds[14], 71), 0)
    head_gain = jnp.clip(1.0 + 0.18 * jax.random.normal(seeds[11], (HEAD_NUMBER * HEAD_DIM,), jnp.float32), 0.1, 1.9)
    conv_output = centred(seeds[12], (CONV_CH, D), CONV_CH ** -0.5, 0.1875, ((0, 2), (1, 16)))
    retention_output = centred(seeds[13], (HEAD_NUMBER * HEAD_DIM, D), (HEAD_NUMBER * HEAD_DIM) ** -0.5, 0.1875, ((0, 2), (1, 16)))
    return {"tokens": tokens, "norm_gain": norm_gain, "outer_gate": outer_gate, "inner_gate": inner_gate, "conv_input": conv_input, "query_proj": query_proj, "key_proj": key_proj, "value_proj": value_proj, "out_gate": out_gate, "conv_taps": conv_taps, "log_decay": log_decay, "head_gain": head_gain, "conv_output": conv_output, "retention_output": retention_output}


EPS = 1e-06
THETA = 10000.0

def rounded(array):
    return lax.optimization_barrier(array.astype(jnp.bfloat16)).astype(jnp.float32)

def rotate(field_in, position_list):
    half_dim = field_in.shape[-1] // 2
    frequency = jnp.exp(-jnp.log(THETA) * jnp.arange(half_dim, dtype=jnp.float32) * (2.0 / field_in.shape[-1]))
    angles = position_list.astype(jnp.float32)[:, None, None] * frequency
    cosine = jnp.cos(angles)
    sine_part = jnp.sin(angles)
    leading = field_in[..., :half_dim]
    trailing = field_in[..., half_dim:]
    return jnp.concatenate([leading * cosine - trailing * sine_part, leading * sine_part + trailing * cosine], axis=-1)

def span_parts(query_rows, key_rows, value_rows, log_rates):
    length = query_rows.shape[0]
    forward_cum = jnp.cumsum(log_rates[0], axis=-1)
    backward_cum = jnp.flip(jnp.cumsum(jnp.flip(log_rates[1], -1), axis=-1), -1)
    row_index = lax.broadcasted_iota(jnp.int32, (length, length), 0)
    col_index = lax.broadcasted_iota(jnp.int32, (length, length), 1)
    lower_part = (col_index <= row_index)[None]
    spread = jnp.where(lower_part, forward_cum[:, :, None] - forward_cum[:, None, :], backward_cum[:, :, None] - backward_cum[:, None, :])
    scores = jnp.einsum('ihe,jhe->hij', query_rows.astype(jnp.float32), key_rows.astype(jnp.float32))
    weighted = rounded(scores * jnp.exp(spread))
    local_part = jnp.einsum('hij,jhe->ihe', weighted, value_rows.astype(jnp.float32))
    key_wide = key_rows.astype(jnp.float32)
    forward_keys = rounded(key_wide * jnp.exp(forward_cum[:, -1:] - forward_cum).T[:, :, None])
    backward_keys = rounded(key_wide * jnp.exp(backward_cum[:, :1] - backward_cum).T[:, :, None])
    forward_state = jnp.einsum('jhd,jhe->hde', forward_keys, value_rows.astype(jnp.float32))
    backward_state = jnp.einsum('jhd,jhe->hde', backward_keys, value_rows.astype(jnp.float32))
    return (local_part, forward_cum, backward_cum, forward_state, backward_state)

def span_item(inputs):
    return span_parts(inputs[0], inputs[1], inputs[2], inputs[3])

def carried(query_rows, forward_cum, backward_cum, into_forward, into_backward):
    query_wide = query_rows.astype(jnp.float32)
    forward_part = jnp.einsum('ihd,hde->ihe', query_wide, rounded(into_forward))
    backward_part = jnp.einsum('ihd,hde->ihe', query_wide, rounded(into_backward))
    return jnp.exp(forward_cum).T[:, :, None] * forward_part + jnp.exp(backward_cum).T[:, :, None] * backward_part

def finish(mixed_heads, gate_rows, head_gain):
    row_count, head_count, head_width = mixed_heads.shape
    scaled = mixed_heads * lax.rsqrt(lax.optimization_barrier(jnp.mean(mixed_heads * mixed_heads, axis=-1, keepdims=True)) + EPS)
    scaled = scaled * head_gain.reshape(head_count, head_width)
    return (jax.nn.silu(gate_rows.astype(jnp.float32)) * scaled.reshape(row_count, head_count * head_width)).astype(jnp.bfloat16)

def forward_step(running, inputs):
    return (jnp.exp(inputs[0])[:, None, None] * running + inputs[1], running)

def reference(tokens, norm_gain, outer_gate, inner_gate, conv_input, query_proj, key_proj, value_proj, out_gate, conv_taps, log_decay, head_gain, conv_output, retention_output):
    wide = tokens.astype(jnp.float32)
    normed = (wide * lax.rsqrt(lax.optimization_barrier(jnp.mean(wide * wide, axis=-1, keepdims=True)) + EPS) * norm_gain).astype(jnp.bfloat16)
    projected = [jnp.dot(normed, weight, preferred_element_type=jnp.float32).astype(jnp.bfloat16) for weight in (outer_gate, inner_gate, conv_input, query_proj, key_proj, value_proj, out_gate)]
    inner_value = (projected[1].astype(jnp.float32) * projected[2].astype(jnp.float32)).astype(jnp.bfloat16)
    padded = jnp.pad(inner_value.astype(jnp.float32), ((1, 1), (0, 0)))
    convolved = conv_taps[0] * padded[:-2] + conv_taps[1] * padded[1:-1] + conv_taps[2] * padded[2:]
    conv_out = (projected[0].astype(jnp.float32) * convolved).astype(jnp.bfloat16)
    position_list = jnp.arange(TOKEN_NUMBER, dtype=jnp.int32)
    shape_heads = (TOKEN_NUMBER, HEAD_NUMBER, HEAD_DIM)
    rotated_query = rotate(projected[3].astype(jnp.float32).reshape(shape_heads), position_list).astype(jnp.bfloat16)
    rotated_key = (rotate(projected[4].astype(jnp.float32).reshape(shape_heads), position_list) * HEAD_DIM ** (-0.5)).astype(jnp.bfloat16)
    value_heads = projected[5].reshape(shape_heads)
    span_shape = (N_SP, TOK_DEV, HEAD_NUMBER, HEAD_DIM)
    span_rates = log_decay.reshape(2, HEAD_NUMBER, N_SP, TOK_DEV).transpose(2, 0, 1, 3)
    span_query = rotated_query.reshape(span_shape)
    local_part, forward_cum, backward_cum, forward_state, backward_state = lax.map(span_item, (span_query, rotated_key.reshape(span_shape), value_heads.reshape(span_shape), span_rates))
    blank = jnp.zeros((HEAD_NUMBER, HEAD_DIM, HEAD_DIM), jnp.float32)
    into_forward = lax.scan(forward_step, blank, (forward_cum[:, :, -1], forward_state))[1]
    into_backward = lax.scan(forward_step, blank, (backward_cum[:, :, 0], backward_state), reverse=True)[1]
    carried_part = jax.vmap(carried)(span_query, forward_cum, backward_cum, into_forward, into_backward)
    mixed_heads = (local_part + carried_part).reshape(shape_heads)
    ret_out = finish(mixed_heads, projected[6], head_gain)
    conv_group = CONV_CH // N_TP
    ret_group = HEAD_NUMBER * HEAD_DIM // N_TP
    total_sum = jnp.zeros((TOKEN_NUMBER, D), jnp.float32)
    for group_index in range(N_TP):
        conv_lo = group_index * conv_group
        ret_lo = group_index * ret_group
        partial_sum = jnp.dot(conv_out[:, conv_lo:conv_lo + conv_group], conv_output[conv_lo:conv_lo + conv_group], preferred_element_type=jnp.float32)
        partial_sum = partial_sum + jnp.dot(ret_out[:, ret_lo:ret_lo + ret_group], retention_output[ret_lo:ret_lo + ret_group], preferred_element_type=jnp.float32)
        total_sum = total_sum + rounded(partial_sum)
    return total_sum.astype(jnp.bfloat16)
```

```python
import jax
import functools
import jax.numpy as jnp
import numpy as np
from jax import lax
from jax.experimental import pallas as pl
from jax.experimental.pallas import tpu as pltpu
from jax.sharding import PartitionSpec as P

HEAD_DIM = 64


EPS = 1e-06
THETA = 10000.0


def with_halo(shard, sides, width):
    for axis, dim in sides:
        size, length = (lax.axis_size(axis), shard.shape[dim])
        up = [(i, (i + 1) % size) for i in range(size - 1)]
        down = [(j, i) for i, j in up]
        last = lax.slice_in_dim(shard, length - width, length, axis=dim)
        first = lax.slice_in_dim(shard, 0, width, axis=dim)
        before = lax.ppermute(last, axis, up)
        after = lax.ppermute(first, axis, down)
        shard = jnp.concatenate([before, shard, after], axis=dim)
    return shard


def rotate(field_in, position_list):
    half_dim = field_in.shape[-1] // 2
    frequency = jnp.exp(
        -jnp.log(THETA) * jnp.arange(half_dim, dtype=jnp.float32) * (2.0 / field_in.shape[-1])
    )
    angles = position_list.astype(jnp.float32)[:, None, None] * frequency
    cosine = jnp.cos(angles)
    sine_part = jnp.sin(angles)
    leading = field_in[..., :half_dim]
    trailing = field_in[..., half_dim:]
    return jnp.concatenate(
        [leading * cosine - trailing * sine_part, leading * sine_part + trailing * cosine], axis=-1
    )


def conv_branch(outer_rows, inner_rows, conv_values, conv_taps):
    inner_value = (inner_rows.astype(jnp.float32) * conv_values.astype(jnp.float32)).astype(
        jnp.bfloat16
    )
    padded = with_halo(inner_value, (("sp", 0),), 1).astype(jnp.float32)
    convolved = conv_taps[0] * padded[:-2] + conv_taps[1] * padded[1:-1] + conv_taps[2] * padded[2:]
    return (outer_rows.astype(jnp.float32) * convolved).astype(jnp.bfloat16)


def span_parts(query_rows, key_rows, value_rows, log_rates):
    length = query_rows.shape[0]
    forward_cum = jnp.cumsum(log_rates[0], axis=-1)
    backward_cum = jnp.flip(jnp.cumsum(jnp.flip(log_rates[1], -1), axis=-1), -1)
    row_index = lax.broadcasted_iota(jnp.int32, (length, length), 0)
    col_index = lax.broadcasted_iota(jnp.int32, (length, length), 1)
    lower_part = (col_index <= row_index)[None]
    spread = jnp.where(
        lower_part,
        forward_cum[:, :, None] - forward_cum[:, None, :],
        backward_cum[:, :, None] - backward_cum[:, None, :],
    )
    scores = jnp.einsum("ihe,jhe->hij", query_rows, key_rows, preferred_element_type=jnp.float32)
    weighted = (scores * jnp.exp(spread)).astype(jnp.bfloat16)
    local_part = jnp.einsum(
        "hij,jhe->ihe", weighted, value_rows, preferred_element_type=jnp.float32
    )
    key_wide = key_rows.astype(jnp.float32)
    forward_keys = (key_wide * jnp.exp(forward_cum[:, -1:] - forward_cum).T[:, :, None]).astype(
        jnp.bfloat16
    )
    backward_keys = (key_wide * jnp.exp(backward_cum[:, :1] - backward_cum).T[:, :, None]).astype(
        jnp.bfloat16
    )
    forward_state = jnp.einsum(
        "jhd,jhe->hde", forward_keys, value_rows, preferred_element_type=jnp.float32
    )
    backward_state = jnp.einsum(
        "jhd,jhe->hde", backward_keys, value_rows, preferred_element_type=jnp.float32
    )
    return (local_part, forward_cum, backward_cum, forward_state, backward_state)


def retention_branch(query_rows, key_rows, value_rows, gate_rows, log_decay, head_gain, offsets):
    row_count = query_rows.shape[0]
    head_count = query_rows.shape[1] // HEAD_DIM
    shape_heads = (row_count, head_count, HEAD_DIM)
    rotated_query = rotate(query_rows.astype(jnp.float32).reshape(shape_heads), offsets).astype(
        jnp.bfloat16
    )
    rotated_key = (
        rotate(key_rows.astype(jnp.float32).reshape(shape_heads), offsets) * HEAD_DIM ** (-0.5)
    ).astype(jnp.bfloat16)
    local_part, forward_cum, backward_cum, forward_state, backward_state = span_parts(
        rotated_query, rotated_key, value_rows.reshape(shape_heads), log_decay
    )
    forward_total = forward_cum[:, -1]
    backward_total = backward_cum[:, 0]
    totals = lax.all_gather(
        jnp.stack([forward_total, backward_total])[None], "sp", axis=0, tiled=True
    )
    inclusive = jnp.cumsum(totals, axis=0)
    exclusive = inclusive - totals
    own_index = lax.axis_index("sp")
    own_inclusive = lax.dynamic_index_in_dim(inclusive, own_index, 0, keepdims=False)
    own_exclusive = lax.dynamic_index_in_dim(exclusive, own_index, 0, keepdims=False)
    pieces = (
        lax.all_gather(forward_state[None], "sp", axis=0, tiled=True),
        lax.all_gather(backward_state[None], "sp", axis=0, tiled=True),
    )
    piece_count = pieces[0].shape[0]
    span_index = lax.iota(jnp.int32, piece_count)
    forward_weight = jnp.where(
        (span_index < own_index)[:, None],
        jnp.exp(jnp.minimum(own_exclusive[0] - inclusive[:, 0], 0.0)),
        0.0,
    )
    backward_weight = jnp.where(
        (span_index > own_index)[:, None],
        jnp.exp(jnp.minimum(exclusive[:, 1] - own_inclusive[1], 0.0)),
        0.0,
    )
    into_forward = jnp.einsum(
        "nh,nhde->hde", forward_weight, pieces[0], precision=lax.Precision.HIGHEST
    )
    into_backward = jnp.einsum(
        "nh,nhde->hde", backward_weight, pieces[1], precision=lax.Precision.HIGHEST
    )
    forward_part = jnp.einsum(
        "ihd,hde->ihe",
        rotated_query,
        into_forward.astype(jnp.bfloat16),
        preferred_element_type=jnp.float32,
    )
    backward_part = jnp.einsum(
        "ihd,hde->ihe",
        rotated_query,
        into_backward.astype(jnp.bfloat16),
        preferred_element_type=jnp.float32,
    )
    mixed_heads = (
        local_part
        + jnp.exp(forward_cum).T[:, :, None] * forward_part
        + jnp.exp(backward_cum).T[:, :, None] * backward_part
    )
    scaled = mixed_heads * lax.rsqrt(
        jnp.mean(mixed_heads * mixed_heads, axis=-1, keepdims=True) + EPS
    )
    scaled = scaled * head_gain.reshape(head_count, HEAD_DIM)
    return (
        jax.nn.silu(gate_rows.astype(jnp.float32))
        * scaled.reshape(row_count, head_count * HEAD_DIM)
    ).astype(jnp.bfloat16)


def local(
    tokens,
    norm_gain,
    outer_gate,
    inner_gate,
    conv_input,
    query_proj,
    key_proj,
    value_proj,
    out_gate,
    conv_taps,
    log_decay,
    head_gain,
    conv_output,
    retention_output,
):
    whole = lax.all_gather(tokens, "tp", axis=1, tiled=True)
    wide = whole.astype(jnp.float32)
    normed = (
        wide * lax.rsqrt(jnp.mean(wide * wide, axis=-1, keepdims=True) + EPS) * norm_gain
    ).astype(jnp.bfloat16)
    row_count = normed.shape[0]
    offsets = lax.axis_index("sp") * row_count + lax.iota(jnp.int32, row_count)
    gathered = (
        lax.all_gather(outer_gate, "sp", axis=0, tiled=True),
        lax.all_gather(inner_gate, "sp", axis=0, tiled=True),
        lax.all_gather(conv_input, "sp", axis=0, tiled=True),
        lax.all_gather(query_proj, "sp", axis=0, tiled=True),
        lax.all_gather(key_proj, "sp", axis=0, tiled=True),
        lax.all_gather(value_proj, "sp", axis=0, tiled=True),
        lax.all_gather(out_gate, "sp", axis=0, tiled=True),
        lax.all_gather(conv_output, "sp", axis=1, tiled=True),
        lax.all_gather(retention_output, "sp", axis=1, tiled=True),
    )
    projected = [
        jnp.dot(normed, weight, preferred_element_type=jnp.float32).astype(jnp.bfloat16)
        for weight in gathered[:7]
    ]
    conv_out = conv_branch(projected[0], projected[1], projected[2], conv_taps)
    ret_out = retention_branch(
        projected[3], projected[4], projected[5], projected[6], log_decay, head_gain, offsets
    )
    conv_weight = gathered[7]
    ret_weight = gathered[8]
    return lax.psum_scatter(
        (
            jnp.dot(conv_out, conv_weight, preferred_element_type=jnp.float32)
            + jnp.dot(ret_out, ret_weight, preferred_element_type=jnp.float32)
        ).astype(jnp.bfloat16),
        "tp",
        scatter_dimension=0,
        tiled=True,
    )


def flipped(place, d):
    if d == 0:
        return place
    if d == 1:
        return place + 1 - 2 * lax.rem(place, 2)
    if d == 2:
        return place + 2 - 4 * lax.rem(lax.div(place, 2), 2)
    return 3 - place


LOG2E = 1.4426950408889634
CLASS_A, CLASS_B, CLASS_OUT = 0, 1, 2


def mixer_kernel(
    planes, group,
    tok_ref, key_w, query_w, value_w, gate_w, inner_w, conv_w, outer_w,
    cout_ref, rout_ref, rate_in, gain_ref, taps_ref, head_gain_ref, turn_ref, base_ref,
    mine_ref, theirs_ref,
    xin, x, w, wo, rates, cums, wide, ssq_out, ssq_in, cosines, sines, decay,
    ef, eb, kf, kb, rq_buf, v_buf, gate_buf, loc, state_f, state_b, pack_out, pack_in, into,
    acc, iv, parts, feat, share,
    own_sem, near_send, near_recv, rate_send, rate_recv, ssq_sem,
    tok_send, tok_recv, half_send, half_recv, far_send, far_recv,
    wo_send, wo_recv, halo_send, halo_recv, pack_send, pack_recv,
    ft_send, ft_recv, share_send, share_recv,
):
    f32, bf16 = jnp.float32, jnp.bfloat16
    own, core = lax.axis_index("sp"), lax.axis_index("tp")
    place, plane = lax.rem(own, group), lax.div(own, group)
    base = plane * group
    length, half = tok_ref.shape
    width = 2 * half
    quarter = half // 2
    rows_in = key_w.shape[0]
    ch = key_w.shape[1] // group
    heads = ch // HEAD_DIM
    all_rows = group * length
    side_rows = cout_ref.shape[0]
    out_cols = cout_ref.shape[1]
    part_cols = group * out_cols
    col_a, col_b = 4 * ch, 3 * ch
    has_up, has_down = plane < planes - 1, plane > 0
    middle = jnp.logical_and(has_up, has_down)
    top = lax.div(plane, planes // 2)
    mesh_id = pl.DeviceIdType.MESH
    chips = [base + flipped(place, d) for d in range(group)]
    partner = (own, 1 - core)
    weights = (key_w, query_w, value_w, gate_w, inner_w, conv_w, outer_w)

    def local_copy(source, target, i):
        return pltpu.make_async_copy(source, target, own_sem.at[i])

    def remote(source, target, send, recv, device):
        return pltpu.make_async_remote_copy(
            src_ref=source, dst_ref=target, send_sem=send, recv_sem=recv,
            device_id=device, device_id_type=mesh_id,
        )

    own_rows = pl.ds(pl.multiple_of(own * rows_in, 128), rows_in)
    own_cols = pl.ds(pl.multiple_of(own * out_cols, 128), out_cols)
    kept = [local_copy(tok_ref, xin, 0)]
    for j, source in enumerate(weights):
        kept.append(
            local_copy(
                source.at[:, pl.ds(pl.multiple_of(place * ch, 128), ch)],
                w.at[own_rows, pl.ds(j * ch, ch)], 1 + j,
            )
        )
    kept.append(local_copy(cout_ref, wo.at[pl.ds(0, side_rows), own_cols], 8))
    kept.append(local_copy(rout_ref, wo.at[pl.ds(side_rows, side_rows), own_cols], 9))
    kept.append(local_copy(rate_in, rates.at[place], 10))
    for copy in kept:
        copy.start()

    barrier = pltpu.get_barrier_semaphore()

    def greet(target):
        pl.semaphore_signal(barrier, inc=1, device_id=target, device_id_type=mesh_id)

    for d in range(1, group):
        greet((chips[d], core))
    greet(partner)
    for k in range(1, planes):
        greet((lax.rem(own + k * group, planes * group), core))
    pl.semaphore_wait(barrier, group + planes - 1)

    near = {}

    def send_near(j, d):
        to = flipped(place, d)
        near[(j, d)] = remote(
            weights[j].at[:, pl.ds(pl.multiple_of(to * ch, 128), ch)],
            w.at[own_rows, pl.ds(j * ch, ch)],
            near_send.at[j, d], near_recv.at[j, d], (chips[d], core),
        )
        near[(j, d)].start()

    for d in range(1, group):
        for j in range(4):
            send_near(j, d)
    rate_moves = [
        remote(rate_in, rates.at[place], rate_send.at[d], rate_recv.at[d], (chips[d], core))
        for d in range(1, group)
    ]
    for copy in rate_moves:
        copy.start()
    for d in range(1, group):
        for j in range(4, 7):
            send_near(j, d)

    def far(kind, direction, q, d):
        if kind == CLASS_OUT:
            block = wo.at[:, pl.ds(pl.multiple_of((q * group + place) * out_cols, 128), out_cols)]
        else:
            start = pl.multiple_of((q * group + flipped(place, d)) * rows_in, 128)
            cols = pl.ds(0, col_a) if kind == CLASS_A else pl.ds(col_a, col_b)
            block = w.at[pl.ds(start, rows_in), cols]
        target = own + group if direction == 0 else own - group
        return remote(
            block, block, far_send.at[kind, direction, q, d], far_recv.at[kind, q, d], (target, core)
        )

    def places_of(kind):
        return 1 if kind == CLASS_OUT else group

    def own_far(kind, d):
        pl.when(has_up)(lambda: far(kind, 0, plane, d).start())
        pl.when(has_down)(lambda: far(kind, 1, plane, d).start())

    def source_plane(r):
        if r == 0:
            return plane
        if r == 1:
            return plane + 1 - 2 * lax.rem(plane, 2)
        return r + top * (planes - 1 - 2 * r)

    def arrive(kind, r, only=None):
        q = source_plane(r)

        def take():
            for d in range(places_of(kind)):
                far(kind, 0, q, d).wait_recv()
                pl.when(jnp.logical_and(q < plane, has_up))(
                    lambda d=d: far(kind, 0, q, d).start()
                )
                pl.when(jnp.logical_and(q > plane, has_down))(
                    lambda d=d: far(kind, 1, q, d).start()
                )

        if only is None:
            take()
        else:
            pl.when(only)(take)

    ends = jnp.logical_not(middle)

    tile = length // 4
    kept[0].wait()
    for j in range(4):
        kept[1 + j].wait()
    own_far(CLASS_A, 0)

    @pl.loop(0, 4)
    def _(t):
        rows = pl.ds(pl.multiple_of(t * tile, tile), tile)
        value = xin[rows, :].astype(f32)
        value = value * value
        total = value[:, :128]
        for c in range(1, half // 128):
            total = total + value[:, c * 128 : (c + 1) * 128]
        ssq_out[rows, :] = total

    ssq_move = remote(ssq_out, ssq_in, ssq_sem.at[0], ssq_sem.at[1], partner)
    ssq_move.start()
    ssq_move.wait_recv()
    own_half = pl.multiple_of(core * half, 128)

    @pl.loop(0, 4)
    def _(t):
        rows = pl.ds(pl.multiple_of(t * tile, tile), tile)
        total = jnp.sum(ssq_out[rows, :] + ssq_in[rows, :], axis=-1, keepdims=True)
        scale = lax.rsqrt(total / width + EPS)
        value = xin[rows, :].astype(f32) * scale * gain_ref[:, pl.ds(own_half, half)]
        x[pl.ds(pl.multiple_of(place * length + t * tile, tile), tile), pl.ds(own_half, half)] = (
            value.astype(bf16)
        )

    def span_rows(s):
        return pl.ds(pl.multiple_of(s * length, 128), length)

    def piece(d, which):
        return x.at[
            span_rows(flipped(place, d)),
            pl.ds(pl.multiple_of(core * half + which * quarter, 128), quarter),
        ]

    tokens = {}

    def send_piece(which, d_from, hop):
        d_there = d_from + hop
        tokens[(which, d_there)] = remote(
            piece(d_from, which), piece(d_from, which),
            tok_send.at[which, d_there], tok_recv.at[which, d_there], (chips[hop], core),
        )
        tokens[(which, d_there)].start()

    def send_half(d):
        block = x.at[span_rows(flipped(place, d)), pl.ds(own_half, half)]
        remote(block, block, half_send.at[d], half_recv.at[d], partner).start()

    send_piece(0, 0, 1)
    send_piece(1, 0, 2)
    send_piece(1, 0, 1)
    send_piece(0, 0, 2)
    send_half(0)

    for d in range(1, group):
        for j in range(4):
            near[(j, d)].wait_recv()
        own_far(CLASS_A, d)

    kept[10].wait()
    for copy in rate_moves:
        copy.wait_recv()
    for s in range(group):
        for way in range(2):
            for h in range(heads):
                cums[pl.ds(s * 8 + way * heads + h, 1), :] = rates[
                    s, way, pl.ds(heads * place + h, 1), :
                ]
        cums[pl.ds(s * 8 + 2 * heads, 8 - 2 * heads), :] = jnp.zeros(
            (8 - 2 * heads, length), f32
        )
    lanes = lax.broadcasted_iota(jnp.int32, (group * 8, length), 1)
    kinds = lax.rem(lax.broadcasted_iota(jnp.int32, (group * 8, length), 0), 8)
    running = cums[...] * LOG2E
    step = 1
    while step < length:
        ahead = jnp.where(lanes >= step, pltpu.roll(running, step, 1), 0.0)
        behind = jnp.where(lanes < length - step, pltpu.roll(running, length - step, 1), 0.0)
        running = running + jnp.where(kinds < heads, ahead, behind)
        step *= 2
    cums[...] = running
    wide[...] = jnp.zeros_like(wide)
    first_head = lax.broadcasted_iota(jnp.int32, (length, ch), 1) < HEAD_DIM
    lane_in_head = lax.rem(lax.broadcasted_iota(jnp.int32, (length, ch), 1), HEAD_DIM)
    leading = lane_in_head < HEAD_DIM // 2

    @pl.loop(0, group)
    def _(s):
        sums = cums[pl.ds(pl.multiple_of(s * 8, 8), 8), :]
        wide[0:8, :] = sums
        columns = wide[...].T
        cf = [columns[:, h : h + 1] for h in range(heads)]
        rb = [columns[:, heads + h : heads + h + 1] for h in range(heads)]
        cf_wide = jnp.where(first_head, cf[0], cf[1])
        rb_wide = jnp.where(first_head, rb[0], rb[1])
        ef[s] = jnp.exp2(cf_wide)
        eb[s] = jnp.exp2(rb_wide)
        kf[s] = jnp.exp2(cf_wide[length - 1 : length, :] - cf_wide)
        kb[s] = jnp.exp2(rb_wide[0:1, :] - rb_wide)
        row_at = lax.broadcasted_iota(jnp.int32, (length, length), 0)
        col_at = lax.broadcasted_iota(jnp.int32, (length, length), 1)
        for h in range(heads):
            spread = jnp.where(
                col_at <= row_at, cf[h] - sums[h : h + 1, :], rb[h] - sums[heads + h : heads + h + 1, :]
            )
            decay[s, h] = jnp.exp2(spread)
        turn = base_ref[base + s]
        cos_0, sin_0 = turn[0:1, :], turn[1:2, :]
        cos_i, sin_i = turn_ref[0], turn_ref[1]
        cosines[s] = cos_0 * cos_i - sin_0 * sin_i
        angle_sine = sin_0 * cos_i + cos_0 * sin_i
        sines[s] = jnp.where(leading, -angle_sine, angle_sine)

    arrive(CLASS_A, 1)
    for d in range(1, group):
        for j in range(4, 7):
            near[(j, d)].wait_recv()
    for j in range(4, 7):
        kept[1 + j].wait()
    for d in range(group):
        own_far(CLASS_B, d)
    tokens[(0, 1)].wait_recv()
    send_piece(0, 1, 2)
    tokens[(1, 2)].wait_recv()
    send_piece(1, 2, 1)
    arrive(CLASS_A, 2)
    tokens[(1, 1)].wait_recv()
    send_half(1)
    tokens[(0, 2)].wait_recv()
    send_half(2)
    arrive(CLASS_A, 3)
    arrive(CLASS_B, 1, middle)
    arrive(CLASS_B, 2, middle)
    kept[8].wait()
    kept[9].wait()
    pl.when(ends)(lambda: own_far(CLASS_OUT, 0))

    def out_piece(r, d, which):
        start = pl.multiple_of((source_plane(r) * group + flipped(place, d)) * out_cols, 128)
        return wo.at[pl.ds(which * side_rows, side_rows), pl.ds(start, out_cols)]

    def out_move(r, which, d_there, hop):
        block = out_piece(r, d_there - hop, which)
        return remote(
            block, block, wo_send.at[r, which, d_there], wo_recv.at[r, which, d_there],
            (chips[hop], core),
        )

    def out_landed(r, which, d):
        block = out_piece(r, d, which)
        remote(
            block, block, wo_send.at[r, which, d], wo_recv.at[r, which, d], (chips[1], core)
        ).wait_recv()

    def spread_out(r):
        for which, hop in ((0, 1), (1, 2), (1, 1), (0, 2)):
            out_move(r, which, hop, hop).start()

    def relay_out(r):
        out_landed(r, 0, 1)
        out_move(r, 0, 3, 2).start()
        out_landed(r, 1, 2)
        out_move(r, 1, 3, 1).start()

    def finish_out(r):
        for which, d in ((1, 1), (0, 2), (0, 3), (1, 3)):
            out_landed(r, which, d)

    def wait_half(d):
        block = x.at[
            span_rows(flipped(place, d)), pl.ds(pl.multiple_of((1 - core) * half, 128), half)
        ]
        remote(block, block, half_send.at[d], half_recv.at[d], partner).wait_recv()

    spread_out(0)
    wait_half(0)

    def one_span(s):
        rows = span_rows(s)
        held = jnp.dot(x[rows, :], w[:, 0:col_a], preferred_element_type=f32)
        cosine, sine = cosines[s], sines[s]

        def turned(value):
            value = value.astype(bf16).astype(f32)
            other = jnp.where(
                leading,
                pltpu.roll(value, ch - HEAD_DIM // 2, 1),
                pltpu.roll(value, HEAD_DIM // 2, 1),
            )
            return value * cosine + other * sine

        rk = (turned(held[:, 0:ch]) * HEAD_DIM ** (-0.5)).astype(bf16).astype(f32)
        rq = turned(held[:, ch : 2 * ch]).astype(bf16)
        value = held[:, 2 * ch : 3 * ch].astype(bf16)
        rq_buf[s] = rq
        v_buf[s] = value
        gate_buf[s] = held[:, 3 * ch : 4 * ch].astype(bf16)
        value_wide = value.astype(f32)
        found = None
        for h in range(heads):
            in_head = first_head if h == 0 else jnp.logical_not(first_head)
            key_head = jnp.where(in_head, rk, 0.0).astype(bf16)
            value_head = jnp.where(in_head, value_wide, 0.0).astype(bf16)
            scores = lax.dot_general(
                rq, key_head, (((1,), (1,)), ((), ())), preferred_element_type=f32
            )
            probs = (scores * decay[s, h]).astype(bf16)
            part = jnp.dot(probs, value_head, preferred_element_type=f32)
            found = part if found is None else found + part
        loc[s] = found
        same_head = (
            lax.div(lax.broadcasted_iota(jnp.int32, (ch, ch), 0), HEAD_DIM)
            == lax.div(lax.broadcasted_iota(jnp.int32, (ch, ch), 1), HEAD_DIM)
        )
        for table, target in ((kf, state_f), (kb, state_b)):
            keys = (rk * table[s]).astype(bf16)
            state = lax.dot_general(
                keys, value, (((0,), (0,)), ((), ())), preferred_element_type=f32
            )
            target[s] = jnp.where(same_head, state, 0.0)

    halo_rows = 16
    halos = [
        remote(
            x.at[pl.ds(all_rows - halo_rows, halo_rows), :], x.at[pl.ds(all_rows, halo_rows), :],
            halo_send.at[0], halo_recv.at[0], (own + group, core),
        ),
        remote(
            x.at[pl.ds(0, halo_rows), :], x.at[pl.ds(all_rows + halo_rows, halo_rows), :],
            halo_send.at[1], halo_recv.at[1], (own - group, core),
        ),
    ]
    blank = jnp.zeros((halo_rows, width), bf16)

    @pl.when(jnp.logical_not(has_down))
    def _():
        x[pl.ds(all_rows, halo_rows), :] = blank

    @pl.when(jnp.logical_not(has_up))
    def _():
        x[pl.ds(all_rows + halo_rows, halo_rows), :] = blank

    @pl.loop(0, group)
    def _(d):
        @pl.when(d == 1)
        def _():
            tokens[(0, 3)].wait_recv()
            tokens[(1, 3)].wait_recv()
            send_half(3)
            wait_half(1)

        @pl.when(d == 2)
        def _():
            wait_half(2)
            relay_out(0)

        @pl.when(d == 3)
        def _():
            wait_half(3)
            pl.when(has_up)(lambda: halos[0].start())
            pl.when(has_down)(lambda: halos[1].start())
            arrive(CLASS_B, 3, middle)

        one_span(lax.rem(lax.rem(place, 2) + lax.rem(d, 2), 2)
                 + 2 * lax.rem(lax.div(place, 2) + lax.div(d, 2), 2))

    def scan_states(state, table, at, order, target):
        passed, inside, reach = jnp.zeros((ch, ch), f32), {}, {}
        over = jnp.ones((1, ch), f32)
        for s in order:
            inside[s], reach[s] = passed, over
            factor = table[s, at : at + 1, :]
            passed = factor * passed + state[s]
            over = over * factor
        pack_out[target, 0:ch, :] = passed
        pack_out[target, ch : ch + 8, :] = jnp.broadcast_to(over, (8, ch))
        return inside, reach

    ahead_in, ahead_reach = scan_states(state_f, ef, length - 1, range(group), 0)
    back_in, back_reach = scan_states(state_b, eb, 0, range(group)[::-1], 1)

    def pack_move(way, k):
        to = own + k * group if way == 0 else own - k * group
        return remote(
            pack_out.at[way], pack_in.at[way, k - 1],
            pack_send.at[way, k], pack_recv.at[way, k], (to, core),
        )

    def gives(way, k):
        return plane + k < planes if way == 0 else plane - k >= 0

    def takes(way, k):
        return gives(1 - way, k)

    for k in range(1, planes):
        for way in range(2):
            pl.when(gives(way, k))(lambda way=way, k=k: pack_move(way, k).start())
    pl.when(middle)(lambda: own_far(CLASS_OUT, 0))

    arrive(CLASS_B, 1, ends)
    arrive(CLASS_B, 2, ends)
    pl.when(has_down)(lambda: halos[0].wait_recv())
    pl.when(has_up)(lambda: halos[1].wait_recv())
    depth = group * rows_in
    most = (planes - 1) * depth
    early = pl.multiple_of(top * depth, 128)
    late = pl.multiple_of((1 - top) * most, 128)
    blocks = 5
    block = (all_rows + 2 * halo_rows) // blocks

    @pl.loop(0, blocks)
    def _(t):
        rows = pl.ds(pl.multiple_of(t * block, 16), block)
        acc[rows, :] = jnp.dot(
            x[rows, pl.ds(early, most)], w[pl.ds(early, most), col_a : col_a + col_b],
            preferred_element_type=f32,
        )

    arrive(CLASS_B, 3, ends)

    @pl.loop(0, blocks)
    def _(t):
        rows = pl.ds(pl.multiple_of(t * block, 16), block)
        held = acc[rows, :] + jnp.dot(
            x[rows, pl.ds(late, depth)], w[pl.ds(late, depth), col_a : col_a + col_b],
            preferred_element_type=f32,
        )
        held = held.astype(bf16).astype(f32)
        iv[pl.ds(pl.multiple_of(t * block + 8, 8), block), :] = (
            (held[:, 0:ch] * held[:, ch : 2 * ch]).astype(bf16).astype(f32)
        )
        acc[rows, 2 * ch : 3 * ch] = held[:, 2 * ch : 3 * ch]

    iv[7:8, :] = iv[all_rows + halo_rows + 7 : all_rows + halo_rows + 8, :]
    iv[all_rows + 8 : all_rows + 9, :] = iv[all_rows + halo_rows + 8 : all_rows + halo_rows + 9, :]
    own_taps = taps_ref[:, pl.ds(pl.multiple_of(place * ch, 128), ch)]
    for s in range(group):
        at = s * length
        near_sum = (
            own_taps[0:1, :] * iv[at + 7 : at + 7 + length, :]
            + own_taps[1:2, :] * iv[at + 8 : at + 8 + length, :]
            + own_taps[2:3, :] * iv[at + 9 : at + 9 + length, :]
        )
        parts[0, s] = (acc[at : at + length, 2 * ch : 3 * ch] * near_sum).astype(bf16)

    def feature_cols(kind):
        return pl.ds(pl.multiple_of(kind * side_rows + place * ch, 128), ch)

    def feature_move(kind, d, s, to):
        return remote(
            parts.at[kind, s], feat.at[:, feature_cols(kind)],
            ft_send.at[kind, d], ft_recv.at[kind, d], (to, core),
        )

    for d in (3, 1, 2):
        feature_move(0, d, flipped(place, d), chips[d]).start()
    feat[:, feature_cols(0)] = parts[0, place]

    arrive(CLASS_OUT, 1)
    spread_out(1)

    incoming = []
    for way in range(2):
        into[way] = jnp.zeros((ch, ch), f32)
        into[way + 2] = jnp.ones((ch, ch), f32)
        for k in range(1, planes):
            @pl.when(takes(way, k))
            def _(way=way, k=k):
                pack_move(way, k).wait_recv()
                into[way] = into[way] + into[way + 2] * pack_in[way, k - 1, 0:ch, :]
                into[way + 2] = into[way + 2] * pack_in[way, k - 1, ch : ch + 1, :]
        incoming.append(into[way])
    for s in range(group):
        state_f[s] = ahead_in[s] + ahead_reach[s] * incoming[0]
        state_b[s] = back_in[s] + back_reach[s] * incoming[1]

    @pl.loop(0, group)
    def _(i):
        d = group - 1 - i
        s = (lax.rem(lax.rem(place, 2) + lax.rem(d, 2), 2)
             + 2 * lax.rem(lax.div(place, 2) + lax.div(d, 2), 2))
        query = rq_buf[s]
        mix = (
            loc[s]
            + ef[s] * jnp.dot(query, state_f[s].astype(bf16), preferred_element_type=f32)
            + eb[s] * jnp.dot(query, state_b[s].astype(bf16), preferred_element_type=f32)
        )
        squares = mix * mix
        first = jnp.sum(jnp.where(first_head, squares, 0.0), axis=-1, keepdims=True)
        second = jnp.sum(jnp.where(first_head, 0.0, squares), axis=-1, keepdims=True)
        scale = lax.rsqrt(jnp.where(first_head, first, second) / HEAD_DIM + EPS)
        gate = gate_buf[s].astype(f32)
        gain = head_gain_ref[:, pl.ds(pl.multiple_of(place * ch, 128), ch)]
        parts[1, s] = (gate / (1.0 + jnp.exp(-gate)) * (mix * scale * gain)).astype(bf16)

        @pl.when(d > 0)
        def _():
            feature_move(1, d, s, base + s).start()

    feat[:, feature_cols(1)] = parts[1, place]

    relay_out(1)
    arrive(CLASS_OUT, 2)
    spread_out(2)
    relay_out(2)
    arrive(CLASS_OUT, 3)
    spread_out(3)
    for kind in range(2):
        for d in (1, 2, 3):
            feature_move(kind, d, flipped(place, d), chips[d]).wait_recv()

    my_rows = length // 2
    shares = []

    def project(r):
        cols = pl.ds(pl.multiple_of(source_plane(r) * part_cols, 128), part_cols)

        def rows_of(c):
            return jnp.dot(
                feat[pl.ds(pl.multiple_of(c * my_rows, 128), my_rows), :], wo[:, cols],
                preferred_element_type=f32,
            ).astype(bf16)

        share[:, cols] = rows_of(1 - core)
        move = remote(
            share.at[:, cols], theirs_ref.at[:, cols], share_send.at[r], share_recv.at[r], partner
        )
        move.start()
        shares.append(move)
        mine_ref[:, cols] = rows_of(core)

    finish_out(0)
    project(0)
    finish_out(1)
    project(1)
    relay_out(3)
    finish_out(2)
    project(2)
    finish_out(3)
    project(3)

    for move in shares:
        move.wait()
    for copy in near.values():
        copy.wait_send()
    for copy in rate_moves:
        copy.wait_send()
    ssq_move.wait_send()
    for copy in tokens.values():
        copy.wait_send()
    for d in range(group):
        halves_block = x.at[span_rows(flipped(place, d)), pl.ds(own_half, half)]
        remote(halves_block, halves_block, half_send.at[d], half_recv.at[d], partner).wait_send()
    for r in range(planes):
        for which, d, hop in ((0, 1, 1), (1, 1, 1), (0, 2, 2), (1, 2, 2), (0, 3, 2), (1, 3, 1)):
            out_move(r, which, d, hop).wait_send()
    pl.when(has_up)(lambda: halos[0].wait_send())
    pl.when(has_down)(lambda: halos[1].wait_send())
    for k in range(1, planes):
        for way in range(2):
            pl.when(gives(way, k))(lambda way=way, k=k: pack_move(way, k).wait_send())
    for kind in range(2):
        for d in range(1, group):
            feature_move(kind, d, flipped(place, d), chips[d]).wait_send()
    for kind in range(3):
        for q in range(planes):
            for d in range(places_of(kind)):
                pl.when(jnp.logical_and(q <= plane, has_up))(
                    lambda kind=kind, q=q, d=d: far(kind, 0, q, d).wait_send()
                )
                pl.when(jnp.logical_and(q >= plane, has_down))(
                    lambda kind=kind, q=q, d=d: far(kind, 1, q, d).wait_send()
                )


def turn_tables(spans, length, channels):
    half_dim = HEAD_DIM // 2
    frequency = THETA ** (-2.0 * (np.arange(channels) % half_dim) / HEAD_DIM)
    inner = np.arange(length)[:, None] * frequency
    outer = (np.arange(spans) * length)[:, None] * frequency
    turn = np.stack([np.cos(inner), np.sin(inner)])
    start = np.zeros((spans, 8, channels))
    start[:, 0], start[:, 1] = np.cos(outer), np.sin(outer)
    return turn.astype(np.float32), start.astype(np.float32)


def mixer(planes, group, arrays):
    (
        tokens, norm_gain, outer_gate, inner_gate, conv_input, query_proj, key_proj, value_proj,
        out_gate, conv_taps, log_decay, head_gain, conv_output, retention_output,
    ) = arrays
    f32, bf16 = jnp.float32, jnp.bfloat16
    length, half = tokens.shape
    width = 2 * half
    ch = outer_gate.shape[1] // group
    heads = ch // HEAD_DIM
    rows, side = group * length, conv_output.shape[0]
    turn, start = turn_tables(planes * group, length, ch)
    dma = pltpu.SemaphoreType.DMA
    vmem, anywhere = pl.BlockSpec(memory_space=pltpu.VMEM), pl.BlockSpec(memory_space=pl.ANY)
    v = pltpu.VMEM
    result = jax.ShapeDtypeStruct((length // 2, width), bf16)
    table = v((group, length, ch), f32)
    mine, theirs = pl.pallas_call(
        functools.partial(mixer_kernel, planes, group),
        out_shape=(result, result),
        in_specs=[anywhere] * 11 + [vmem] * 5,
        out_specs=[vmem, vmem],
        scratch_shapes=[
            v((length, half), bf16), v((rows + 32, width), bf16), v((width, 7 * ch), bf16),
            v((2 * side, width), bf16), v((group,) + log_decay.shape, f32),
            v((8 * group, length), f32), v((128, length), f32),
            v((length, 128), f32), v((length, 128), f32),
            table, table, v((group, heads, length, length), f32),
            table, table, table, table,
            v((group, length, ch), bf16), v((group, length, ch), bf16), v((group, length, ch), bf16),
            table, v((group, ch, ch), f32), v((group, ch, ch), f32),
            v((2, ch + 8, ch), f32), v((2, planes - 1, ch + 8, ch), f32), v((4, ch, ch), f32),
            v((rows + 32, 3 * ch), f32), v((rows + 48, ch), f32),
            v((2, group, length, ch), bf16), v((length, 2 * side), bf16),
            v((length // 2, width), bf16),
            dma((11,)), dma((7, group)), dma((7, group)), dma((group,)), dma((group,)), dma((2,)),
            dma((2, group)), dma((2, group)), dma((group,)), dma((group,)),
            dma((3, 2, planes, group)), dma((3, planes, group)),
            dma((planes, 2, group)), dma((planes, 2, group)), dma((2,)), dma((2,)),
            dma((2, planes)), dma((2, planes)), dma((2, group)), dma((2, group)),
            dma((planes,)), dma((planes,)),
        ],
        compiler_params=pltpu.CompilerParams(
            collective_id=0, has_side_effects=True, vmem_limit_bytes=60 * 2**20
        ),
    )(
        tokens, key_proj, query_proj, value_proj, out_gate, inner_gate, conv_input, outer_gate,
        conv_output, retention_output, log_decay, norm_gain.reshape(1, -1), conv_taps,
        head_gain.reshape(1, -1), jnp.asarray(turn), jnp.asarray(start),
    )
    return (mine.astype(f32) + theirs.astype(f32)).astype(bf16)


LANES = 128

def plan(*arrays):
    spans, cores = lax.axis_size("sp"), lax.axis_size("tp")
    group = arrays[2].shape[1] // LANES
    planes = spans // group
    fits = (
        cores == 2
        and group == 4
        and planes * group == spans
        and planes == 2 * cores
        and arrays[0].shape[1] == 2 * group * arrays[2].shape[0]
    )
    return mixer(planes, group, arrays) if fits else local(*arrays)


def solution(mesh):
    return jax.shard_map(
        plan,
        mesh=mesh,
        in_specs=(
            P("sp", "tp"),
            P(),
            P("sp", "tp"),
            P("sp", "tp"),
            P("sp", "tp"),
            P("sp", "tp"),
            P("sp", "tp"),
            P("sp", "tp"),
            P("sp", "tp"),
            P(None, "tp"),
            P(None, "tp", "sp"),
            P("tp"),
            P("tp", "sp"),
            P("tp", "sp"),
        ),
        out_specs=P(("sp", "tp"), None),
        check_vma=False,
    )
```

```python
import jax
import functools
import jax.numpy as jnp
import numpy as np
from jax import lax
from jax.experimental import pallas as pl
from jax.experimental.pallas import tpu as pltpu
from jax.sharding import PartitionSpec as P

HEAD_DIM = 64


EPS = 1e-06
THETA = 10000.0


def with_halo(shard, sides, width):
    for axis, dim in sides:
        size, length = (lax.axis_size(axis), shard.shape[dim])
        up = [(i, (i + 1) % size) for i in range(size - 1)]
        down = [(j, i) for i, j in up]
        last = lax.slice_in_dim(shard, length - width, length, axis=dim)
        first = lax.slice_in_dim(shard, 0, width, axis=dim)
        before = lax.ppermute(last, axis, up)
        after = lax.ppermute(first, axis, down)
        shard = jnp.concatenate([before, shard, after], axis=dim)
    return shard


def rotate(field_in, position_list):
    half_dim = field_in.shape[-1] // 2
    frequency = jnp.exp(
        -jnp.log(THETA) * jnp.arange(half_dim, dtype=jnp.float32) * (2.0 / field_in.shape[-1])
    )
    angles = position_list.astype(jnp.float32)[:, None, None] * frequency
    cosine = jnp.cos(angles)
    sine_part = jnp.sin(angles)
    leading = field_in[..., :half_dim]
    trailing = field_in[..., half_dim:]
    return jnp.concatenate(
        [leading * cosine - trailing * sine_part, leading * sine_part + trailing * cosine], axis=-1
    )


def conv_branch(outer_rows, inner_rows, conv_values, conv_taps):
    inner_value = (inner_rows.astype(jnp.float32) * conv_values.astype(jnp.float32)).astype(
        jnp.bfloat16
    )
    padded = with_halo(inner_value, (("sp", 0),), 1).astype(jnp.float32)
    convolved = conv_taps[0] * padded[:-2] + conv_taps[1] * padded[1:-1] + conv_taps[2] * padded[2:]
    return (outer_rows.astype(jnp.float32) * convolved).astype(jnp.bfloat16)


def span_parts(query_rows, key_rows, value_rows, log_rates):
    length = query_rows.shape[0]
    forward_cum = jnp.cumsum(log_rates[0], axis=-1)
    backward_cum = jnp.flip(jnp.cumsum(jnp.flip(log_rates[1], -1), axis=-1), -1)
    row_index = lax.broadcasted_iota(jnp.int32, (length, length), 0)
    col_index = lax.broadcasted_iota(jnp.int32, (length, length), 1)
    lower_part = (col_index <= row_index)[None]
    spread = jnp.where(
        lower_part,
        forward_cum[:, :, None] - forward_cum[:, None, :],
        backward_cum[:, :, None] - backward_cum[:, None, :],
    )
    scores = jnp.einsum("ihe,jhe->hij", query_rows, key_rows, preferred_element_type=jnp.float32)
    weighted = (scores * jnp.exp(spread)).astype(jnp.bfloat16)
    local_part = jnp.einsum(
        "hij,jhe->ihe", weighted, value_rows, preferred_element_type=jnp.float32
    )
    key_wide = key_rows.astype(jnp.float32)
    forward_keys = (key_wide * jnp.exp(forward_cum[:, -1:] - forward_cum).T[:, :, None]).astype(
        jnp.bfloat16
    )
    backward_keys = (key_wide * jnp.exp(backward_cum[:, :1] - backward_cum).T[:, :, None]).astype(
        jnp.bfloat16
    )
    forward_state = jnp.einsum(
        "jhd,jhe->hde", forward_keys, value_rows, preferred_element_type=jnp.float32
    )
    backward_state = jnp.einsum(
        "jhd,jhe->hde", backward_keys, value_rows, preferred_element_type=jnp.float32
    )
    return (local_part, forward_cum, backward_cum, forward_state, backward_state)


def retention_branch(query_rows, key_rows, value_rows, gate_rows, log_decay, head_gain, offsets):
    row_count = query_rows.shape[0]
    head_count = query_rows.shape[1] // HEAD_DIM
    shape_heads = (row_count, head_count, HEAD_DIM)
    rotated_query = rotate(query_rows.astype(jnp.float32).reshape(shape_heads), offsets).astype(
        jnp.bfloat16
    )
    rotated_key = (
        rotate(key_rows.astype(jnp.float32).reshape(shape_heads), offsets) * HEAD_DIM ** (-0.5)
    ).astype(jnp.bfloat16)
    local_part, forward_cum, backward_cum, forward_state, backward_state = span_parts(
        rotated_query, rotated_key, value_rows.reshape(shape_heads), log_decay
    )
    forward_total = forward_cum[:, -1]
    backward_total = backward_cum[:, 0]
    totals = lax.all_gather(
        jnp.stack([forward_total, backward_total])[None], "sp", axis=0, tiled=True
    )
    inclusive = jnp.cumsum(totals, axis=0)
    exclusive = inclusive - totals
    own_index = lax.axis_index("sp")
    own_inclusive = lax.dynamic_index_in_dim(inclusive, own_index, 0, keepdims=False)
    own_exclusive = lax.dynamic_index_in_dim(exclusive, own_index, 0, keepdims=False)
    pieces = (
        lax.all_gather(forward_state[None], "sp", axis=0, tiled=True),
        lax.all_gather(backward_state[None], "sp", axis=0, tiled=True),
    )
    piece_count = pieces[0].shape[0]
    span_index = lax.iota(jnp.int32, piece_count)
    forward_weight = jnp.where(
        (span_index < own_index)[:, None],
        jnp.exp(jnp.minimum(own_exclusive[0] - inclusive[:, 0], 0.0)),
        0.0,
    )
    backward_weight = jnp.where(
        (span_index > own_index)[:, None],
        jnp.exp(jnp.minimum(exclusive[:, 1] - own_inclusive[1], 0.0)),
        0.0,
    )
    into_forward = jnp.einsum(
        "nh,nhde->hde", forward_weight, pieces[0], precision=lax.Precision.HIGHEST
    )
    into_backward = jnp.einsum(
        "nh,nhde->hde", backward_weight, pieces[1], precision=lax.Precision.HIGHEST
    )
    forward_part = jnp.einsum(
        "ihd,hde->ihe",
        rotated_query,
        into_forward.astype(jnp.bfloat16),
        preferred_element_type=jnp.float32,
    )
    backward_part = jnp.einsum(
        "ihd,hde->ihe",
        rotated_query,
        into_backward.astype(jnp.bfloat16),
        preferred_element_type=jnp.float32,
    )
    mixed_heads = (
        local_part
        + jnp.exp(forward_cum).T[:, :, None] * forward_part
        + jnp.exp(backward_cum).T[:, :, None] * backward_part
    )
    scaled = mixed_heads * lax.rsqrt(
        jnp.mean(mixed_heads * mixed_heads, axis=-1, keepdims=True) + EPS
    )
    scaled = scaled * head_gain.reshape(head_count, HEAD_DIM)
    return (
        jax.nn.silu(gate_rows.astype(jnp.float32))
        * scaled.reshape(row_count, head_count * HEAD_DIM)
    ).astype(jnp.bfloat16)


def local(
    tokens,
    norm_gain,
    outer_gate,
    inner_gate,
    conv_input,
    query_proj,
    key_proj,
    value_proj,
    out_gate,
    conv_taps,
    log_decay,
    head_gain,
    conv_output,
    retention_output,
):
    whole = lax.all_gather(tokens, "tp", axis=1, tiled=True)
    wide = whole.astype(jnp.float32)
    normed = (
        wide * lax.rsqrt(jnp.mean(wide * wide, axis=-1, keepdims=True) + EPS) * norm_gain
    ).astype(jnp.bfloat16)
    row_count = normed.shape[0]
    offsets = lax.axis_index("sp") * row_count + lax.iota(jnp.int32, row_count)
    gathered = (
        lax.all_gather(outer_gate, "sp", axis=0, tiled=True),
        lax.all_gather(inner_gate, "sp", axis=0, tiled=True),
        lax.all_gather(conv_input, "sp", axis=0, tiled=True),
        lax.all_gather(query_proj, "sp", axis=0, tiled=True),
        lax.all_gather(key_proj, "sp", axis=0, tiled=True),
        lax.all_gather(value_proj, "sp", axis=0, tiled=True),
        lax.all_gather(out_gate, "sp", axis=0, tiled=True),
        lax.all_gather(conv_output, "sp", axis=1, tiled=True),
        lax.all_gather(retention_output, "sp", axis=1, tiled=True),
    )
    projected = [
        jnp.dot(normed, weight, preferred_element_type=jnp.float32).astype(jnp.bfloat16)
        for weight in gathered[:7]
    ]
    conv_out = conv_branch(projected[0], projected[1], projected[2], conv_taps)
    ret_out = retention_branch(
        projected[3], projected[4], projected[5], projected[6], log_decay, head_gain, offsets
    )
    conv_weight = gathered[7]
    ret_weight = gathered[8]
    return lax.psum_scatter(
        (
            jnp.dot(conv_out, conv_weight, preferred_element_type=jnp.float32)
            + jnp.dot(ret_out, ret_weight, preferred_element_type=jnp.float32)
        ).astype(jnp.bfloat16),
        "tp",
        scatter_dimension=0,
        tiled=True,
    )


def flipped(place, d):
    if d == 0:
        return place
    if d == 1:
        return place + 1 - 2 * lax.rem(place, 2)
    if d == 2:
        return place + 2 - 4 * lax.rem(lax.div(place, 2), 2)
    return 3 - place


LOG2E = 1.4426950408889634
CLASS_A, CLASS_B, CLASS_OUT = 0, 1, 2


def mixer_kernel(
    planes, group,
    tok_ref, key_w, query_w, value_w, gate_w, inner_w, conv_w, outer_w,
    cout_ref, rout_ref, rate_in, gain_in, taps_in, head_gain_in, turn_in, base_in,
    out_ref, gain_ref, taps_ref, head_gain_ref, turn_ref, base_ref,
    xin, x, w, wo, rate_own, rate_pack, rates, cums, wide, ssq_out, ssq_in, cosines, sines, decay,
    ef, eb, kf, kb, rq_buf, v_buf, gate_buf, loc, state_f, state_b, pack_out, pack_in, into,
    acc, iv, parts, feat, share, theirs,
    own_sem, near_send, near_recv, rate_send, rate_recv, ssq_sem,
    tok_send, tok_recv, half_send, half_recv, far_send, far_recv, out_recv,
    wo_send, wo_recv, halo_send, halo_recv, pack_send, pack_recv,
    ft_send, ft_recv, share_send, share_recv,
):
    f32, bf16 = jnp.float32, jnp.bfloat16
    own, core = lax.axis_index("sp"), lax.axis_index("tp")
    place, plane = lax.rem(own, group), lax.div(own, group)
    base = plane * group
    length, half = tok_ref.shape
    width = 2 * half
    quarter = half // 2
    rows_in = key_w.shape[0]
    ch = key_w.shape[1] // group
    heads = ch // HEAD_DIM
    all_rows = group * length
    side_rows = cout_ref.shape[0]
    out_cols = cout_ref.shape[1]
    part_cols = group * out_cols
    col_a, col_b = 4 * ch, 3 * ch
    has_up, has_down = plane < planes - 1, plane > 0
    middle = jnp.logical_and(has_up, has_down)
    top = lax.div(plane, planes // 2)
    mesh_id = pl.DeviceIdType.MESH
    chips = [base + flipped(place, d) for d in range(group)]
    partner = (own, 1 - core)
    weights = (key_w, query_w, value_w, gate_w, inner_w, conv_w, outer_w)

    def local_copy(source, target, i):
        return pltpu.make_async_copy(source, target, own_sem.at[i])

    def remote(source, target, send, recv, device):
        return pltpu.make_async_remote_copy(
            src_ref=source, dst_ref=target, send_sem=send, recv_sem=recv,
            device_id=device, device_id_type=mesh_id,
        )

    own_rows = pl.ds(pl.multiple_of(own * rows_in, 128), rows_in)
    own_cols = pl.ds(pl.multiple_of(own * out_cols, 128), out_cols)
    kept = [local_copy(tok_ref, xin, 0), local_copy(rate_in, rate_own, 1)]
    for j, source in enumerate(weights):
        kept.append(
            local_copy(
                source.at[:, pl.ds(pl.multiple_of(place * ch, 128), ch)],
                w.at[own_rows, pl.ds(j * ch, ch)], 2 + j // 4,
            )
        )
    kept.append(local_copy(cout_ref, wo.at[pl.ds(0, side_rows), own_cols], 4))
    kept.append(local_copy(rout_ref, wo.at[pl.ds(side_rows, side_rows), own_cols], 4))
    place_cols = pl.ds(pl.multiple_of(place * ch, 128), ch)
    small = [
        local_copy(gain_in, gain_ref, 5),
        local_copy(taps_in, taps_ref, 6),
        local_copy(head_gain_in, head_gain_ref, 7),
        local_copy(turn_in, turn_ref, 8),
        local_copy(base_in.at[pl.ds(base, group)], base_ref, 9),
    ]
    for copy in kept + small:
        copy.start()

    def class_cols(kind):
        return pl.ds(0, col_a) if kind == CLASS_A else pl.ds(col_a, col_b)

    def own_here(kind):
        block = wo.at[:, own_cols] if kind == CLASS_OUT else w.at[own_rows, class_cols(kind)]
        local_copy(block, block, 2 + kind).wait()

    barrier = pltpu.get_barrier_semaphore()

    def greet(target):
        pl.semaphore_signal(barrier, inc=1, device_id=target, device_id_type=mesh_id)

    for d in range(1, group):
        greet((chips[d], core))
    greet(partner)
    for k in range(1, planes):
        greet((lax.rem(own + k * group, planes * group), core))
    pl.semaphore_wait(barrier, group + planes - 1)

    def send_near(j, d):
        to = flipped(place, d)
        remote(
            weights[j].at[:, pl.ds(pl.multiple_of(to * ch, 128), ch)],
            w.at[own_rows, pl.ds(j * ch, ch)],
            near_send.at[j // 4, d - 1], near_recv.at[j // 4, d - 1], (chips[d], core),
        ).start()

    def near_block(kind, d):
        start = pl.multiple_of((base + flipped(place, d)) * rows_in, 128)
        block = w.at[pl.ds(start, rows_in), class_cols(kind)]
        return remote(
            block, block, near_send.at[kind, d - 1], near_recv.at[kind, d - 1], (chips[d], core)
        )

    for d in range(1, group):
        for j in range(4):
            send_near(j, d)

    rate_rows = 2 * heads
    kept[1].wait()
    rate_moves = []
    for d in range(group):
        to = flipped(place, d)
        for way in range(2):
            for h in range(heads):
                rate_pack[d, pl.ds(way * heads + h, 1), :] = rate_own[
                    way, pl.ds(heads * to + h, 1), :
                ]
        rate_pack[d, pl.ds(rate_rows, 8 - rate_rows), :] = jnp.zeros((8 - rate_rows, length), f32)
    for d in range(1, group):
        rate_moves.append(
            remote(
                rate_pack.at[d], rates.at[place], rate_send.at[0], rate_recv.at[d - 1],
                (chips[d], core),
            )
        )
    for copy in rate_moves:
        copy.start()
    for d in range(1, group):
        for j in range(4, 7):
            send_near(j, d)

    def far(kind, direction, q, d):
        if kind == CLASS_OUT:
            block = wo.at[:, pl.ds(pl.multiple_of((q * group + place) * out_cols, 128), out_cols)]
        else:
            start = pl.multiple_of((q * group + flipped(place, d)) * rows_in, 128)
            block = w.at[pl.ds(start, rows_in), class_cols(kind)]
        landed = out_recv.at[q] if kind == CLASS_OUT else far_recv.at[kind, q, d]
        target = own + group if direction == 0 else own - group
        return remote(block, block, far_send.at[kind, direction, q], landed, (target, core))

    def far_sent(kind, direction, q):
        if kind == CLASS_OUT:
            far(kind, direction, q, 0).wait_send()
        else:
            block = w.at[
                pl.ds(pl.multiple_of(q * group * rows_in, 128), group * rows_in), class_cols(kind)
            ]
            remote(
                block, block, far_send.at[kind, direction, q], far_recv.at[kind, q, 0],
                (own + group, core),
            ).wait_send()

    def places_of(kind):
        return 1 if kind == CLASS_OUT else group

    def own_far(kind, d):
        pl.when(has_up)(lambda: far(kind, 0, plane, d).start())
        pl.when(has_down)(lambda: far(kind, 1, plane, d).start())

    def source_plane(r):
        if r == 0:
            return plane
        if r == 1:
            return plane + 1 - 2 * lax.rem(plane, 2)
        return r + top * (planes - 1 - 2 * r)

    def arrive(kind, r, only=None, blocks=None):
        q = source_plane(r)

        def take():
            for d in range(places_of(kind)) if blocks is None else blocks:
                far(kind, 0, q, d).wait_recv()
                pl.when(jnp.logical_and(q < plane, has_up))(
                    lambda d=d: far(kind, 0, q, d).start()
                )
                pl.when(jnp.logical_and(q > plane, has_down))(
                    lambda d=d: far(kind, 1, q, d).start()
                )

        if only is None:
            take()
        else:
            pl.when(only)(take)

    ends = jnp.logical_not(middle)

    tile = length // 4
    kept[0].wait()
    own_here(CLASS_A)
    own_far(CLASS_A, 0)
    own_here(CLASS_OUT)
    own_far(CLASS_OUT, 0)

    @pl.loop(0, 4)
    def _(t):
        rows = pl.ds(pl.multiple_of(t * tile, tile), tile)
        value = xin[rows, :].astype(f32)
        value = value * value
        total = value[:, :128]
        for c in range(1, half // 128):
            total = total + value[:, c * 128 : (c + 1) * 128]
        ssq_out[rows, :] = total

    ssq_move = remote(ssq_out, ssq_in, ssq_sem.at[0], ssq_sem.at[1], partner)
    ssq_move.start()
    ssq_move.wait_recv()
    small[0].wait()
    own_half = pl.multiple_of(core * half, 128)

    @pl.loop(0, 4)
    def _(t):
        rows = pl.ds(pl.multiple_of(t * tile, tile), tile)
        total = jnp.sum(ssq_out[rows, :] + ssq_in[rows, :], axis=-1, keepdims=True)
        scale = lax.rsqrt(total / width + EPS)
        value = xin[rows, :].astype(f32) * scale * gain_ref[:, pl.ds(own_half, half)]
        x[pl.ds(pl.multiple_of(place * length + t * tile, tile), tile), pl.ds(own_half, half)] = (
            value.astype(bf16)
        )

    def span_rows(s):
        return pl.ds(pl.multiple_of(s * length, 128), length)

    def piece(d, which):
        return x.at[
            span_rows(flipped(place, d)),
            pl.ds(pl.multiple_of(core * half + which * quarter, 128), quarter),
        ]

    tokens = {}

    def send_piece(which, d_from, hop):
        d_there = d_from + hop
        tokens[(which, d_there)] = remote(
            piece(d_from, which), piece(d_from, which),
            tok_send.at[0], tok_recv.at[which, d_there - 1], (chips[hop], core),
        )
        tokens[(which, d_there)].start()

    def send_half(d):
        block = x.at[span_rows(flipped(place, d)), pl.ds(own_half, half)]
        remote(block, block, half_send.at[0], half_recv.at[d], partner).start()

    send_piece(0, 0, 1)
    send_piece(1, 0, 2)
    send_piece(1, 0, 1)
    send_piece(0, 0, 2)
    send_half(0)

    for d in range(1, group):
        near_block(CLASS_A, d).wait_recv()
        own_far(CLASS_A, d)

    for copy in small[1:]:
        copy.wait()
    for copy in rate_moves:
        copy.wait_recv()
    rates[place] = rate_pack[0]
    for s in range(group):
        cums[s * 8 : s * 8 + 8, :] = rates[s]
    lanes = lax.broadcasted_iota(jnp.int32, (group * 8, length), 1)
    kinds = lax.rem(lax.broadcasted_iota(jnp.int32, (group * 8, length), 0), 8)
    running = cums[...] * LOG2E
    step = 1
    while step < length:
        ahead = jnp.where(lanes >= step, pltpu.roll(running, step, 1), 0.0)
        behind = jnp.where(lanes < length - step, pltpu.roll(running, length - step, 1), 0.0)
        running = running + jnp.where(kinds < heads, ahead, behind)
        step *= 2
    cums[...] = running
    wide[...] = jnp.zeros_like(wide)
    first_head = lax.broadcasted_iota(jnp.int32, (length, ch), 1) < HEAD_DIM
    lane_in_head = lax.rem(lax.broadcasted_iota(jnp.int32, (length, ch), 1), HEAD_DIM)
    leading = lane_in_head < HEAD_DIM // 2

    @pl.loop(0, group)
    def _(s):
        sums = cums[pl.ds(pl.multiple_of(s * 8, 8), 8), :]
        wide[0:8, :] = sums
        columns = wide[...].T
        cf = [columns[:, h : h + 1] for h in range(heads)]
        rb = [columns[:, heads + h : heads + h + 1] for h in range(heads)]
        cf_wide = jnp.where(first_head, cf[0], cf[1])
        rb_wide = jnp.where(first_head, rb[0], rb[1])
        ef[s] = jnp.exp2(cf_wide)
        eb[s] = jnp.exp2(rb_wide)
        kf[s] = jnp.exp2(cf_wide[length - 1 : length, :] - cf_wide)
        kb[s] = jnp.exp2(rb_wide[0:1, :] - rb_wide)
        row_at = lax.broadcasted_iota(jnp.int32, (length, length), 0)
        col_at = lax.broadcasted_iota(jnp.int32, (length, length), 1)
        for h in range(heads):
            spread = jnp.where(
                col_at <= row_at, cf[h] - sums[h : h + 1, :], rb[h] - sums[heads + h : heads + h + 1, :]
            )
            decay[s, h] = jnp.exp2(spread)
        turn = base_ref[s]
        cos_0, sin_0 = turn[0:1, :], turn[1:2, :]
        cos_i, sin_i = turn_ref[0], turn_ref[1]
        cosines[s] = cos_0 * cos_i - sin_0 * sin_i
        angle_sine = sin_0 * cos_i + cos_0 * sin_i
        sines[s] = jnp.where(leading, -angle_sine, angle_sine)

    def out_piece(r, d, which):
        start = pl.multiple_of((source_plane(r) * group + flipped(place, d)) * out_cols, 128)
        return wo.at[pl.ds(which * side_rows, side_rows), pl.ds(start, out_cols)]

    def out_move(r, which, d_there, hop):
        block = out_piece(r, d_there - hop, which)
        return remote(
            block, block, wo_send.at[0], wo_recv.at[r, which, d_there - 1],
            (chips[hop], core),
        )

    def out_landed(r, which, d):
        block = out_piece(r, d, which)
        remote(
            block, block, wo_send.at[0], wo_recv.at[r, which, d - 1], (chips[1], core)
        ).wait_recv()

    def spread_out(r):
        for which, hop in ((0, 1), (1, 2), (1, 1), (0, 2)):
            out_move(r, which, hop, hop).start()

    def relay_out(r):
        out_landed(r, 0, 1)
        out_move(r, 0, 3, 2).start()
        out_landed(r, 1, 2)
        out_move(r, 1, 3, 1).start()

    def finish_out(r):
        for which, d in ((1, 1), (0, 2), (0, 3), (1, 3)):
            out_landed(r, which, d)

    def wait_half(d):
        block = x.at[
            span_rows(flipped(place, d)), pl.ds(pl.multiple_of((1 - core) * half, 128), half)
        ]
        remote(block, block, half_send.at[0], half_recv.at[d], partner).wait_recv()

    for d in range(group):
        arrive(CLASS_A, 1, middle, (d,))
        arrive(CLASS_A, 2, middle, (d,))
    arrive(CLASS_OUT, 1, middle)
    for d in range(1, group):
        near_block(CLASS_B, d).wait_recv()
    own_here(CLASS_B)

    @pl.when(ends)
    def _():
        for d in range(group):
            own_far(CLASS_B, d)

    tokens[(0, 1)].wait_recv()
    send_piece(0, 1, 2)
    tokens[(1, 2)].wait_recv()
    send_piece(1, 2, 1)
    spread_out(0)
    arrive(CLASS_OUT, 1, ends)
    spread_out(1)
    arrive(CLASS_A, 3, middle)
    arrive(CLASS_OUT, 2, middle)

    @pl.when(middle)
    def _():
        for d in range(group):
            own_far(CLASS_B, d)

    tokens[(1, 1)].wait_recv()
    send_half(1)
    tokens[(0, 2)].wait_recv()
    send_half(2)
    for r in range(1, planes):
        arrive(CLASS_A, r, ends)
    arrive(CLASS_OUT, 3, middle)
    arrive(CLASS_B, 1, middle)
    wait_half(0)

    same_head = (
        lax.div(lax.broadcasted_iota(jnp.int32, (ch, ch), 0), HEAD_DIM)
        == lax.div(lax.broadcasted_iota(jnp.int32, (ch, ch), 1), HEAD_DIM)
    )

    def one_span(s):
        rows = span_rows(s)
        held = jnp.dot(x[rows, :], w[:, 0:col_a], preferred_element_type=f32)
        cosine, sine = cosines[s], sines[s]

        def turned(value):
            value = value.astype(bf16).astype(f32)
            other = jnp.where(
                leading,
                pltpu.roll(value, ch - HEAD_DIM // 2, 1),
                pltpu.roll(value, HEAD_DIM // 2, 1),
            )
            return value * cosine + other * sine

        rk = (turned(held[:, 0:ch]) * HEAD_DIM ** (-0.5)).astype(bf16).astype(f32)
        rq = turned(held[:, ch : 2 * ch]).astype(bf16)
        value = held[:, 2 * ch : 3 * ch].astype(bf16)
        rq_buf[s] = rq
        v_buf[s] = value
        gate_buf[s] = held[:, 3 * ch : 4 * ch].astype(bf16)
        value_wide = value.astype(f32)
        found = None
        for h in range(heads):
            in_head = first_head if h == 0 else jnp.logical_not(first_head)
            key_head = jnp.where(in_head, rk, 0.0).astype(bf16)
            value_head = jnp.where(in_head, value_wide, 0.0).astype(bf16)
            scores = lax.dot_general(
                rq, key_head, (((1,), (1,)), ((), ())), preferred_element_type=f32
            )
            probs = (scores * decay[s, h]).astype(bf16)
            part = jnp.dot(probs, value_head, preferred_element_type=f32)
            found = part if found is None else found + part
        loc[s] = found
        for table, target in ((kf, state_f), (kb, state_b)):
            keys = (rk * table[s]).astype(bf16)
            state = lax.dot_general(
                keys, value, (((0,), (0,)), ((), ())), preferred_element_type=f32
            )
            target[s] = jnp.where(same_head, state, 0.0)

    halo_rows = 16
    halos = [
        remote(
            x.at[pl.ds(all_rows - halo_rows, halo_rows), :], x.at[pl.ds(all_rows, halo_rows), :],
            halo_send.at[0], halo_recv.at[0], (own + group, core),
        ),
        remote(
            x.at[pl.ds(0, halo_rows), :], x.at[pl.ds(all_rows + halo_rows, halo_rows), :],
            halo_send.at[1], halo_recv.at[1], (own - group, core),
        ),
    ]
    blank = jnp.zeros((halo_rows, width), bf16)

    @pl.when(jnp.logical_not(has_down))
    def _():
        x[pl.ds(all_rows, halo_rows), :] = blank

    @pl.when(jnp.logical_not(has_up))
    def _():
        x[pl.ds(all_rows + halo_rows, halo_rows), :] = blank

    @pl.loop(0, group)
    def _(d):
        @pl.when(d == 1)
        def _():
            tokens[(0, 3)].wait_recv()
            tokens[(1, 3)].wait_recv()
            send_half(3)
            wait_half(1)

        @pl.when(d == 2)
        def _():
            wait_half(2)

        @pl.when(d == 3)
        def _():
            wait_half(3)
            pl.when(has_up)(lambda: halos[0].start())
            pl.when(has_down)(lambda: halos[1].start())
            relay_out(0)
            arrive(CLASS_OUT, 2, ends)
            spread_out(2)

        one_span(lax.rem(lax.rem(place, 2) + lax.rem(d, 2), 2)
                 + 2 * lax.rem(lax.div(place, 2) + lax.div(d, 2), 2))

    def scan_states(state, table, at, order, target):
        passed, inside, reach = jnp.zeros((ch, ch), f32), {}, {}
        over = jnp.ones((1, ch), f32)
        for s in order:
            inside[s], reach[s] = passed, over
            factor = table[s, at : at + 1, :]
            passed = factor * passed + state[s]
            over = over * factor
        folded = passed[0:HEAD_DIM, :]
        for h in range(1, heads):
            folded = folded + passed[h * HEAD_DIM : (h + 1) * HEAD_DIM, :]
        pack_out[target, 0:HEAD_DIM, :] = folded
        pack_out[target, HEAD_DIM : HEAD_DIM + 8, :] = jnp.broadcast_to(over, (8, ch))
        return inside, reach

    ahead_in, ahead_reach = scan_states(state_f, ef, length - 1, range(group), 0)
    back_in, back_reach = scan_states(state_b, eb, 0, range(group)[::-1], 1)

    def pack_move(way, k):
        to = own + k * group if way == 0 else own - k * group
        return remote(
            pack_out.at[way], pack_in.at[way, k - 1],
            pack_send.at[way, k - 1], pack_recv.at[way, k - 1], (to, core),
        )

    def gives(way, k):
        return plane + k < planes if way == 0 else plane - k >= 0

    def takes(way, k):
        return gives(1 - way, k)

    for k in range(1, planes):
        for way in range(2):
            pl.when(gives(way, k))(lambda way=way, k=k: pack_move(way, k).start())
    arrive(CLASS_B, 2, middle)
    arrive(CLASS_B, 3, middle)

    def feature_cols(kind):
        return pl.ds(pl.multiple_of(kind * side_rows + place * ch, 128), ch)

    def feature_move(kind, d, s, to):
        return remote(
            parts.at[kind, s], feat.at[:, feature_cols(kind)],
            ft_send.at[0], ft_recv.at[kind, d - 1], (to, core),
        )

    relay_out(1)
    arrive(CLASS_OUT, 3, ends)
    spread_out(3)
    incoming = []
    for way in range(2):
        into[way] = jnp.zeros((HEAD_DIM, ch), f32)
        into[way + 2] = jnp.ones((HEAD_DIM, ch), f32)
        for k in range(1, planes):
            @pl.when(takes(way, k))
            def _(way=way, k=k):
                pack_move(way, k).wait_recv()
                into[way] = into[way] + into[way + 2] * pack_in[way, k - 1, 0:HEAD_DIM, :]
                into[way + 2] = into[way + 2] * pack_in[
                    way, k - 1, HEAD_DIM : HEAD_DIM + 1, :
                ]
        incoming.append(
            jnp.where(same_head, jnp.concatenate([into[way]] * heads, axis=0), 0.0)
        )
    for s in range(group):
        state_f[s] = ahead_in[s] + ahead_reach[s] * incoming[0]
        state_b[s] = back_in[s] + back_reach[s] * incoming[1]

    @pl.loop(0, group)
    def _(i):
        d = group - 1 - i
        s = (lax.rem(lax.rem(place, 2) + lax.rem(d, 2), 2)
             + 2 * lax.rem(lax.div(place, 2) + lax.div(d, 2), 2))
        query = rq_buf[s]
        mix = (
            loc[s]
            + ef[s] * jnp.dot(query, state_f[s].astype(bf16), preferred_element_type=f32)
            + eb[s] * jnp.dot(query, state_b[s].astype(bf16), preferred_element_type=f32)
        )
        squares = mix * mix
        first = jnp.sum(jnp.where(first_head, squares, 0.0), axis=-1, keepdims=True)
        second = jnp.sum(jnp.where(first_head, 0.0, squares), axis=-1, keepdims=True)
        scale = lax.rsqrt(jnp.where(first_head, first, second) / HEAD_DIM + EPS)
        gate = gate_buf[s].astype(f32)
        parts[1, s] = (
            gate / (1.0 + jnp.exp(-gate)) * (mix * scale * head_gain_ref[:, place_cols])
        ).astype(bf16)

        @pl.when(d > 0)
        def _():
            feature_move(1, d, s, base + s).start()

    feat[:, feature_cols(1)] = parts[1, place]

    relay_out(2)
    arrive(CLASS_B, 1, ends)
    arrive(CLASS_B, 2, ends)
    pl.when(has_down)(lambda: halos[0].wait_recv())
    pl.when(has_up)(lambda: halos[1].wait_recv())
    depth = group * rows_in
    most = (planes - 1) * depth
    early = pl.multiple_of(top * depth, 128)
    late = pl.multiple_of((1 - top) * most, 128)
    blocks = 5
    block = (all_rows + 2 * halo_rows) // blocks

    @pl.loop(0, blocks)
    def _(t):
        rows = pl.ds(pl.multiple_of(t * block, 16), block)
        acc[rows, :] = jnp.dot(
            x[rows, pl.ds(early, most)], w[pl.ds(early, most), col_a : col_a + col_b],
            preferred_element_type=f32,
        )

    relay_out(3)
    arrive(CLASS_B, 3, ends)

    @pl.loop(0, blocks)
    def _(t):
        rows = pl.ds(pl.multiple_of(t * block, 16), block)
        held = acc[rows, :] + jnp.dot(
            x[rows, pl.ds(late, depth)], w[pl.ds(late, depth), col_a : col_a + col_b],
            preferred_element_type=f32,
        )
        held = held.astype(bf16).astype(f32)
        iv[pl.ds(pl.multiple_of(t * block + 8, 8), block), :] = (
            (held[:, 0:ch] * held[:, ch : 2 * ch]).astype(bf16).astype(f32)
        )
        acc[rows, 2 * ch : 3 * ch] = held[:, 2 * ch : 3 * ch]

    iv[7:8, :] = iv[all_rows + halo_rows + 7 : all_rows + halo_rows + 8, :]
    iv[all_rows + 8 : all_rows + 9, :] = iv[all_rows + halo_rows + 8 : all_rows + halo_rows + 9, :]
    own_taps = taps_ref[:, place_cols]
    for s in range(group):
        at = s * length
        near_sum = (
            own_taps[0:1, :] * iv[at + 7 : at + 7 + length, :]
            + own_taps[1:2, :] * iv[at + 8 : at + 8 + length, :]
            + own_taps[2:3, :] * iv[at + 9 : at + 9 + length, :]
        )
        parts[0, s] = (acc[at : at + length, 2 * ch : 3 * ch] * near_sum).astype(bf16)

    for d in (3, 1, 2):
        feature_move(0, d, flipped(place, d), chips[d]).start()
    feat[:, feature_cols(0)] = parts[0, place]

    my_rows = length // 2

    def part_at(r):
        return pl.ds(pl.multiple_of(source_plane(r) * part_cols, 128), part_cols)

    def features_here(kind):
        for d in range(1, group):
            feature_move(kind, d, flipped(place, d), chips[d]).wait_recv()

    def row_half(c):
        return pl.ds(pl.multiple_of(c * my_rows, 128), my_rows)

    def share_move(r):
        return remote(
            share.at[:, part_at(r)], theirs.at[:, part_at(r)],
            share_send.at[0], share_recv.at[r], partner,
        )

    def project(r):
        def rows_of(c):
            return (
                decay[r, 0, row_half(c), :]
                + jnp.dot(
                    feat[row_half(c), 0:side_rows], wo[0:side_rows, part_at(r)],
                    preferred_element_type=f32,
                )
            ).astype(bf16)

        share[:, part_at(r)] = rows_of(1 - core)
        share_move(r).start()
        out_ref[:, part_at(r)] = rows_of(core)

    def add_theirs(r):
        share_move(r).wait_recv()
        out_ref[:, part_at(r)] = (
            out_ref[:, part_at(r)].astype(f32) + theirs[:, part_at(r)].astype(f32)
        ).astype(bf16)

    features_here(1)
    for r in range(planes):
        finish_out(r)
        decay[r, 0] = jnp.dot(
            feat[:, side_rows:], wo[side_rows:, part_at(r)], preferred_element_type=f32
        )
    features_here(0)
    for r in range(planes):
        project(r)
    for r in range(planes):
        add_theirs(r)

    remote(share, theirs, share_send.at[0], share_recv.at[0], partner).wait_send()
    for kind in range(2):
        for d in range(1, group):
            near_block(kind, d).wait_send()
    for copy in rate_moves:
        copy.wait_send()
    ssq_move.wait_send()

    def sent(block, semaphore, landed):
        remote(block, block, semaphore, landed, partner).wait_send()

    sent(
        x.at[pl.ds(0, (group - 1) * length), pl.ds(0, 2 * quarter)], tok_send.at[0],
        tok_recv.at[0, 0],
    )
    sent(x.at[pl.ds(0, all_rows), pl.ds(0, half)], half_send.at[0], half_recv.at[0])
    sent(wo.at[:, pl.ds(0, (group - 1) * planes * out_cols)], wo_send.at[0], wo_recv.at[0, 0, 0])
    sent(parts.at[:, pl.ds(0, group - 1)], ft_send.at[0], ft_recv.at[0, 0])
    pl.when(has_up)(lambda: halos[0].wait_send())
    pl.when(has_down)(lambda: halos[1].wait_send())
    for k in range(1, planes):
        for way in range(2):
            pl.when(gives(way, k))(lambda way=way, k=k: pack_move(way, k).wait_send())
    for kind in range(3):
        for q in range(planes):
            pl.when(jnp.logical_and(q <= plane, has_up))(functools.partial(far_sent, kind, 0, q))
            pl.when(jnp.logical_and(q >= plane, has_down))(functools.partial(far_sent, kind, 1, q))


def turn_tables(spans, length, channels):
    half_dim = HEAD_DIM // 2
    frequency = THETA ** (-2.0 * (np.arange(channels) % half_dim) / HEAD_DIM)
    inner = np.arange(length)[:, None] * frequency
    outer = (np.arange(spans) * length)[:, None] * frequency
    turn = np.stack([np.cos(inner), np.sin(inner)])
    start = np.zeros((spans, 8, channels))
    start[:, 0], start[:, 1] = np.cos(outer), np.sin(outer)
    return turn.astype(np.float32), start.astype(np.float32)


def mixer(planes, group, arrays):
    (
        tokens, norm_gain, outer_gate, inner_gate, conv_input, query_proj, key_proj, value_proj,
        out_gate, conv_taps, log_decay, head_gain, conv_output, retention_output,
    ) = arrays
    f32, bf16 = jnp.float32, jnp.bfloat16
    length, half = tokens.shape
    width = 2 * half
    ch = outer_gate.shape[1] // group
    heads = ch // HEAD_DIM
    rows, side = group * length, conv_output.shape[0]
    turn, start = turn_tables(planes * group, length, ch)
    dma = pltpu.SemaphoreType.DMA
    vmem, held = pl.BlockSpec(memory_space=pltpu.VMEM), pl.BlockSpec(memory_space=pltpu.HBM)
    v = pltpu.VMEM
    result = jax.ShapeDtypeStruct((length // 2, width), bf16)
    table = v((group, length, ch), f32)
    return pl.pallas_call(
        functools.partial(mixer_kernel, planes, group),
        out_shape=result,
        in_specs=[held] * 16,
        out_specs=vmem,
        scratch_shapes=[
            v((1, width), f32), v(conv_taps.shape, f32), v((1, head_gain.shape[0]), f32), v(turn.shape, f32),
            v((group,) + start.shape[1:], f32),
            v((length, half), bf16), v((rows + 32, width), bf16), v((width, 7 * ch), bf16),
            v((2 * side, width), bf16), v(log_decay.shape, f32),
            v((group, 8, length), f32), v((group, 8, length), f32),
            v((8 * group, length), f32), v((128, length), f32),
            v((length, 128), f32), v((length, 128), f32),
            table, table, v((group, heads, length, length), f32),
            table, table, table, table,
            v((group, length, ch), bf16), v((group, length, ch), bf16), v((group, length, ch), bf16),
            table, v((group, ch, ch), f32), v((group, ch, ch), f32),
            v((2, HEAD_DIM + 8, ch), f32), v((2, planes - 1, HEAD_DIM + 8, ch), f32),
            v((4, HEAD_DIM, ch), f32),
            v((rows + 32, 3 * ch), f32), v((rows + 48, ch), f32),
            v((2, group, length, ch), bf16), v((length, 2 * side), bf16),
            v((length // 2, width), bf16), v((length // 2, width), bf16),
            dma((10,)), dma((2, group - 1)), dma((2, group - 1)), dma((1,)), dma((group - 1,)), dma((2,)),
            dma((1,)), dma((2, group - 1)), dma((1,)), dma((group,)),
            dma((3, 2, planes)), dma((2, planes, group)), dma((planes,)),
            dma((1,)), dma((planes, 2, group - 1)), dma((2,)), dma((2,)),
            dma((2, planes - 1)), dma((2, planes - 1)), dma((1,)), dma((2, group - 1)),
            dma((1,)), dma((planes,)),
        ],
        compiler_params=pltpu.CompilerParams(
            collective_id=0, has_side_effects=True, vmem_limit_bytes=50 * 2**20
        ),
    )(
        *(
            pltpu.with_memory_space_constraint(source, pltpu.HBM)
            for source in (
                tokens, key_proj, query_proj, value_proj, out_gate, inner_gate, conv_input,
                outer_gate, conv_output, retention_output, log_decay, norm_gain.reshape(1, -1),
                conv_taps, head_gain.reshape(1, -1), jnp.asarray(turn), jnp.asarray(start),
            )
        )
    )


LANES = 128

def plan(*arrays):
    spans, cores = lax.axis_size("sp"), lax.axis_size("tp")
    group = arrays[2].shape[1] // LANES
    planes = spans // group
    fits = (
        cores == 2
        and group == 4
        and planes * group == spans
        and planes == 2 * cores
        and arrays[0].shape[1] == 2 * group * arrays[2].shape[0]
    )
    return mixer(planes, group, arrays) if fits else local(*arrays)


def solution(mesh):
    return jax.shard_map(
        plan,
        mesh=mesh,
        in_specs=(
            P("sp", "tp"),
            P(),
            P("sp", "tp"),
            P("sp", "tp"),
            P("sp", "tp"),
            P("sp", "tp"),
            P("sp", "tp"),
            P("sp", "tp"),
            P("sp", "tp"),
            P(None, "tp"),
            P(None, "tp", "sp"),
            P("tp"),
            P("tp", "sp"),
            P("tp", "sp"),
        ),
        out_specs=P(("sp", "tp"), None),
        check_vma=False,
    )
```

```python
import jax
import functools
import jax.numpy as jnp
import numpy as np
from jax import lax
from jax.experimental import pallas as pl
from jax.experimental.pallas import tpu as pltpu
from jax.sharding import PartitionSpec as P

HEAD_DIM = 64


EPS = 1e-06
THETA = 10000.0


def with_halo(shard, sides, width):
    for axis, dim in sides:
        size, length = (lax.axis_size(axis), shard.shape[dim])
        up = [(i, (i + 1) % size) for i in range(size - 1)]
        down = [(j, i) for i, j in up]
        last = lax.slice_in_dim(shard, length - width, length, axis=dim)
        first = lax.slice_in_dim(shard, 0, width, axis=dim)
        before = lax.ppermute(last, axis, up)
        after = lax.ppermute(first, axis, down)
        shard = jnp.concatenate([before, shard, after], axis=dim)
    return shard


def rotate(field_in, position_list):
    half_dim = field_in.shape[-1] // 2
    frequency = jnp.exp(
        -jnp.log(THETA) * jnp.arange(half_dim, dtype=jnp.float32) * (2.0 / field_in.shape[-1])
    )
    angles = position_list.astype(jnp.float32)[:, None, None] * frequency
    cosine = jnp.cos(angles)
    sine_part = jnp.sin(angles)
    leading = field_in[..., :half_dim]
    trailing = field_in[..., half_dim:]
    return jnp.concatenate(
        [leading * cosine - trailing * sine_part, leading * sine_part + trailing * cosine], axis=-1
    )


def conv_branch(outer_rows, inner_rows, conv_values, conv_taps):
    inner_value = (inner_rows.astype(jnp.float32) * conv_values.astype(jnp.float32)).astype(
        jnp.bfloat16
    )
    padded = with_halo(inner_value, (("sp", 0),), 1).astype(jnp.float32)
    convolved = conv_taps[0] * padded[:-2] + conv_taps[1] * padded[1:-1] + conv_taps[2] * padded[2:]
    return (outer_rows.astype(jnp.float32) * convolved).astype(jnp.bfloat16)


def span_parts(query_rows, key_rows, value_rows, log_rates):
    length = query_rows.shape[0]
    forward_cum = jnp.cumsum(log_rates[0], axis=-1)
    backward_cum = jnp.flip(jnp.cumsum(jnp.flip(log_rates[1], -1), axis=-1), -1)
    row_index = lax.broadcasted_iota(jnp.int32, (length, length), 0)
    col_index = lax.broadcasted_iota(jnp.int32, (length, length), 1)
    lower_part = (col_index <= row_index)[None]
    spread = jnp.where(
        lower_part,
        forward_cum[:, :, None] - forward_cum[:, None, :],
        backward_cum[:, :, None] - backward_cum[:, None, :],
    )
    scores = jnp.einsum("ihe,jhe->hij", query_rows, key_rows, preferred_element_type=jnp.float32)
    weighted = (scores * jnp.exp(spread)).astype(jnp.bfloat16)
    local_part = jnp.einsum(
        "hij,jhe->ihe", weighted, value_rows, preferred_element_type=jnp.float32
    )
    key_wide = key_rows.astype(jnp.float32)
    forward_keys = (key_wide * jnp.exp(forward_cum[:, -1:] - forward_cum).T[:, :, None]).astype(
        jnp.bfloat16
    )
    backward_keys = (key_wide * jnp.exp(backward_cum[:, :1] - backward_cum).T[:, :, None]).astype(
        jnp.bfloat16
    )
    forward_state = jnp.einsum(
        "jhd,jhe->hde", forward_keys, value_rows, preferred_element_type=jnp.float32
    )
    backward_state = jnp.einsum(
        "jhd,jhe->hde", backward_keys, value_rows, preferred_element_type=jnp.float32
    )
    return (local_part, forward_cum, backward_cum, forward_state, backward_state)


def retention_branch(query_rows, key_rows, value_rows, gate_rows, log_decay, head_gain, offsets):
    row_count = query_rows.shape[0]
    head_count = query_rows.shape[1] // HEAD_DIM
    shape_heads = (row_count, head_count, HEAD_DIM)
    rotated_query = rotate(query_rows.astype(jnp.float32).reshape(shape_heads), offsets).astype(
        jnp.bfloat16
    )
    rotated_key = (
        rotate(key_rows.astype(jnp.float32).reshape(shape_heads), offsets) * HEAD_DIM ** (-0.5)
    ).astype(jnp.bfloat16)
    local_part, forward_cum, backward_cum, forward_state, backward_state = span_parts(
        rotated_query, rotated_key, value_rows.reshape(shape_heads), log_decay
    )
    forward_total = forward_cum[:, -1]
    backward_total = backward_cum[:, 0]
    totals = lax.all_gather(
        jnp.stack([forward_total, backward_total])[None], "sp", axis=0, tiled=True
    )
    inclusive = jnp.cumsum(totals, axis=0)
    exclusive = inclusive - totals
    own_index = lax.axis_index("sp")
    own_inclusive = lax.dynamic_index_in_dim(inclusive, own_index, 0, keepdims=False)
    own_exclusive = lax.dynamic_index_in_dim(exclusive, own_index, 0, keepdims=False)
    pieces = (
        lax.all_gather(forward_state[None], "sp", axis=0, tiled=True),
        lax.all_gather(backward_state[None], "sp", axis=0, tiled=True),
    )
    piece_count = pieces[0].shape[0]
    span_index = lax.iota(jnp.int32, piece_count)
    forward_weight = jnp.where(
        (span_index < own_index)[:, None],
        jnp.exp(jnp.minimum(own_exclusive[0] - inclusive[:, 0], 0.0)),
        0.0,
    )
    backward_weight = jnp.where(
        (span_index > own_index)[:, None],
        jnp.exp(jnp.minimum(exclusive[:, 1] - own_inclusive[1], 0.0)),
        0.0,
    )
    into_forward = jnp.einsum(
        "nh,nhde->hde", forward_weight, pieces[0], precision=lax.Precision.HIGHEST
    )
    into_backward = jnp.einsum(
        "nh,nhde->hde", backward_weight, pieces[1], precision=lax.Precision.HIGHEST
    )
    forward_part = jnp.einsum(
        "ihd,hde->ihe",
        rotated_query,
        into_forward.astype(jnp.bfloat16),
        preferred_element_type=jnp.float32,
    )
    backward_part = jnp.einsum(
        "ihd,hde->ihe",
        rotated_query,
        into_backward.astype(jnp.bfloat16),
        preferred_element_type=jnp.float32,
    )
    mixed_heads = (
        local_part
        + jnp.exp(forward_cum).T[:, :, None] * forward_part
        + jnp.exp(backward_cum).T[:, :, None] * backward_part
    )
    scaled = mixed_heads * lax.rsqrt(
        jnp.mean(mixed_heads * mixed_heads, axis=-1, keepdims=True) + EPS
    )
    scaled = scaled * head_gain.reshape(head_count, HEAD_DIM)
    return (
        jax.nn.silu(gate_rows.astype(jnp.float32))
        * scaled.reshape(row_count, head_count * HEAD_DIM)
    ).astype(jnp.bfloat16)


def local(
    tokens,
    norm_gain,
    outer_gate,
    inner_gate,
    conv_input,
    query_proj,
    key_proj,
    value_proj,
    out_gate,
    conv_taps,
    log_decay,
    head_gain,
    conv_output,
    retention_output,
):
    whole = lax.all_gather(tokens, "tp", axis=1, tiled=True)
    wide = whole.astype(jnp.float32)
    normed = (
        wide * lax.rsqrt(jnp.mean(wide * wide, axis=-1, keepdims=True) + EPS) * norm_gain
    ).astype(jnp.bfloat16)
    row_count = normed.shape[0]
    offsets = lax.axis_index("sp") * row_count + lax.iota(jnp.int32, row_count)
    gathered = (
        lax.all_gather(outer_gate, "sp", axis=0, tiled=True),
        lax.all_gather(inner_gate, "sp", axis=0, tiled=True),
        lax.all_gather(conv_input, "sp", axis=0, tiled=True),
        lax.all_gather(query_proj, "sp", axis=0, tiled=True),
        lax.all_gather(key_proj, "sp", axis=0, tiled=True),
        lax.all_gather(value_proj, "sp", axis=0, tiled=True),
        lax.all_gather(out_gate, "sp", axis=0, tiled=True),
        lax.all_gather(conv_output, "sp", axis=1, tiled=True),
        lax.all_gather(retention_output, "sp", axis=1, tiled=True),
    )
    projected = [
        jnp.dot(normed, weight, preferred_element_type=jnp.float32).astype(jnp.bfloat16)
        for weight in gathered[:7]
    ]
    conv_out = conv_branch(projected[0], projected[1], projected[2], conv_taps)
    ret_out = retention_branch(
        projected[3], projected[4], projected[5], projected[6], log_decay, head_gain, offsets
    )
    conv_weight = gathered[7]
    ret_weight = gathered[8]
    return lax.psum_scatter(
        (
            jnp.dot(conv_out, conv_weight, preferred_element_type=jnp.float32)
            + jnp.dot(ret_out, ret_weight, preferred_element_type=jnp.float32)
        ).astype(jnp.bfloat16),
        "tp",
        scatter_dimension=0,
        tiled=True,
    )


def flipped(place, d):
    if d == 0:
        return place
    if d == 1:
        return place + 1 - 2 * lax.rem(place, 2)
    if d == 2:
        return place + 2 - 4 * lax.rem(lax.div(place, 2), 2)
    return 3 - place


LOG2E = 1.4426950408889634
CLASS_A, CLASS_B, CLASS_OUT = 0, 1, 2


def mixer_kernel(
    planes, group,
    tok_ref, key_w, query_w, value_w, gate_w, inner_w, conv_w, outer_w,
    cout_ref, rout_ref, rate_in, gain_in, taps_in, head_gain_in, turn_in, base_in,
    out_ref, gain_ref, taps_ref, head_gain_ref, turn_ref, base_ref,
    xin, x, w, wo, rate_own, rate_pack, rates, cums, wide, ssq_out, ssq_in, cosines, sines, decay,
    ef, eb, kf, kb, rq_buf, v_buf, gate_buf, loc, state_f, state_b, pack_out, pack_in, into,
    acc, edges, parts, feat, share, theirs,
    own_sem, near_send, near_recv, rate_send, rate_recv, ssq_sem,
    tok_send, tok_recv, half_send, half_recv, far_send, far_recv, out_recv,
    wo_send, wo_recv, pair_sem, halo_send, halo_recv, pack_send, pack_recv,
    ft_send, ft_recv, share_send, share_recv,
):
    f32, bf16 = jnp.float32, jnp.bfloat16
    own, core = lax.axis_index("sp"), lax.axis_index("tp")
    place, plane = lax.rem(own, group), lax.div(own, group)
    base = plane * group
    length, half = tok_ref.shape
    width = 2 * half
    quarter = half // 2
    rows_in = key_w.shape[0]
    ch = key_w.shape[1] // group
    heads = ch // HEAD_DIM
    all_rows = group * length
    side_rows = cout_ref.shape[0]
    out_cols = cout_ref.shape[1]
    part_cols = group * out_cols
    col_a, col_b = 4 * ch, 3 * ch
    has_up, has_down = plane < planes - 1, plane > 0
    middle = jnp.logical_and(has_up, has_down)
    top = lax.div(plane, planes // 2)
    mesh_id = pl.DeviceIdType.MESH
    chips = [base + flipped(place, d) for d in range(group)]
    partner = (own, 1 - core)
    weights = (key_w, query_w, value_w, gate_w, inner_w, conv_w, outer_w)

    def local_copy(source, target, i):
        return pltpu.make_async_copy(source, target, own_sem.at[i])

    def remote(source, target, send, recv, device):
        return pltpu.make_async_remote_copy(
            src_ref=source, dst_ref=target, send_sem=send, recv_sem=recv,
            device_id=device, device_id_type=mesh_id,
        )

    own_rows = pl.ds(pl.multiple_of(own * rows_in, 128), rows_in)
    own_cols = pl.ds(pl.multiple_of(own * out_cols, 128), out_cols)
    kept = [local_copy(tok_ref, xin, 0), local_copy(rate_in, rate_own, 1)]
    for j, source in enumerate(weights):
        kept.append(
            local_copy(
                source.at[:, pl.ds(pl.multiple_of(place * ch, 128), ch)],
                w.at[own_rows, pl.ds(j * ch, ch)], 2 + j // 4,
            )
        )
    kept.append(local_copy(cout_ref, wo.at[pl.ds(0, side_rows), own_cols], 4))
    kept.append(local_copy(rout_ref, wo.at[pl.ds(side_rows, side_rows), own_cols], 4))
    place_cols = pl.ds(pl.multiple_of(place * ch, 128), ch)
    small = [
        local_copy(gain_in, gain_ref, 5),
        local_copy(taps_in, taps_ref, 6),
        local_copy(head_gain_in, head_gain_ref, 7),
        local_copy(turn_in, turn_ref, 8),
        local_copy(base_in.at[pl.ds(base, group)], base_ref, 9),
    ]
    for copy in kept + small:
        copy.start()

    def class_cols(kind):
        return pl.ds(0, col_a) if kind == CLASS_A else pl.ds(col_a, col_b)

    def own_here(kind):
        block = wo.at[:, own_cols] if kind == CLASS_OUT else w.at[own_rows, class_cols(kind)]
        local_copy(block, block, 2 + kind).wait()

    barrier = pltpu.get_barrier_semaphore()

    def greet(target):
        pl.semaphore_signal(barrier, inc=1, device_id=target, device_id_type=mesh_id)

    for d in range(1, group):
        greet((chips[d], core))
    greet(partner)
    for k in range(1, planes):
        greet((lax.rem(own + k * group, planes * group), core))
    pl.semaphore_wait(barrier, group + planes - 1)

    def send_near(j, d):
        to = flipped(place, d)
        remote(
            weights[j].at[:, pl.ds(pl.multiple_of(to * ch, 128), ch)],
            w.at[own_rows, pl.ds(j * ch, ch)],
            near_send.at[j // 4, d - 1], near_recv.at[j // 4, d - 1], (chips[d], core),
        ).start()

    def near_block(kind, d):
        start = pl.multiple_of((base + flipped(place, d)) * rows_in, 128)
        block = w.at[pl.ds(start, rows_in), class_cols(kind)]
        return remote(
            block, block, near_send.at[kind, d - 1], near_recv.at[kind, d - 1], (chips[d], core)
        )

    for d in range(1, group):
        for j in range(4):
            send_near(j, d)

    rate_rows = 2 * heads
    kept[1].wait()
    rate_moves = []
    for d in range(group):
        to = flipped(place, d)
        for way in range(2):
            for h in range(heads):
                row = rate_own[way, pl.ds(heads * to + h, 1), :]
                for part in range(2):
                    rate_pack[d, pl.ds(part * rate_rows + way * heads + h, 1), :] = row[
                        :, part * length // 2 : (part + 1) * length // 2
                    ]
    for d in range(1, group):
        rate_moves.append(
            remote(
                rate_pack.at[d], rates.at[place], rate_send.at[0], rate_recv.at[d - 1],
                (chips[d], core),
            )
        )
    for copy in rate_moves:
        copy.start()
    for d in range(1, group):
        for j in range(4, 7):
            send_near(j, d)

    def far(kind, direction, q, d):
        if kind == CLASS_OUT:
            block = wo.at[:, pl.ds(pl.multiple_of((q * group + place) * out_cols, 128), out_cols)]
        else:
            start = pl.multiple_of((q * group + flipped(place, d)) * rows_in, 128)
            block = w.at[pl.ds(start, rows_in), class_cols(kind)]
        landed = out_recv.at[q] if kind == CLASS_OUT else far_recv.at[kind, q, d]
        target = own + group if direction == 0 else own - group
        return remote(block, block, far_send.at[kind, direction, q], landed, (target, core))

    def far_sent(kind, direction, q):
        if kind == CLASS_OUT:
            far(kind, direction, q, 0).wait_send()
        else:
            block = w.at[
                pl.ds(pl.multiple_of(q * group * rows_in, 128), group * rows_in), class_cols(kind)
            ]
            remote(
                block, block, far_send.at[kind, direction, q], far_recv.at[kind, q, 0],
                (own + group, core),
            ).wait_send()

    def places_of(kind):
        return 1 if kind == CLASS_OUT else group

    def own_far(kind, d):
        pl.when(has_up)(lambda: far(kind, 0, plane, d).start())
        pl.when(has_down)(lambda: far(kind, 1, plane, d).start())

    def source_plane(r):
        if r == 0:
            return plane
        if r == 1:
            return plane + 1 - 2 * lax.rem(plane, 2)
        return r + top * (planes - 1 - 2 * r)

    def arrive(kind, r, only=None, blocks=None):
        q = source_plane(r)

        def take():
            for d in range(places_of(kind)) if blocks is None else blocks:
                far(kind, 0, q, d).wait_recv()
                pl.when(jnp.logical_and(q < plane, has_up))(
                    lambda d=d: far(kind, 0, q, d).start()
                )
                pl.when(jnp.logical_and(q > plane, has_down))(
                    lambda d=d: far(kind, 1, q, d).start()
                )

        if only is None:
            take()
        else:
            pl.when(only)(take)

    ends = jnp.logical_not(middle)

    tile = length // 4
    kept[0].wait()
    own_here(CLASS_A)
    own_far(CLASS_A, 0)
    own_here(CLASS_OUT)
    own_far(CLASS_OUT, 0)

    @pl.loop(0, 4)
    def _(t):
        rows = pl.ds(pl.multiple_of(t * tile, tile), tile)
        value = xin[rows, :].astype(f32)
        value = value * value
        total = value[:, :128]
        for c in range(1, half // 128):
            total = total + value[:, c * 128 : (c + 1) * 128]
        ssq_out[rows, :] = total

    ssq_move = remote(ssq_out, ssq_in, ssq_sem.at[0], ssq_sem.at[1], partner)
    ssq_move.start()
    ssq_move.wait_recv()
    small[0].wait()
    own_half = pl.multiple_of(core * half, 128)

    @pl.loop(0, 4)
    def _(t):
        rows = pl.ds(pl.multiple_of(t * tile, tile), tile)
        total = jnp.sum(ssq_out[rows, :] + ssq_in[rows, :], axis=-1, keepdims=True)
        scale = lax.rsqrt(total / width + EPS)
        value = xin[rows, :].astype(f32) * scale * gain_ref[:, pl.ds(own_half, half)]
        x[pl.ds(pl.multiple_of(place * length + t * tile, tile), tile), pl.ds(own_half, half)] = (
            value.astype(bf16)
        )

    def place_at(d):
        across = lax.rem(lax.rem(place, 2) + lax.rem(d, 2), 2)
        return across + 2 * lax.rem(lax.div(place, 2) + lax.div(d, 2), 2)

    def span_rows(s):
        return pl.ds(pl.multiple_of(s * length, 128), length)

    def piece(d, which):
        return x.at[
            span_rows(flipped(place, d)),
            pl.ds(pl.multiple_of(core * half + which * quarter, 128), quarter),
        ]

    tokens = {}

    def send_piece(which, d_from, hop):
        d_there = d_from + hop
        tokens[(which, d_there)] = remote(
            piece(d_from, which), piece(d_from, which),
            tok_send.at[0], tok_recv.at[which, d_there - 1], (chips[hop], core),
        )
        tokens[(which, d_there)].start()

    def send_half(d):
        block = x.at[span_rows(flipped(place, d)), pl.ds(own_half, half)]
        remote(block, block, half_send.at[0], half_recv.at[d], partner).start()

    send_piece(0, 0, 1)
    send_piece(1, 0, 2)
    send_piece(1, 0, 1)
    send_piece(0, 0, 2)
    send_half(0)

    for d in range(1, group):
        near_block(CLASS_A, d).wait_recv()
        own_far(CLASS_A, d)

    for copy in small[1:]:
        copy.wait()
    for copy in rate_moves:
        copy.wait_recv()
    rates[place] = rate_pack[0]
    for s in range(group):
        for part in range(2):
            cums[s * 8 : s * 8 + rate_rows, part * length // 2 : (part + 1) * length // 2] = rates[
                s, part * rate_rows : (part + 1) * rate_rows, :
            ]
        cums[s * 8 + rate_rows : s * 8 + 8, :] = jnp.zeros((8 - rate_rows, length), f32)
    lanes = lax.broadcasted_iota(jnp.int32, (group * 8, length), 1)
    kinds = lax.rem(lax.broadcasted_iota(jnp.int32, (group * 8, length), 0), 8)
    running = cums[...] * LOG2E
    step = 1
    while step < length:
        ahead = jnp.where(lanes >= step, pltpu.roll(running, step, 1), 0.0)
        behind = jnp.where(lanes < length - step, pltpu.roll(running, length - step, 1), 0.0)
        running = running + jnp.where(kinds < heads, ahead, behind)
        step *= 2
    cums[...] = running
    wide[...] = jnp.zeros_like(wide)
    first_head = lax.broadcasted_iota(jnp.int32, (length, ch), 1) < HEAD_DIM
    lane_in_head = lax.rem(lax.broadcasted_iota(jnp.int32, (length, ch), 1), HEAD_DIM)
    leading = lane_in_head < HEAD_DIM // 2

    @pl.loop(0, group)
    def _(s):
        sums = cums[pl.ds(pl.multiple_of(s * 8, 8), 8), :]
        wide[0:8, :] = sums
        columns = wide[...].T
        cf = [columns[:, h : h + 1] for h in range(heads)]
        rb = [columns[:, heads + h : heads + h + 1] for h in range(heads)]
        cf_wide = jnp.where(first_head, cf[0], cf[1])
        rb_wide = jnp.where(first_head, rb[0], rb[1])
        ef[s] = jnp.exp2(cf_wide)
        eb[s] = jnp.exp2(rb_wide)
        kf[s] = jnp.exp2(cf_wide[length - 1 : length, :] - cf_wide)
        kb[s] = jnp.exp2(rb_wide[0:1, :] - rb_wide)
        row_at = lax.broadcasted_iota(jnp.int32, (length, length), 0)
        col_at = lax.broadcasted_iota(jnp.int32, (length, length), 1)
        for h in range(heads):
            spread = jnp.where(
                col_at <= row_at, cf[h] - sums[h : h + 1, :], rb[h] - sums[heads + h : heads + h + 1, :]
            )
            decay[s, h] = jnp.exp2(spread)
        turn = base_ref[s]
        cos_0, sin_0 = turn[0:1, :], turn[1:2, :]
        cos_i, sin_i = turn_ref[0], turn_ref[1]
        cosines[s] = cos_0 * cos_i - sin_0 * sin_i
        angle_sine = sin_0 * cos_i + cos_0 * sin_i
        sines[s] = jnp.where(leading, -angle_sine, angle_sine)

    def out_piece(r, d, which):
        start = pl.multiple_of((source_plane(r) * group + flipped(place, d)) * out_cols, 128)
        return wo.at[pl.ds(which * side_rows, side_rows), pl.ds(start, out_cols)]

    def out_move(r, which, d_there, hop):
        block = out_piece(r, d_there - hop, which)
        return remote(
            block, block, wo_send.at[0], wo_recv.at[r, which, d_there - 1],
            (chips[hop], core),
        )

    def out_landed(r, which, d):
        block = out_piece(r, d, which)
        remote(
            block, block, wo_send.at[0], wo_recv.at[r, which, d - 1], (chips[1], core)
        ).wait_recv()

    def spread_out(r):
        for which, hop in ((0, 1), (1, 2), (1, 1), (0, 2)):
            out_move(r, which, hop, hop).start()

    def relay_out(r):
        out_landed(r, 0, 1)
        out_move(r, 0, 3, 2).start()
        out_landed(r, 1, 2)
        out_move(r, 1, 3, 1).start()

    def finish_out(r):
        for which, d in ((1, 1), (0, 2)) if r == 1 else ((1, 1), (0, 2), (0, 3), (1, 3)):
            out_landed(r, which, d)
        if r == 1:
            out_landed(r, 0, 1)
            out_landed(r, 1, 2)
            pair_block(source_plane(1)).wait_recv()

    def wait_half(d):
        block = x.at[
            span_rows(flipped(place, d)), pl.ds(pl.multiple_of((1 - core) * half, 128), half)
        ]
        remote(block, block, half_send.at[0], half_recv.at[d], partner).wait_recv()

    for d in range(group):
        arrive(CLASS_A, 1, middle, (d,))
        arrive(CLASS_A, 2, middle, (d,))
    arrive(CLASS_OUT, 1, middle)
    for d in range(1, group):
        near_block(CLASS_B, d).wait_recv()
    own_here(CLASS_B)

    @pl.when(ends)
    def _():
        for d in range(group):
            own_far(CLASS_B, d)

    tokens[(0, 1)].wait_recv()
    send_piece(0, 1, 2)
    tokens[(1, 2)].wait_recv()
    send_piece(1, 2, 1)
    spread_out(0)
    arrive(CLASS_OUT, 1, ends)
    spread_out(1)
    arrive(CLASS_A, 3, middle)
    arrive(CLASS_OUT, 2, middle)

    @pl.when(middle)
    def _():
        for d in range(group):
            own_far(CLASS_B, d)

    tokens[(1, 1)].wait_recv()
    send_half(1)
    tokens[(0, 2)].wait_recv()
    send_half(2)
    for r in range(1, planes):
        arrive(CLASS_A, r, ends)
    arrive(CLASS_OUT, 3, middle)
    arrive(CLASS_B, 1, middle)
    wait_half(0)

    same_head = (
        lax.div(lax.broadcasted_iota(jnp.int32, (ch, ch), 0), HEAD_DIM)
        == lax.div(lax.broadcasted_iota(jnp.int32, (ch, ch), 1), HEAD_DIM)
    )

    def one_span(s):
        rows = span_rows(s)
        held = jnp.dot(x[rows, :], w[:, 0:col_a], preferred_element_type=f32)
        cosine, sine = cosines[s], sines[s]

        def turned(value):
            value = value.astype(bf16).astype(f32)
            other = jnp.where(
                leading,
                pltpu.roll(value, ch - HEAD_DIM // 2, 1),
                pltpu.roll(value, HEAD_DIM // 2, 1),
            )
            return value * cosine + other * sine

        rk = (turned(held[:, 0:ch]) * HEAD_DIM ** (-0.5)).astype(bf16).astype(f32)
        rq = turned(held[:, ch : 2 * ch]).astype(bf16)
        value = held[:, 2 * ch : 3 * ch].astype(bf16)
        rq_buf[s] = rq
        v_buf[s] = value
        gate_buf[s] = held[:, 3 * ch : 4 * ch].astype(bf16)
        value_wide = value.astype(f32)
        found = None
        for h in range(heads):
            in_head = first_head if h == 0 else jnp.logical_not(first_head)
            key_head = jnp.where(in_head, rk, 0.0).astype(bf16)
            value_head = jnp.where(in_head, value_wide, 0.0).astype(bf16)
            scores = lax.dot_general(
                rq, key_head, (((1,), (1,)), ((), ())), preferred_element_type=f32
            )
            probs = (scores * decay[s, h]).astype(bf16)
            part = jnp.dot(probs, value_head, preferred_element_type=f32)
            found = part if found is None else found + part
        loc[s] = found
        for table, target in ((kf, state_f), (kb, state_b)):
            keys = (rk * table[s]).astype(bf16)
            state = lax.dot_general(
                keys, value, (((0,), (0,)), ((), ())), preferred_element_type=f32
            )
            target[s] = jnp.where(same_head, state, 0.0)

    halo_rows = 16
    halo_at = (all_rows, all_rows + halo_rows)

    def halo_move(way):
        cols = pl.ds(own_half, half)
        source = x.at[pl.ds((all_rows - halo_rows) * (1 - way), halo_rows), cols]
        return remote(
            source, x.at[pl.ds(halo_at[way], halo_rows), cols],
            halo_send.at[way], halo_recv.at[way], (own + group if way == 0 else own - group, core),
        )

    def halo_pass(way):
        block = x.at[pl.ds(halo_at[way], halo_rows), pl.ds(own_half, half)]
        return remote(block, block, halo_send.at[2 + way], halo_recv.at[2 + way], partner)

    def halo_comes(way):
        return has_down if way == 0 else has_up

    blank = jnp.zeros((halo_rows, width), bf16)

    @pl.when(jnp.logical_not(has_down))
    def _():
        x[pl.ds(all_rows, halo_rows), :] = blank

    @pl.when(jnp.logical_not(has_up))
    def _():
        x[pl.ds(all_rows + halo_rows, halo_rows), :] = blank

    @pl.loop(0, group)
    def _(d):
        @pl.when(d == 1)
        def _():
            tokens[(0, 3)].wait_recv()
            tokens[(1, 3)].wait_recv()
            send_half(3)
            wait_half(1)

        @pl.when(d == 2)
        def _():
            wait_half(2)

        @pl.when(d == 3)
        def _():
            wait_half(3)
            pl.when(has_up)(lambda: halo_move(0).start())
            pl.when(has_down)(lambda: halo_move(1).start())
            relay_out(0)
            arrive(CLASS_OUT, 2, ends)
            spread_out(2)

        one_span(place_at(d))

    def scan_states(state, table, at, order, target):
        passed, inside, reach = jnp.zeros((ch, ch), f32), {}, {}
        over = jnp.ones((1, ch), f32)
        for s in order:
            inside[s], reach[s] = passed, over
            factor = table[s, at : at + 1, :]
            passed = factor * passed + state[s]
            over = over * factor
        folded = passed[0:HEAD_DIM, :]
        for h in range(1, heads):
            folded = folded + passed[h * HEAD_DIM : (h + 1) * HEAD_DIM, :]
        pack_out[target, 0:HEAD_DIM, :] = folded
        pack_out[target, HEAD_DIM : HEAD_DIM + 8, :] = jnp.broadcast_to(over, (8, ch))
        return inside, reach

    ahead_in, ahead_reach = scan_states(state_f, ef, length - 1, range(group), 0)
    back_in, back_reach = scan_states(state_b, eb, 0, range(group)[::-1], 1)

    def pack_move(way, k):
        to = own + k * group if way == 0 else own - k * group
        return remote(
            pack_out.at[way], pack_in.at[way, k - 1],
            pack_send.at[way, k - 1], pack_recv.at[way, k - 1], (to, core),
        )

    def gives(way, k):
        return plane + k < planes if way == 0 else plane - k >= 0

    def takes(way, k):
        return gives(1 - way, k)

    for k in range(1, planes):
        for way in range(2):
            pl.when(gives(way, k))(lambda way=way, k=k: pack_move(way, k).start())
    arrive(CLASS_B, 2, middle)
    arrive(CLASS_B, 3, middle)

    def feature_cols(kind):
        return pl.ds(pl.multiple_of(kind * side_rows + place * ch, 128), ch)

    def feature_move(kind, d, s, to):
        return remote(
            parts.at[kind, s], feat.at[:, feature_cols(kind)],
            ft_send.at[0], ft_recv.at[kind, d - 1], (to, core),
        )

    finish_out(0)

    def pair_block(q):
        start = pl.multiple_of((q * group + flipped(place, 3)) * out_cols, 128)
        block = wo.at[:, pl.ds(start, out_cols)]
        return remote(
            block, block, pair_sem.at[0], pair_sem.at[1],
            ((plane + 1 - 2 * lax.rem(plane, 2)) * group + place, core),
        )

    pair_block(plane).start()
    arrive(CLASS_OUT, 3, ends)
    spread_out(3)
    incoming = []
    for way in range(2):
        into[way] = jnp.zeros((HEAD_DIM, ch), f32)
        into[way + 2] = jnp.ones((HEAD_DIM, ch), f32)
        for k in range(1, planes):
            @pl.when(takes(way, k))
            def _(way=way, k=k):
                pack_move(way, k).wait_recv()
                into[way] = into[way] + into[way + 2] * pack_in[way, k - 1, 0:HEAD_DIM, :]
                into[way + 2] = into[way + 2] * pack_in[
                    way, k - 1, HEAD_DIM : HEAD_DIM + 1, :
                ]
        incoming.append(
            jnp.where(same_head, jnp.concatenate([into[way]] * heads, axis=0), 0.0)
        )
    for s in range(group):
        state_f[s] = ahead_in[s] + ahead_reach[s] * incoming[0]
        state_b[s] = back_in[s] + back_reach[s] * incoming[1]

    @pl.loop(0, group)
    def _(i):
        d = group - 1 - i
        s = place_at(d)
        query = rq_buf[s]
        mix = (
            loc[s]
            + ef[s] * jnp.dot(query, state_f[s].astype(bf16), preferred_element_type=f32)
            + eb[s] * jnp.dot(query, state_b[s].astype(bf16), preferred_element_type=f32)
        )
        squares = mix * mix
        first = jnp.sum(jnp.where(first_head, squares, 0.0), axis=-1, keepdims=True)
        second = jnp.sum(jnp.where(first_head, 0.0, squares), axis=-1, keepdims=True)
        scale = lax.rsqrt(jnp.where(first_head, first, second) / HEAD_DIM + EPS)
        gate = gate_buf[s].astype(f32)
        parts[1, s] = (
            gate / (1.0 + jnp.exp(-gate)) * (mix * scale * head_gain_ref[:, place_cols])
        ).astype(bf16)

        @pl.when(d > 0)
        def _():
            feature_move(1, d, s, base + s).start()

    feat[:, feature_cols(1)] = parts[1, place]

    for way in range(2):
        @pl.when(halo_comes(way))
        def _(way=way):
            halo_move(way).wait_recv()
            halo_pass(way).start()
    relay_out(2)
    arrive(CLASS_B, 1, ends)
    arrive(CLASS_B, 2, ends)
    for way in range(2):
        pl.when(halo_comes(way))(lambda way=way: halo_pass(way).wait_recv())
    depth = group * rows_in
    most = (planes - 1) * depth
    early = pl.multiple_of(top * depth, 128)
    late = pl.multiple_of((1 - top) * most, 128)
    blocks = 5
    block = (all_rows + 2 * halo_rows) // blocks

    @pl.loop(0, blocks)
    def _(t):
        rows = pl.ds(pl.multiple_of(t * block, 16), block)
        acc[rows, :] = jnp.dot(
            x[rows, pl.ds(early, most)], w[pl.ds(early, most), col_a : col_a + col_b],
            preferred_element_type=f32,
        )

    relay_out(3)
    arrive(CLASS_B, 3, ends)

    spans_at = [s * length - halo_rows for s in range(1, group)] + [all_rows]
    late_w = w[pl.ds(late, depth), col_a : col_a + col_b]
    near_rows = jnp.concatenate(
        [x[at : at + 2 * halo_rows, pl.ds(late, depth)] for at in spans_at], axis=0
    )
    near_sums = jnp.concatenate(
        [acc[at : at + 2 * halo_rows, 0 : 2 * ch] for at in spans_at], axis=0
    )

    def inner_product(held):
        held = held.astype(bf16).astype(f32)
        return (held[:, 0:ch] * held[:, ch : 2 * ch]).astype(bf16).astype(f32)

    edge_values = inner_product(
        near_sums + jnp.dot(near_rows, late_w[:, 0 : 2 * ch], preferred_element_type=f32)
    )
    for s in range(group):
        before = ((s - 1) % group) * 2 * halo_rows + halo_rows - 1
        after = s * 2 * halo_rows + halo_rows
        edges[s, 0:1, :] = edge_values[before : before + 1, :]
        edges[s, 1:2, :] = edge_values[after : after + 1, :]
    row_of = lax.broadcasted_iota(jnp.int32, (length, ch), 0)

    @pl.loop(0, group)
    def _(i):
        turned_round = lax.div(i, 2)
        d = (1 - turned_round) * (1 + 2 * i) + turned_round * (6 - 2 * i)
        s = place_at(d)
        rows = span_rows(s)
        held = acc[rows, :] + jnp.dot(
            x[rows, pl.ds(late, depth)], w[pl.ds(late, depth), col_a : col_a + col_b],
            preferred_element_type=f32,
        )
        inner = inner_product(held)
        before = jnp.where(row_of == 0, edges[s, 0:1, :], pltpu.roll(inner, 1, 0))
        after = jnp.where(row_of == length - 1, edges[s, 1:2, :], pltpu.roll(inner, length - 1, 0))
        near_sum = (
            taps_ref[0:1, place_cols] * before
            + taps_ref[1:2, place_cols] * inner
            + taps_ref[2:3, place_cols] * after
        )
        parts[0, s] = (held[:, 2 * ch : 3 * ch].astype(bf16).astype(f32) * near_sum).astype(bf16)

        @pl.when(d > 0)
        def _():
            feature_move(0, d, s, base + s).start()

    feat[:, feature_cols(0)] = parts[0, place]

    my_rows = length // 2

    def part_at(r):
        return pl.ds(pl.multiple_of(source_plane(r) * part_cols, 128), part_cols)

    def features_here(kind, places=(1, 2, 3)):
        for d in places:
            feature_move(kind, d, flipped(place, d), chips[d]).wait_recv()

    def row_half(c):
        return pl.ds(pl.multiple_of(c * my_rows, 128), my_rows)

    def share_move(r):
        return remote(
            share.at[:, part_at(r)], theirs.at[:, part_at(r)],
            share_send.at[0], share_recv.at[r], partner,
        )

    pair_rows = 2 * ch
    own_pair = lax.div(place, 2)

    def conv_part(c, r, pair):
        at = pl.ds(pl.multiple_of(pair * pair_rows, 128), pair_rows)
        rows = pl.ds(0, length) if c is None else row_half(c)
        return jnp.dot(feat[rows, at], wo[at, part_at(r)], preferred_element_type=f32)

    def rows_of(c, r):
        return (decay[r, 0, row_half(c), :] + conv_part(c, r, 1 - own_pair)).astype(bf16)

    def add_theirs(r):
        share_move(r).wait_recv()
        out_ref[:, part_at(r)] = (
            out_ref[:, part_at(r)].astype(f32) + theirs[:, part_at(r)].astype(f32)
        ).astype(bf16)

    features_here(1)
    for r in range(planes):
        if r > 0:
            finish_out(r)
        decay[r, 0] = jnp.dot(
            feat[:, side_rows:], wo[side_rows:, part_at(r)], preferred_element_type=f32
        )
    for kind in range(2):
        for d in range(1, group):
            near_block(kind, d).wait_send()
    for copy in rate_moves:
        copy.wait_send()
    ssq_move.wait_send()

    def sent(block, semaphore, landed):
        remote(block, block, semaphore, landed, partner).wait_send()

    sent(
        x.at[pl.ds(0, (group - 1) * length), pl.ds(0, 2 * quarter)], tok_send.at[0],
        tok_recv.at[0, 0],
    )
    sent(x.at[pl.ds(0, all_rows), pl.ds(0, half)], half_send.at[0], half_recv.at[0])
    sent(wo.at[:, pl.ds(0, ((group - 1) * planes - 1) * out_cols)], wo_send.at[0], wo_recv.at[0, 0, 0])
    pair_block(plane).wait_send()
    pl.when(has_up)(lambda: halo_move(0).wait_send())
    pl.when(has_down)(lambda: halo_move(1).wait_send())
    for way in range(2):
        pl.when(halo_comes(way))(lambda way=way: halo_pass(way).wait_send())
    for k in range(1, planes):
        for way in range(2):
            pl.when(gives(way, k))(lambda way=way, k=k: pack_move(way, k).wait_send())
    for kind in range(3):
        for q in range(planes):
            pl.when(jnp.logical_and(q <= plane, has_up))(functools.partial(far_sent, kind, 0, q))
            pl.when(jnp.logical_and(q >= plane, has_down))(functools.partial(far_sent, kind, 1, q))

    features_here(0, (1,))
    for r in range(planes):
        decay[r, 0] = decay[r, 0] + conv_part(None, r, own_pair)
    features_here(0, (2, 3))
    for r in range(planes):
        share[:, part_at(r)] = rows_of(1 - core, r)
        share_move(r).start()
    for r in range(planes):
        out_ref[:, part_at(r)] = rows_of(core, r)
    for r in range(planes):
        add_theirs(r)
    remote(share, theirs, share_send.at[0], share_recv.at[0], partner).wait_send()
    sent(parts.at[:, pl.ds(0, group - 1)], ft_send.at[0], ft_recv.at[0, 0])


def turn_tables(spans, length, channels):
    half_dim = HEAD_DIM // 2
    frequency = THETA ** (-2.0 * (np.arange(channels) % half_dim) / HEAD_DIM)
    inner = np.arange(length)[:, None] * frequency
    outer = (np.arange(spans) * length)[:, None] * frequency
    turn = np.stack([np.cos(inner), np.sin(inner)])
    start = np.zeros((spans, 8, channels))
    start[:, 0], start[:, 1] = np.cos(outer), np.sin(outer)
    return turn.astype(np.float32), start.astype(np.float32)


def mixer(planes, group, arrays):
    (
        tokens, norm_gain, outer_gate, inner_gate, conv_input, query_proj, key_proj, value_proj,
        out_gate, conv_taps, log_decay, head_gain, conv_output, retention_output,
    ) = arrays
    f32, bf16 = jnp.float32, jnp.bfloat16
    length, half = tokens.shape
    width = 2 * half
    ch = outer_gate.shape[1] // group
    heads = ch // HEAD_DIM
    rows, side = group * length, conv_output.shape[0]
    turn, start = turn_tables(planes * group, length, ch)
    dma = pltpu.SemaphoreType.DMA
    vmem, held = pl.BlockSpec(memory_space=pltpu.VMEM), pl.BlockSpec(memory_space=pltpu.HBM)
    v = pltpu.VMEM
    result = jax.ShapeDtypeStruct((length // 2, width), bf16)
    table = v((group, length, ch), f32)
    return pl.pallas_call(
        functools.partial(mixer_kernel, planes, group),
        out_shape=result,
        in_specs=[held] * 16,
        out_specs=vmem,
        scratch_shapes=[
            v((1, width), f32), v(conv_taps.shape, f32), v((1, head_gain.shape[0]), f32), v(turn.shape, f32),
            v((group,) + start.shape[1:], f32),
            v((length, half), bf16), v((rows + 32, width), bf16), v((width, 7 * ch), bf16),
            v((2 * side, width), bf16), v(log_decay.shape, f32),
            v((group, 4 * heads, length // 2), f32), v((group, 4 * heads, length // 2), f32),
            v((8 * group, length), f32), v((128, length), f32),
            v((length, 128), f32), v((length, 128), f32),
            table, table, v((group, heads, length, length), f32),
            table, table, table, table,
            v((group, length, ch), bf16), v((group, length, ch), bf16), v((group, length, ch), bf16),
            table, v((group, ch, ch), f32), v((group, ch, ch), f32),
            v((2, HEAD_DIM + 8, ch), f32), v((2, planes - 1, HEAD_DIM + 8, ch), f32),
            v((4, HEAD_DIM, ch), f32),
            v((rows + 32, 3 * ch), f32), v((group, 8, ch), f32),
            v((2, group, length, ch), bf16), v((length, 2 * side), bf16),
            v((length // 2, width), bf16), v((length // 2, width), bf16),
            dma((10,)), dma((2, group - 1)), dma((2, group - 1)), dma((1,)), dma((group - 1,)), dma((2,)),
            dma((1,)), dma((2, group - 1)), dma((1,)), dma((group,)),
            dma((3, 2, planes)), dma((2, planes, group)), dma((planes,)),
            dma((1,)), dma((planes, 2, group - 1)), dma((2,)), dma((4,)), dma((4,)),
            dma((2, planes - 1)), dma((2, planes - 1)), dma((1,)), dma((2, group - 1)),
            dma((1,)), dma((planes,)),
        ],
        compiler_params=pltpu.CompilerParams(
            collective_id=0, has_side_effects=True, vmem_limit_bytes=50 * 2**20
        ),
    )(
        *(
            pltpu.with_memory_space_constraint(source, pltpu.HBM)
            for source in (
                tokens, key_proj, query_proj, value_proj, out_gate, inner_gate, conv_input,
                outer_gate, conv_output, retention_output, log_decay, norm_gain.reshape(1, -1),
                conv_taps, head_gain.reshape(1, -1), jnp.asarray(turn), jnp.asarray(start),
            )
        )
    )


LANES = 128

def plan(*arrays):
    spans, cores = lax.axis_size("sp"), lax.axis_size("tp")
    group = arrays[2].shape[1] // LANES
    planes = spans // group
    fits = (
        cores == 2
        and group == 4
        and planes * group == spans
        and planes == 2 * cores
        and arrays[0].shape[1] == 2 * group * arrays[2].shape[0]
    )
    return mixer(planes, group, arrays) if fits else local(*arrays)


def solution(mesh):
    return jax.shard_map(
        plan,
        mesh=mesh,
        in_specs=(
            P("sp", "tp"),
            P(),
            P("sp", "tp"),
            P("sp", "tp"),
            P("sp", "tp"),
            P("sp", "tp"),
            P("sp", "tp"),
            P("sp", "tp"),
            P("sp", "tp"),
            P(None, "tp"),
            P(None, "tp", "sp"),
            P("tp"),
            P("tp", "sp"),
            P("tp", "sp"),
        ),
        out_specs=P(("sp", "tp"), None),
        check_vma=False,
    )
```

```python
import jax
import functools
import jax.numpy as jnp
import numpy as np
from jax import lax
from jax.experimental import pallas as pl
from jax.experimental.pallas import tpu as pltpu
from jax.sharding import PartitionSpec as P

HEAD_DIM = 64


EPS = 1e-06
THETA = 10000.0


def with_halo(shard, sides, width):
    for axis, dim in sides:
        size, length = (lax.axis_size(axis), shard.shape[dim])
        up = [(i, (i + 1) % size) for i in range(size - 1)]
        down = [(j, i) for i, j in up]
        last = lax.slice_in_dim(shard, length - width, length, axis=dim)
        first = lax.slice_in_dim(shard, 0, width, axis=dim)
        before = lax.ppermute(last, axis, up)
        after = lax.ppermute(first, axis, down)
        shard = jnp.concatenate([before, shard, after], axis=dim)
    return shard


def rotate(field_in, position_list):
    half_dim = field_in.shape[-1] // 2
    frequency = jnp.exp(
        -jnp.log(THETA) * jnp.arange(half_dim, dtype=jnp.float32) * (2.0 / field_in.shape[-1])
    )
    angles = position_list.astype(jnp.float32)[:, None, None] * frequency
    cosine = jnp.cos(angles)
    sine_part = jnp.sin(angles)
    leading = field_in[..., :half_dim]
    trailing = field_in[..., half_dim:]
    return jnp.concatenate(
        [leading * cosine - trailing * sine_part, leading * sine_part + trailing * cosine], axis=-1
    )


def conv_branch(outer_rows, inner_rows, conv_values, conv_taps):
    inner_value = (inner_rows.astype(jnp.float32) * conv_values.astype(jnp.float32)).astype(
        jnp.bfloat16
    )
    padded = with_halo(inner_value, (("sp", 0),), 1).astype(jnp.float32)
    convolved = conv_taps[0] * padded[:-2] + conv_taps[1] * padded[1:-1] + conv_taps[2] * padded[2:]
    return (outer_rows.astype(jnp.float32) * convolved).astype(jnp.bfloat16)


def span_parts(query_rows, key_rows, value_rows, log_rates):
    length = query_rows.shape[0]
    forward_cum = jnp.cumsum(log_rates[0], axis=-1)
    backward_cum = jnp.flip(jnp.cumsum(jnp.flip(log_rates[1], -1), axis=-1), -1)
    row_index = lax.broadcasted_iota(jnp.int32, (length, length), 0)
    col_index = lax.broadcasted_iota(jnp.int32, (length, length), 1)
    lower_part = (col_index <= row_index)[None]
    spread = jnp.where(
        lower_part,
        forward_cum[:, :, None] - forward_cum[:, None, :],
        backward_cum[:, :, None] - backward_cum[:, None, :],
    )
    scores = jnp.einsum("ihe,jhe->hij", query_rows, key_rows, preferred_element_type=jnp.float32)
    weighted = (scores * jnp.exp(spread)).astype(jnp.bfloat16)
    local_part = jnp.einsum(
        "hij,jhe->ihe", weighted, value_rows, preferred_element_type=jnp.float32
    )
    key_wide = key_rows.astype(jnp.float32)
    forward_keys = (key_wide * jnp.exp(forward_cum[:, -1:] - forward_cum).T[:, :, None]).astype(
        jnp.bfloat16
    )
    backward_keys = (key_wide * jnp.exp(backward_cum[:, :1] - backward_cum).T[:, :, None]).astype(
        jnp.bfloat16
    )
    forward_state = jnp.einsum(
        "jhd,jhe->hde", forward_keys, value_rows, preferred_element_type=jnp.float32
    )
    backward_state = jnp.einsum(
        "jhd,jhe->hde", backward_keys, value_rows, preferred_element_type=jnp.float32
    )
    return (local_part, forward_cum, backward_cum, forward_state, backward_state)


def retention_branch(query_rows, key_rows, value_rows, gate_rows, log_decay, head_gain, offsets):
    row_count = query_rows.shape[0]
    head_count = query_rows.shape[1] // HEAD_DIM
    shape_heads = (row_count, head_count, HEAD_DIM)
    rotated_query = rotate(query_rows.astype(jnp.float32).reshape(shape_heads), offsets).astype(
        jnp.bfloat16
    )
    rotated_key = (
        rotate(key_rows.astype(jnp.float32).reshape(shape_heads), offsets) * HEAD_DIM ** (-0.5)
    ).astype(jnp.bfloat16)
    local_part, forward_cum, backward_cum, forward_state, backward_state = span_parts(
        rotated_query, rotated_key, value_rows.reshape(shape_heads), log_decay
    )
    forward_total = forward_cum[:, -1]
    backward_total = backward_cum[:, 0]
    totals = lax.all_gather(
        jnp.stack([forward_total, backward_total])[None], "sp", axis=0, tiled=True
    )
    inclusive = jnp.cumsum(totals, axis=0)
    exclusive = inclusive - totals
    own_index = lax.axis_index("sp")
    own_inclusive = lax.dynamic_index_in_dim(inclusive, own_index, 0, keepdims=False)
    own_exclusive = lax.dynamic_index_in_dim(exclusive, own_index, 0, keepdims=False)
    pieces = (
        lax.all_gather(forward_state[None], "sp", axis=0, tiled=True),
        lax.all_gather(backward_state[None], "sp", axis=0, tiled=True),
    )
    piece_count = pieces[0].shape[0]
    span_index = lax.iota(jnp.int32, piece_count)
    forward_weight = jnp.where(
        (span_index < own_index)[:, None],
        jnp.exp(jnp.minimum(own_exclusive[0] - inclusive[:, 0], 0.0)),
        0.0,
    )
    backward_weight = jnp.where(
        (span_index > own_index)[:, None],
        jnp.exp(jnp.minimum(exclusive[:, 1] - own_inclusive[1], 0.0)),
        0.0,
    )
    into_forward = jnp.einsum(
        "nh,nhde->hde", forward_weight, pieces[0], precision=lax.Precision.HIGHEST
    )
    into_backward = jnp.einsum(
        "nh,nhde->hde", backward_weight, pieces[1], precision=lax.Precision.HIGHEST
    )
    forward_part = jnp.einsum(
        "ihd,hde->ihe",
        rotated_query,
        into_forward.astype(jnp.bfloat16),
        preferred_element_type=jnp.float32,
    )
    backward_part = jnp.einsum(
        "ihd,hde->ihe",
        rotated_query,
        into_backward.astype(jnp.bfloat16),
        preferred_element_type=jnp.float32,
    )
    mixed_heads = (
        local_part
        + jnp.exp(forward_cum).T[:, :, None] * forward_part
        + jnp.exp(backward_cum).T[:, :, None] * backward_part
    )
    scaled = mixed_heads * lax.rsqrt(
        jnp.mean(mixed_heads * mixed_heads, axis=-1, keepdims=True) + EPS
    )
    scaled = scaled * head_gain.reshape(head_count, HEAD_DIM)
    return (
        jax.nn.silu(gate_rows.astype(jnp.float32))
        * scaled.reshape(row_count, head_count * HEAD_DIM)
    ).astype(jnp.bfloat16)


def local(
    tokens,
    norm_gain,
    outer_gate,
    inner_gate,
    conv_input,
    query_proj,
    key_proj,
    value_proj,
    out_gate,
    conv_taps,
    log_decay,
    head_gain,
    conv_output,
    retention_output,
):
    whole = lax.all_gather(tokens, "tp", axis=1, tiled=True)
    wide = whole.astype(jnp.float32)
    normed = (
        wide * lax.rsqrt(jnp.mean(wide * wide, axis=-1, keepdims=True) + EPS) * norm_gain
    ).astype(jnp.bfloat16)
    row_count = normed.shape[0]
    offsets = lax.axis_index("sp") * row_count + lax.iota(jnp.int32, row_count)
    gathered = (
        lax.all_gather(outer_gate, "sp", axis=0, tiled=True),
        lax.all_gather(inner_gate, "sp", axis=0, tiled=True),
        lax.all_gather(conv_input, "sp", axis=0, tiled=True),
        lax.all_gather(query_proj, "sp", axis=0, tiled=True),
        lax.all_gather(key_proj, "sp", axis=0, tiled=True),
        lax.all_gather(value_proj, "sp", axis=0, tiled=True),
        lax.all_gather(out_gate, "sp", axis=0, tiled=True),
        lax.all_gather(conv_output, "sp", axis=1, tiled=True),
        lax.all_gather(retention_output, "sp", axis=1, tiled=True),
    )
    projected = [
        jnp.dot(normed, weight, preferred_element_type=jnp.float32).astype(jnp.bfloat16)
        for weight in gathered[:7]
    ]
    conv_out = conv_branch(projected[0], projected[1], projected[2], conv_taps)
    ret_out = retention_branch(
        projected[3], projected[4], projected[5], projected[6], log_decay, head_gain, offsets
    )
    conv_weight = gathered[7]
    ret_weight = gathered[8]
    return lax.psum_scatter(
        (
            jnp.dot(conv_out, conv_weight, preferred_element_type=jnp.float32)
            + jnp.dot(ret_out, ret_weight, preferred_element_type=jnp.float32)
        ).astype(jnp.bfloat16),
        "tp",
        scatter_dimension=0,
        tiled=True,
    )


def flipped(place, d):
    if d == 0:
        return place
    if d == 1:
        return place + 1 - 2 * lax.rem(place, 2)
    if d == 2:
        return place + 2 - 4 * lax.rem(lax.div(place, 2), 2)
    return 3 - place


LOG2E = 1.4426950408889634
CLASS_A, CLASS_B, CLASS_OUT = 0, 1, 2


def mixer_kernel(
    planes, group,
    tok_ref, key_w, query_w, value_w, gate_w, inner_w, conv_w, outer_w,
    cout_ref, rout_ref, rate_in, gain_in, taps_in, head_gain_in, turn_in, base_in,
    out_ref, gain_ref, taps_ref, head_gain_ref, turn_ref, base_ref,
    xin, x, w, wo, rate_own, rate_pack, rates, cums, wide, ssq_out, ssq_in, cosines, sines, decay,
    ef, eb, kf, kb, rq_buf, v_buf, gate_buf, loc, state_f, state_b, pack_out, pack_in, into,
    acc, edges, parts, feat,
    own_sem, near_send, near_recv, rate_send, rate_recv, ssq_sem,
    tok_send, tok_recv, half_send, half_recv, far_send, far_recv, out_recv,
    wo_send, wo_recv, mate_send, mate_recv, pair_sem, halo_send, halo_recv, pack_send, pack_recv,
    ft_send, ft_recv,
):
    f32, bf16 = jnp.float32, jnp.bfloat16
    own, core = lax.axis_index("sp"), lax.axis_index("tp")
    place, plane = lax.rem(own, group), lax.div(own, group)
    base = plane * group
    length, half = tok_ref.shape
    width = 2 * half
    quarter = half // 2
    rows_in = key_w.shape[0]
    ch = key_w.shape[1] // group
    heads = ch // HEAD_DIM
    all_rows = group * length
    side_rows = cout_ref.shape[0]
    out_cols = cout_ref.shape[1]
    part_cols = group * out_cols
    col_a, col_b = 4 * ch, 3 * ch
    has_up, has_down = plane < planes - 1, plane > 0
    middle = jnp.logical_and(has_up, has_down)
    top = lax.div(plane, planes // 2)
    mesh_id = pl.DeviceIdType.MESH
    chips = [base + flipped(place, d) for d in range(group)]
    partner = (own, 1 - core)
    weights = (key_w, query_w, value_w, gate_w, inner_w, conv_w, outer_w)

    def local_copy(source, target, i):
        return pltpu.make_async_copy(source, target, own_sem.at[i])

    def remote(source, target, send, recv, device):
        return pltpu.make_async_remote_copy(
            src_ref=source, dst_ref=target, send_sem=send, recv_sem=recv,
            device_id=device, device_id_type=mesh_id,
        )

    own_rows = pl.ds(pl.multiple_of(own * rows_in, 128), rows_in)
    own_cols = pl.ds(pl.multiple_of(own * out_cols, 128), out_cols)
    kept = [local_copy(tok_ref, xin, 0), local_copy(rate_in, rate_own, 1)]
    for j, source in enumerate(weights):
        kept.append(
            local_copy(
                source.at[:, pl.ds(pl.multiple_of(place * ch, 128), ch)],
                w.at[own_rows, pl.ds(j * ch, ch)], 2 + j // 4,
            )
        )
    kept.append(local_copy(cout_ref, wo.at[core, pl.ds(0, side_rows), own_cols], 4))
    kept.append(local_copy(rout_ref, wo.at[core, pl.ds(side_rows, side_rows), own_cols], 4))
    place_cols = pl.ds(pl.multiple_of(place * ch, 128), ch)
    small = [
        local_copy(gain_in, gain_ref, 5),
        local_copy(taps_in, taps_ref, 6),
        local_copy(head_gain_in, head_gain_ref, 7),
        local_copy(turn_in, turn_ref, 8),
        local_copy(base_in.at[pl.ds(base, group)], base_ref, 9),
    ]
    for copy in kept + small:
        copy.start()

    def class_cols(kind):
        return pl.ds(0, col_a) if kind == CLASS_A else pl.ds(col_a, col_b)

    def own_here(kind):
        block = wo.at[core, :, own_cols] if kind == CLASS_OUT else w.at[own_rows, class_cols(kind)]
        local_copy(block, block, 2 + kind).wait()

    barrier = pltpu.get_barrier_semaphore()

    def greet(target):
        pl.semaphore_signal(barrier, inc=1, device_id=target, device_id_type=mesh_id)

    for d in range(1, group):
        for c in range(2):
            greet((chips[d], c))
    greet(partner)
    for k in range(1, planes):
        greet((lax.rem(own + k * group, planes * group), core))
    pl.semaphore_wait(barrier, 2 * group + planes - 2)

    def send_near(j, d):
        to = flipped(place, d)
        remote(
            weights[j].at[:, pl.ds(pl.multiple_of(to * ch, 128), ch)],
            w.at[own_rows, pl.ds(j * ch, ch)],
            near_send.at[0], near_recv.at[j // 4, d - 1], (chips[d], core),
        ).start()

    def near_block(kind, d):
        start = pl.multiple_of((base + flipped(place, d)) * rows_in, 128)
        block = w.at[pl.ds(start, rows_in), class_cols(kind)]
        return remote(
            block, block, near_send.at[0], near_recv.at[kind, d - 1], (chips[d], core)
        )

    for d in range(1, group):
        for j in range(4):
            send_near(j, d)

    rate_rows = 2 * heads
    kept[1].wait()
    rate_moves = []
    for d in range(group):
        to = flipped(place, d)
        for way in range(2):
            for h in range(heads):
                row = rate_own[way, pl.ds(heads * to + h, 1), :]
                for part in range(2):
                    rate_pack[d, pl.ds(part * rate_rows + way * heads + h, 1), :] = row[
                        :, part * length // 2 : (part + 1) * length // 2
                    ]
    for d in range(1, group):
        rate_moves.append(
            remote(
                rate_pack.at[d], rates.at[place], rate_send.at[0], rate_recv.at[d - 1],
                (chips[d], core),
            )
        )
    for copy in rate_moves:
        copy.start()
    for d in range(1, group):
        for j in range(4, 7):
            send_near(j, d)

    def far(kind, direction, q, d):
        if kind == CLASS_OUT:
            block = wo.at[
                core, :, pl.ds(pl.multiple_of((q * group + place) * out_cols, 128), out_cols)
            ]
        else:
            start = pl.multiple_of((q * group + flipped(place, d)) * rows_in, 128)
            block = w.at[pl.ds(start, rows_in), class_cols(kind)]
        to = plane + 1 - 2 * direction
        return remote(
            block, block, far_send.at[kind, direction], far_landed(kind, q, d, to),
            (own + group * (1 - 2 * direction), core),
        )

    def far_landed(kind, q, d, at):
        slot = q - (q > at).astype(jnp.int32)
        return out_recv.at[slot] if kind == CLASS_OUT else far_recv.at[kind, slot, d]

    def far_arrived(kind, q, d):
        if kind == CLASS_OUT:
            block = wo.at[
                core, :, pl.ds(pl.multiple_of((q * group + place) * out_cols, 128), out_cols)
            ]
        else:
            start = pl.multiple_of((q * group + flipped(place, d)) * rows_in, 128)
            block = w.at[pl.ds(start, rows_in), class_cols(kind)]
        remote(
            block, block, far_send.at[kind, 0], far_landed(kind, q, d, plane), partner
        ).wait_recv()

    def far_sent(kind, direction, units):
        if kind == CLASS_OUT:
            block, landed = wo.at[core, :, pl.ds(0, units * out_cols)], out_recv.at[0]
        else:
            block = w.at[pl.ds(0, units * group * rows_in), class_cols(kind)]
            landed = far_recv.at[kind, 0, 0]
        remote(block, block, far_send.at[kind, direction], landed, partner).wait_send()

    def places_of(kind):
        return 1 if kind == CLASS_OUT else group

    def own_far(kind, d):
        pl.when(has_up)(lambda: far(kind, 0, plane, d).start())
        pl.when(has_down)(lambda: far(kind, 1, plane, d).start())

    def source_plane(r):
        if r == 0:
            return plane
        if r == 1:
            return plane + 1 - 2 * lax.rem(plane, 2)
        return r + top * (planes - 1 - 2 * r)

    def arrive(kind, r, only=None, blocks=None):
        q = source_plane(r)

        def take():
            for d in range(places_of(kind)) if blocks is None else blocks:
                far_arrived(kind, q, d)
                pl.when(jnp.logical_and(q < plane, has_up))(
                    lambda d=d: far(kind, 0, q, d).start()
                )
                pl.when(jnp.logical_and(q > plane, has_down))(
                    lambda d=d: far(kind, 1, q, d).start()
                )

        if only is None:
            take()
        else:
            pl.when(only)(take)

    ends = jnp.logical_not(middle)

    tile = length // 4
    kept[0].wait()
    own_here(CLASS_A)
    own_far(CLASS_A, 0)
    own_here(CLASS_OUT)
    own_far(CLASS_OUT, 0)

    @pl.loop(0, 4)
    def _(t):
        rows = pl.ds(pl.multiple_of(t * tile, tile), tile)
        value = xin[rows, :].astype(f32)
        value = value * value
        total = value[:, :128]
        for c in range(1, half // 128):
            total = total + value[:, c * 128 : (c + 1) * 128]
        ssq_out[rows, :] = total

    ssq_move = remote(ssq_out, ssq_in, ssq_sem.at[0], ssq_sem.at[1], partner)
    ssq_move.start()
    ssq_move.wait_recv()
    small[0].wait()
    own_half = pl.multiple_of(core * half, 128)

    @pl.loop(0, 4)
    def _(t):
        rows = pl.ds(pl.multiple_of(t * tile, tile), tile)
        total = jnp.sum(ssq_out[rows, :] + ssq_in[rows, :], axis=-1, keepdims=True)
        scale = lax.rsqrt(total / width + EPS)
        value = xin[rows, :].astype(f32) * scale * gain_ref[:, pl.ds(own_half, half)]
        x[pl.ds(pl.multiple_of(place * length + t * tile, tile), tile), pl.ds(own_half, half)] = (
            value.astype(bf16)
        )

    def place_at(d):
        across = lax.rem(lax.rem(place, 2) + lax.rem(d, 2), 2)
        return across + 2 * lax.rem(lax.div(place, 2) + lax.div(d, 2), 2)

    def span_rows(s):
        return pl.ds(pl.multiple_of(s * length, 128), length)

    def piece(d, which):
        return x.at[
            span_rows(flipped(place, d)),
            pl.ds(pl.multiple_of(core * half + which * quarter, 128), quarter),
        ]

    tokens = {}

    def token_landed(which, d):
        return tok_recv.at[4] if d == 3 else tok_recv.at[which * 2 + d - 1]

    def send_piece(which, d_from, hop):
        d_there = d_from + hop
        tokens[(which, d_there)] = remote(
            piece(d_from, which), piece(d_from, which),
            tok_send.at[0], token_landed(which, d_there), (chips[hop], core),
        )
        tokens[(which, d_there)].start()

    def send_half(d):
        block = x.at[span_rows(flipped(place, d)), pl.ds(own_half, half)]
        remote(block, block, half_send.at[0], half_recv.at[d], partner).start()

    send_piece(0, 0, 1)
    send_piece(1, 0, 2)
    send_piece(1, 0, 1)
    send_piece(0, 0, 2)
    send_half(0)

    for d in range(1, group):
        near_block(CLASS_A, d).wait_recv()
        own_far(CLASS_A, d)

    for copy in small[1:]:
        copy.wait()
    for copy in rate_moves:
        copy.wait_recv()
    rates[place] = rate_pack[0]
    for s in range(group):
        for part in range(2):
            cums[s * 8 : s * 8 + rate_rows, part * length // 2 : (part + 1) * length // 2] = rates[
                s, part * rate_rows : (part + 1) * rate_rows, :
            ]
        cums[s * 8 + rate_rows : s * 8 + 8, :] = jnp.zeros((8 - rate_rows, length), f32)
    lanes = lax.broadcasted_iota(jnp.int32, (group * 8, length), 1)
    kinds = lax.rem(lax.broadcasted_iota(jnp.int32, (group * 8, length), 0), 8)
    running = cums[...] * LOG2E
    step = 1
    while step < length:
        ahead = jnp.where(lanes >= step, pltpu.roll(running, step, 1), 0.0)
        behind = jnp.where(lanes < length - step, pltpu.roll(running, length - step, 1), 0.0)
        running = running + jnp.where(kinds < heads, ahead, behind)
        step *= 2
    cums[...] = running
    wide[...] = jnp.zeros_like(wide)
    first_head = lax.broadcasted_iota(jnp.int32, (length, ch), 1) < HEAD_DIM
    lane_in_head = lax.rem(lax.broadcasted_iota(jnp.int32, (length, ch), 1), HEAD_DIM)
    leading = lane_in_head < HEAD_DIM // 2

    @pl.loop(0, group)
    def _(s):
        sums = cums[pl.ds(pl.multiple_of(s * 8, 8), 8), :]
        wide[0:8, :] = sums
        columns = wide[...].T
        cf = [columns[:, h : h + 1] for h in range(heads)]
        rb = [columns[:, heads + h : heads + h + 1] for h in range(heads)]
        cf_wide = jnp.where(first_head, cf[0], cf[1])
        rb_wide = jnp.where(first_head, rb[0], rb[1])
        ef[s] = jnp.exp2(cf_wide)
        eb[s] = jnp.exp2(rb_wide)
        kf[s] = jnp.exp2(cf_wide[length - 1 : length, :] - cf_wide)
        kb[s] = jnp.exp2(rb_wide[0:1, :] - rb_wide)
        row_at = lax.broadcasted_iota(jnp.int32, (length, length), 0)
        col_at = lax.broadcasted_iota(jnp.int32, (length, length), 1)
        for h in range(heads):
            spread = jnp.where(
                col_at <= row_at, cf[h] - sums[h : h + 1, :], rb[h] - sums[heads + h : heads + h + 1, :]
            )
            decay[s, h] = jnp.exp2(spread)
        turn = base_ref[s]
        cos_0, sin_0 = turn[0:1, :], turn[1:2, :]
        cos_i, sin_i = turn_ref[0], turn_ref[1]
        cosines[s] = cos_0 * cos_i - sin_0 * sin_i
        angle_sine = sin_0 * cos_i + cos_0 * sin_i
        sines[s] = jnp.where(leading, -angle_sine, angle_sine)

    def out_piece(r, d, which):
        start = pl.multiple_of((source_plane(r) * group + flipped(place, d)) * out_cols, 128)
        return wo.at[core, pl.ds(which * side_rows, side_rows), pl.ds(start, out_cols)]

    def out_move(r, which, d_there, hop):
        block = out_piece(r, d_there - hop, which)
        return remote(
            block, block, wo_send.at[0], out_sem(r, which, d_there),
            (chips[hop], core),
        )

    def out_sem(r, which, d):
        first = (which, d) == (0, 1)
        return wo_recv.at[r, 0 if first else 1 if (which, d) == (1, 2) else 2]

    def out_landed(r, which, d):
        block = out_piece(r, d, which)
        remote(block, block, wo_send.at[0], out_sem(r, which, d), partner).wait_recv()

    def spread_out(r):
        for which, hop in ((0, 1), (1, 2), (1, 1), (0, 2)):
            out_move(r, which, hop, hop).start()

    def relay_out(r):
        out_landed(r, 0, 1)
        out_move(r, 0, 3, 2).start()
        out_landed(r, 1, 2)
        out_move(r, 1, 3, 1).start()

    def finish_out(r):
        pieces = 1 if r == 1 else 2
        block = wo.at[core, :, pl.ds(0, pieces * out_cols)]
        remote(block, block, wo_send.at[0], wo_recv.at[r, 2], partner).wait_recv()
        if r == 1:
            out_landed(r, 0, 1)
            out_landed(r, 1, 2)

    def part_at(r):
        return pl.ds(pl.multiple_of(source_plane(r) * part_cols, 128), part_cols)

    def out_block(r, d):
        start = pl.multiple_of((source_plane(r) * group + flipped(place, d)) * out_cols, 128)
        return pl.ds(start, out_cols)

    def mate_copy(cols, i):
        block = wo.at[core, :, cols]
        return remote(block, block, mate_send.at[0], mate_recv.at[i], partner)

    def mate_here(cols, i):
        block = wo.at[1 - core, :, cols]
        remote(block, block, mate_send.at[0], mate_recv.at[i], partner).wait_recv()

    def wait_half(d):
        block = x.at[
            span_rows(flipped(place, d)), pl.ds(pl.multiple_of((1 - core) * half, 128), half)
        ]
        remote(block, block, half_send.at[0], half_recv.at[d], partner).wait_recv()

    for d in range(group):
        arrive(CLASS_A, 1, middle, (d,))
        arrive(CLASS_A, 2, middle, (d,))
    arrive(CLASS_OUT, 1, middle)
    for d in range(1, group):
        near_block(CLASS_B, d).wait_recv()
    own_here(CLASS_B)

    @pl.when(ends)
    def _():
        for d in range(group):
            own_far(CLASS_B, d)

    tokens[(0, 1)].wait_recv()
    send_piece(0, 1, 2)
    tokens[(1, 2)].wait_recv()
    send_piece(1, 2, 1)
    spread_out(0)
    arrive(CLASS_OUT, 1, ends)
    spread_out(1)
    arrive(CLASS_A, 3, middle)
    arrive(CLASS_OUT, 2, middle)

    @pl.when(middle)
    def _():
        for d in range(group):
            own_far(CLASS_B, d)

    tokens[(1, 1)].wait_recv()
    send_half(1)
    tokens[(0, 2)].wait_recv()
    send_half(2)
    for r in range(1, planes):
        arrive(CLASS_A, r, ends)
    arrive(CLASS_OUT, 3, middle)
    arrive(CLASS_B, 1, middle)
    wait_half(0)

    same_head = (
        lax.div(lax.broadcasted_iota(jnp.int32, (ch, ch), 0), HEAD_DIM)
        == lax.div(lax.broadcasted_iota(jnp.int32, (ch, ch), 1), HEAD_DIM)
    )

    def one_span(s):
        rows = span_rows(s)
        held = jnp.dot(x[rows, :], w[:, 0:col_a], preferred_element_type=f32)
        cosine, sine = cosines[s], sines[s]

        def turned(value):
            value = value.astype(bf16).astype(f32)
            other = jnp.where(
                leading,
                pltpu.roll(value, ch - HEAD_DIM // 2, 1),
                pltpu.roll(value, HEAD_DIM // 2, 1),
            )
            return value * cosine + other * sine

        rk = (turned(held[:, 0:ch]) * HEAD_DIM ** (-0.5)).astype(bf16).astype(f32)
        rq = turned(held[:, ch : 2 * ch]).astype(bf16)
        value = held[:, 2 * ch : 3 * ch].astype(bf16)
        rq_buf[s] = rq
        v_buf[s] = value
        gate_buf[s] = held[:, 3 * ch : 4 * ch].astype(bf16)
        value_wide = value.astype(f32)
        found = None
        for h in range(heads):
            in_head = first_head if h == 0 else jnp.logical_not(first_head)
            key_head = jnp.where(in_head, rk, 0.0).astype(bf16)
            value_head = jnp.where(in_head, value_wide, 0.0).astype(bf16)
            scores = lax.dot_general(
                rq, key_head, (((1,), (1,)), ((), ())), preferred_element_type=f32
            )
            probs = (scores * decay[s, h]).astype(bf16)
            part = jnp.dot(probs, value_head, preferred_element_type=f32)
            found = part if found is None else found + part
        loc[s] = found
        for table, target in ((kf, state_f), (kb, state_b)):
            keys = (rk * table[s]).astype(bf16)
            state = lax.dot_general(
                keys, value, (((0,), (0,)), ((), ())), preferred_element_type=f32
            )
            target[s] = jnp.where(same_head, state, 0.0)

    halo_rows = 16
    halo_at = (all_rows, all_rows + halo_rows)

    def halo_move(way):
        cols = pl.ds(own_half, half)
        source = x.at[pl.ds((all_rows - halo_rows) * (1 - way), halo_rows), cols]
        return remote(
            source, x.at[pl.ds(halo_at[way], halo_rows), cols],
            halo_send.at[way], halo_recv.at[way], (own + group if way == 0 else own - group, core),
        )

    def halo_pass(way):
        block = x.at[pl.ds(halo_at[way], halo_rows), pl.ds(own_half, half)]
        return remote(block, block, halo_send.at[2 + way], halo_recv.at[2 + way], partner)

    def halo_comes(way):
        return has_down if way == 0 else has_up

    blank = jnp.zeros((halo_rows, width), bf16)

    @pl.when(jnp.logical_not(has_down))
    def _():
        x[pl.ds(all_rows, halo_rows), :] = blank

    @pl.when(jnp.logical_not(has_up))
    def _():
        x[pl.ds(all_rows + halo_rows, halo_rows), :] = blank

    @pl.loop(0, group)
    def _(d):
        @pl.when(d == 1)
        def _():
            last = x.at[
                span_rows(flipped(place, 3)), pl.ds(pl.multiple_of(core * half, 128), half)
            ]
            remote(last, last, tok_send.at[0], token_landed(0, 3), partner).wait_recv()
            send_half(3)
            wait_half(1)

        @pl.when(d == 2)
        def _():
            wait_half(2)

        @pl.when(d == 3)
        def _():
            wait_half(3)
            pl.when(has_up)(lambda: halo_move(0).start())
            pl.when(has_down)(lambda: halo_move(1).start())
            relay_out(0)
            arrive(CLASS_OUT, 2, ends)
            spread_out(2)

        one_span(place_at(d))

    def scan_states(state, table, at, order, target):
        passed, inside, reach = jnp.zeros((ch, ch), f32), {}, {}
        over = jnp.ones((1, ch), f32)
        for s in order:
            inside[s], reach[s] = passed, over
            factor = table[s, at : at + 1, :]
            passed = factor * passed + state[s]
            over = over * factor
        folded = passed[0:HEAD_DIM, :]
        for h in range(1, heads):
            folded = folded + passed[h * HEAD_DIM : (h + 1) * HEAD_DIM, :]
        pack_out[target, 0:HEAD_DIM, :] = folded
        pack_out[target, HEAD_DIM : HEAD_DIM + 8, :] = jnp.broadcast_to(over, (8, ch))
        return inside, reach

    ahead_in, ahead_reach = scan_states(state_f, ef, length - 1, range(group), 0)
    back_in, back_reach = scan_states(state_b, eb, 0, range(group)[::-1], 1)

    def pack_move(way, k):
        to = own + k * group if way == 0 else own - k * group
        return remote(
            pack_out.at[way], pack_in.at[way, k - 1],
            pack_send.at[way, k - 1], pack_recv.at[way, k - 1], (to, core),
        )

    def gives(way, k):
        return plane + k < planes if way == 0 else plane - k >= 0

    def takes(way, k):
        return gives(1 - way, k)

    for k in range(1, planes):
        for way in range(2):
            pl.when(gives(way, k))(lambda way=way, k=k: pack_move(way, k).start())
    arrive(CLASS_B, 2, middle)
    arrive(CLASS_B, 3, middle)

    def feature_cols(kind):
        return pl.ds(pl.multiple_of(kind * side_rows + place * ch, 128), ch)

    my_rows = length // 2

    def row_half(c):
        return pl.ds(pl.multiple_of(c * my_rows, 128), my_rows)

    def feature_move(kind, d, s, c):
        sender = ft_send.at[0]
        return remote(
            parts.at[kind, s, row_half(c)], feat.at[core, :, feature_cols(kind)],
            sender, ft_recv.at[kind, d], (base + s, c),
        )

    def feature_mate(kind):
        return remote(
            parts.at[kind, place, row_half(1 - core)], feat.at[core, :, feature_cols(kind)],
            ft_send.at[1], ft_recv.at[kind, 0], partner,
        )

    def own_features(kind):
        feature_mate(kind).start()
        feat[core, :, feature_cols(kind)] = parts[kind, place, row_half(core), :]

    finish_out(0)

    def pair_block(q):
        start = pl.multiple_of((q * group + flipped(place, 3)) * out_cols, 128)
        block = wo.at[core, :, pl.ds(start, out_cols)]
        return remote(
            block, block, pair_sem.at[0], pair_sem.at[1],
            ((plane + 1 - 2 * lax.rem(plane, 2)) * group + place, core),
        )

    pair_block(plane).start()
    mate_copy(part_at(0), 0).start()
    arrive(CLASS_OUT, 3, ends)
    spread_out(3)
    incoming = []
    for way in range(2):
        into[way] = jnp.zeros((HEAD_DIM, ch), f32)
        into[way + 2] = jnp.ones((HEAD_DIM, ch), f32)
        for k in range(1, planes):
            @pl.when(takes(way, k))
            def _(way=way, k=k):
                pack_move(way, k).wait_recv()
                into[way] = into[way] + into[way + 2] * pack_in[way, k - 1, 0:HEAD_DIM, :]
                into[way + 2] = into[way + 2] * pack_in[
                    way, k - 1, HEAD_DIM : HEAD_DIM + 1, :
                ]
        incoming.append(
            jnp.where(same_head, jnp.concatenate([into[way]] * heads, axis=0), 0.0)
        )
    for s in range(group):
        state_f[s] = ahead_in[s] + ahead_reach[s] * incoming[0]
        state_b[s] = back_in[s] + back_reach[s] * incoming[1]

    @pl.loop(0, group)
    def _(i):
        d = group - 1 - i
        s = place_at(d)
        query = rq_buf[s]
        mix = (
            loc[s]
            + ef[s] * jnp.dot(query, state_f[s].astype(bf16), preferred_element_type=f32)
            + eb[s] * jnp.dot(query, state_b[s].astype(bf16), preferred_element_type=f32)
        )
        squares = mix * mix
        first = jnp.sum(jnp.where(first_head, squares, 0.0), axis=-1, keepdims=True)
        second = jnp.sum(jnp.where(first_head, 0.0, squares), axis=-1, keepdims=True)
        scale = lax.rsqrt(jnp.where(first_head, first, second) / HEAD_DIM + EPS)
        gate = gate_buf[s].astype(f32)
        parts[1, s] = (
            gate / (1.0 + jnp.exp(-gate)) * (mix * scale * head_gain_ref[:, place_cols])
        ).astype(bf16)

        @pl.when(d > 0)
        def _():
            for c in range(2):
                feature_move(1, d, s, c).start()

    own_features(1)

    for way in range(2):
        @pl.when(halo_comes(way))
        def _(way=way):
            halo_move(way).wait_recv()
            halo_pass(way).start()
    relay_out(2)
    arrive(CLASS_B, 1, ends)
    arrive(CLASS_B, 2, ends)
    for way in range(2):
        pl.when(halo_comes(way))(lambda way=way: halo_pass(way).wait_recv())
    depth = group * rows_in
    most = (planes - 1) * depth
    early = pl.multiple_of(top * depth, 128)
    late = pl.multiple_of((1 - top) * most, 128)
    blocks = 5
    block = (all_rows + 2 * halo_rows) // blocks

    @pl.loop(0, blocks)
    def _(t):
        rows = pl.ds(pl.multiple_of(t * block, 16), block)
        acc[rows, :] = jnp.dot(
            x[rows, pl.ds(early, most)], w[pl.ds(early, most), col_a : col_a + col_b],
            preferred_element_type=f32,
        )

    relay_out(3)
    finish_out(1)
    for d in range(group - 1):
        mate_copy(out_block(1, d), 1).start()
    arrive(CLASS_B, 3, ends)

    spans_at = [s * length - halo_rows for s in range(1, group)] + [all_rows]
    late_w = w[pl.ds(late, depth), col_a : col_a + col_b]
    near_rows = jnp.concatenate(
        [x[at : at + 2 * halo_rows, pl.ds(late, depth)] for at in spans_at], axis=0
    )
    near_sums = jnp.concatenate(
        [acc[at : at + 2 * halo_rows, 0 : 2 * ch] for at in spans_at], axis=0
    )

    def inner_product(held):
        held = held.astype(bf16).astype(f32)
        return (held[:, 0:ch] * held[:, ch : 2 * ch]).astype(bf16).astype(f32)

    edge_values = inner_product(
        near_sums + jnp.dot(near_rows, late_w[:, 0 : 2 * ch], preferred_element_type=f32)
    )
    for s in range(group):
        before = ((s - 1) % group) * 2 * halo_rows + halo_rows - 1
        after = s * 2 * halo_rows + halo_rows
        edges[s, 0:1, :] = edge_values[before : before + 1, :]
        edges[s, 1:2, :] = edge_values[after : after + 1, :]
    row_of = lax.broadcasted_iota(jnp.int32, (length, ch), 0)

    @pl.loop(0, group)
    def _(i):
        turned_round = lax.div(i, 2)
        d = (1 - turned_round) * (1 + 2 * i) + turned_round * (6 - 2 * i)
        s = place_at(d)
        rows = span_rows(s)
        held = acc[rows, :] + jnp.dot(
            x[rows, pl.ds(late, depth)], w[pl.ds(late, depth), col_a : col_a + col_b],
            preferred_element_type=f32,
        )
        inner = inner_product(held)
        before = jnp.where(row_of == 0, edges[s, 0:1, :], pltpu.roll(inner, 1, 0))
        after = jnp.where(row_of == length - 1, edges[s, 1:2, :], pltpu.roll(inner, length - 1, 0))
        near_sum = (
            taps_ref[0:1, place_cols] * before
            + taps_ref[1:2, place_cols] * inner
            + taps_ref[2:3, place_cols] * after
        )
        parts[0, s] = (held[:, 2 * ch : 3 * ch].astype(bf16).astype(f32) * near_sum).astype(bf16)

        @pl.when(d > 0)
        def _():
            for c in range(2):
                feature_move(0, d, s, c).start()

    own_features(0)

    def features_here(kind, places):
        for d in places:
            rows = my_rows if d == 0 else length
            block = parts.at[0, 0, pl.ds(0, rows)]
            remote(block, block, ft_send.at[0], ft_recv.at[kind, d], partner).wait_recv()

    def product(rows, r):
        total = None
        for c in range(2):
            part = jnp.dot(feat[c, :, rows], wo[c, rows, part_at(r)], preferred_element_type=f32)
            total = part if total is None else total + part
        return total

    def retention_product(r):
        decay[r, 0, 0:my_rows, :] = product(pl.ds(side_rows, side_rows), r)

    pair_rows = 2 * ch
    own_pair = lax.div(place, 2)

    def conv_product(r, pair):
        at = pl.ds(pl.multiple_of(pair * pair_rows, 128), pair_rows)
        return decay[r, 0, 0:my_rows, :] + product(at, r)

    features_here(1, range(group))
    mate_here(part_at(0), 0)
    retention_product(0)
    finish_out(2)
    mate_copy(part_at(2), 3).start()
    finish_out(3)
    mate_copy(part_at(3), 4).start()
    mate_here(part_at(2), 3)
    retention_product(2)
    pair_block(source_plane(1)).wait_recv()
    mate_copy(out_block(1, 3), 2).start()
    mate_here(part_at(3), 4)
    retention_product(3)
    features_here(0, (0, 1))
    for r in (0, 2, 3):
        decay[r, 0, 0:my_rows, :] = conv_product(r, own_pair)
    mate_here(pl.ds(0, (group - 1) * out_cols), 1)
    mate_here(out_block(1, 3), 2)
    retention_product(1)
    decay[1, 0, 0:my_rows, :] = conv_product(1, own_pair)

    for copy in rate_moves:
        copy.wait_send()
    ssq_move.wait_send()

    def sent(block, semaphore, landed):
        remote(block, block, semaphore, landed, partner).wait_send()

    sent(
        x.at[pl.ds(0, (group - 1) * length), pl.ds(0, 2 * quarter)], tok_send.at[0],
        tok_recv.at[0],
    )
    sent(x.at[pl.ds(0, all_rows), pl.ds(0, half)], half_send.at[0], half_recv.at[0])
    sent(
        wo.at[core, :, pl.ds(0, ((group - 1) * planes - 1) * out_cols)], wo_send.at[0],
        wo_recv.at[0, 0],
    )
    pair_block(plane).wait_send()
    sent(
        w.at[pl.ds(0, (group - 1) * rows_in), :], near_send.at[0], near_recv.at[0, 0]
    )
    sent(wo.at[core], mate_send.at[0], mate_recv.at[0])
    pl.when(has_up)(lambda: halo_move(0).wait_send())
    pl.when(has_down)(lambda: halo_move(1).wait_send())
    for way in range(2):
        pl.when(halo_comes(way))(lambda way=way: halo_pass(way).wait_send())
    for k in range(1, planes):
        for way in range(2):
            pl.when(gives(way, k))(lambda way=way, k=k: pack_move(way, k).wait_send())
    for kind in range(3):
        for units in range(1, planes):
            pl.when(plane == units - 1)(functools.partial(far_sent, kind, 0, units))
            pl.when(plane == planes - units)(functools.partial(far_sent, kind, 1, units))

    features_here(0, (2, 3))
    for r in range(planes):
        out_ref[:, part_at(r)] = conv_product(r, 1 - own_pair).astype(bf16)
    sent(parts.at[:, pl.ds(0, group - 1)], ft_send.at[0], ft_recv.at[0, 0])
    sent(parts.at[:, 0, pl.ds(0, my_rows)], ft_send.at[1], ft_recv.at[0, 0])


def turn_tables(spans, length, channels):
    half_dim = HEAD_DIM // 2
    frequency = THETA ** (-2.0 * (np.arange(channels) % half_dim) / HEAD_DIM)
    inner = np.arange(length)[:, None] * frequency
    outer = (np.arange(spans) * length)[:, None] * frequency
    turn = np.stack([np.cos(inner), np.sin(inner)])
    start = np.zeros((spans, 8, channels))
    start[:, 0], start[:, 1] = np.cos(outer), np.sin(outer)
    return turn.astype(np.float32), start.astype(np.float32)


def mixer(planes, group, arrays):
    (
        tokens, norm_gain, outer_gate, inner_gate, conv_input, query_proj, key_proj, value_proj,
        out_gate, conv_taps, log_decay, head_gain, conv_output, retention_output,
    ) = arrays
    f32, bf16 = jnp.float32, jnp.bfloat16
    length, half = tokens.shape
    width = 2 * half
    ch = outer_gate.shape[1] // group
    heads = ch // HEAD_DIM
    rows, side = group * length, conv_output.shape[0]
    turn, start = turn_tables(planes * group, length, ch)
    dma = pltpu.SemaphoreType.DMA
    vmem, held = pl.BlockSpec(memory_space=pltpu.VMEM), pl.BlockSpec(memory_space=pltpu.HBM)
    v = pltpu.VMEM
    result = jax.ShapeDtypeStruct((length // 2, width), bf16)
    table = v((group, length, ch), f32)
    return pl.pallas_call(
        functools.partial(mixer_kernel, planes, group),
        out_shape=result,
        in_specs=[held] * 16,
        out_specs=vmem,
        scratch_shapes=[
            v((1, width), f32), v(conv_taps.shape, f32), v((1, head_gain.shape[0]), f32), v(turn.shape, f32),
            v((group,) + start.shape[1:], f32),
            v((length, half), bf16), v((rows + 32, width), bf16), v((width, 7 * ch), bf16),
            v((2, 2 * side, width), bf16), v(log_decay.shape, f32),
            v((group, 4 * heads, length // 2), f32), v((group, 4 * heads, length // 2), f32),
            v((8 * group, length), f32), v((128, length), f32),
            v((length, 128), f32), v((length, 128), f32),
            table, table, v((group, heads, length, length), f32),
            table, table, table, table,
            v((group, length, ch), bf16), v((group, length, ch), bf16), v((group, length, ch), bf16),
            table, v((group, ch, ch), f32), v((group, ch, ch), f32),
            v((2, HEAD_DIM + 8, ch), f32), v((2, planes - 1, HEAD_DIM + 8, ch), f32),
            v((4, HEAD_DIM, ch), f32),
            v((rows + 32, 3 * ch), f32), v((group, 8, ch), f32),
            v((2, group, length, ch), bf16), v((2, length // 2, 2 * side), bf16),
            dma((10,)), dma((1,)), dma((2, group - 1)), dma((1,)), dma((group - 1,)), dma((2,)),
            dma((1,)), dma((5,)), dma((1,)), dma((group,)),
            dma((3, 2)), dma((2, planes - 1, group)), dma((planes - 1,)),
            dma((1,)), dma((planes, 3)), dma((1,)), dma((5,)), dma((2,)), dma((4,)), dma((4,)),
            dma((2, planes - 1)), dma((2, planes - 1)), dma((2,)), dma((2, group)),
        ],
        compiler_params=pltpu.CompilerParams(
            collective_id=0, has_side_effects=True, vmem_limit_bytes=50 * 2**20
        ),
    )(
        *(
            pltpu.with_memory_space_constraint(source, pltpu.HBM)
            for source in (
                tokens, key_proj, query_proj, value_proj, out_gate, inner_gate, conv_input,
                outer_gate, conv_output, retention_output, log_decay, norm_gain.reshape(1, -1),
                conv_taps, head_gain.reshape(1, -1), jnp.asarray(turn), jnp.asarray(start),
            )
        )
    )


LANES = 128

def plan(*arrays):
    spans, cores = lax.axis_size("sp"), lax.axis_size("tp")
    group = arrays[2].shape[1] // LANES
    planes = spans // group
    fits = (
        cores == 2
        and group == 4
        and planes * group == spans
        and planes == 2 * cores
        and arrays[0].shape[1] == 2 * group * arrays[2].shape[0]
    )
    return mixer(planes, group, arrays) if fits else local(*arrays)


def solution(mesh):
    return jax.shard_map(
        plan,
        mesh=mesh,
        in_specs=(
            P("sp", "tp"),
            P(),
            P("sp", "tp"),
            P("sp", "tp"),
            P("sp", "tp"),
            P("sp", "tp"),
            P("sp", "tp"),
            P("sp", "tp"),
            P("sp", "tp"),
            P(None, "tp"),
            P(None, "tp", "sp"),
            P("tp"),
            P("tp", "sp"),
            P("tp", "sp"),
        ),
        out_specs=P(("sp", "tp"), None),
        check_vma=False,
    )
```

```python
import jax
import functools
import jax.numpy as jnp
import numpy as np
from jax import lax
from jax.experimental import pallas as pl
from jax.experimental.pallas import tpu as pltpu
from jax.sharding import PartitionSpec as P

HEAD_DIM = 64


EPS = 1e-06
THETA = 10000.0


def with_halo(shard, sides, width):
    for axis, dim in sides:
        size, length = (lax.axis_size(axis), shard.shape[dim])
        up = [(i, (i + 1) % size) for i in range(size - 1)]
        down = [(j, i) for i, j in up]
        last = lax.slice_in_dim(shard, length - width, length, axis=dim)
        first = lax.slice_in_dim(shard, 0, width, axis=dim)
        before = lax.ppermute(last, axis, up)
        after = lax.ppermute(first, axis, down)
        shard = jnp.concatenate([before, shard, after], axis=dim)
    return shard


def rotate(field_in, position_list):
    half_dim = field_in.shape[-1] // 2
    frequency = jnp.exp(
        -jnp.log(THETA) * jnp.arange(half_dim, dtype=jnp.float32) * (2.0 / field_in.shape[-1])
    )
    angles = position_list.astype(jnp.float32)[:, None, None] * frequency
    cosine = jnp.cos(angles)
    sine_part = jnp.sin(angles)
    leading = field_in[..., :half_dim]
    trailing = field_in[..., half_dim:]
    return jnp.concatenate(
        [leading * cosine - trailing * sine_part, leading * sine_part + trailing * cosine], axis=-1
    )


def conv_branch(outer_rows, inner_rows, conv_values, conv_taps):
    inner_value = (inner_rows.astype(jnp.float32) * conv_values.astype(jnp.float32)).astype(
        jnp.bfloat16
    )
    padded = with_halo(inner_value, (("sp", 0),), 1).astype(jnp.float32)
    convolved = conv_taps[0] * padded[:-2] + conv_taps[1] * padded[1:-1] + conv_taps[2] * padded[2:]
    return (outer_rows.astype(jnp.float32) * convolved).astype(jnp.bfloat16)


def span_parts(query_rows, key_rows, value_rows, log_rates):
    length = query_rows.shape[0]
    forward_cum = jnp.cumsum(log_rates[0], axis=-1)
    backward_cum = jnp.flip(jnp.cumsum(jnp.flip(log_rates[1], -1), axis=-1), -1)
    row_index = lax.broadcasted_iota(jnp.int32, (length, length), 0)
    col_index = lax.broadcasted_iota(jnp.int32, (length, length), 1)
    lower_part = (col_index <= row_index)[None]
    spread = jnp.where(
        lower_part,
        forward_cum[:, :, None] - forward_cum[:, None, :],
        backward_cum[:, :, None] - backward_cum[:, None, :],
    )
    scores = jnp.einsum("ihe,jhe->hij", query_rows, key_rows, preferred_element_type=jnp.float32)
    weighted = (scores * jnp.exp(spread)).astype(jnp.bfloat16)
    local_part = jnp.einsum(
        "hij,jhe->ihe", weighted, value_rows, preferred_element_type=jnp.float32
    )
    key_wide = key_rows.astype(jnp.float32)
    forward_keys = (key_wide * jnp.exp(forward_cum[:, -1:] - forward_cum).T[:, :, None]).astype(
        jnp.bfloat16
    )
    backward_keys = (key_wide * jnp.exp(backward_cum[:, :1] - backward_cum).T[:, :, None]).astype(
        jnp.bfloat16
    )
    forward_state = jnp.einsum(
        "jhd,jhe->hde", forward_keys, value_rows, preferred_element_type=jnp.float32
    )
    backward_state = jnp.einsum(
        "jhd,jhe->hde", backward_keys, value_rows, preferred_element_type=jnp.float32
    )
    return (local_part, forward_cum, backward_cum, forward_state, backward_state)


def retention_branch(query_rows, key_rows, value_rows, gate_rows, log_decay, head_gain, offsets):
    row_count = query_rows.shape[0]
    head_count = query_rows.shape[1] // HEAD_DIM
    shape_heads = (row_count, head_count, HEAD_DIM)
    rotated_query = rotate(query_rows.astype(jnp.float32).reshape(shape_heads), offsets).astype(
        jnp.bfloat16
    )
    rotated_key = (
        rotate(key_rows.astype(jnp.float32).reshape(shape_heads), offsets) * HEAD_DIM ** (-0.5)
    ).astype(jnp.bfloat16)
    local_part, forward_cum, backward_cum, forward_state, backward_state = span_parts(
        rotated_query, rotated_key, value_rows.reshape(shape_heads), log_decay
    )
    forward_total = forward_cum[:, -1]
    backward_total = backward_cum[:, 0]
    totals = lax.all_gather(
        jnp.stack([forward_total, backward_total])[None], "sp", axis=0, tiled=True
    )
    inclusive = jnp.cumsum(totals, axis=0)
    exclusive = inclusive - totals
    own_index = lax.axis_index("sp")
    own_inclusive = lax.dynamic_index_in_dim(inclusive, own_index, 0, keepdims=False)
    own_exclusive = lax.dynamic_index_in_dim(exclusive, own_index, 0, keepdims=False)
    pieces = (
        lax.all_gather(forward_state[None], "sp", axis=0, tiled=True),
        lax.all_gather(backward_state[None], "sp", axis=0, tiled=True),
    )
    piece_count = pieces[0].shape[0]
    span_index = lax.iota(jnp.int32, piece_count)
    forward_weight = jnp.where(
        (span_index < own_index)[:, None],
        jnp.exp(jnp.minimum(own_exclusive[0] - inclusive[:, 0], 0.0)),
        0.0,
    )
    backward_weight = jnp.where(
        (span_index > own_index)[:, None],
        jnp.exp(jnp.minimum(exclusive[:, 1] - own_inclusive[1], 0.0)),
        0.0,
    )
    into_forward = jnp.einsum(
        "nh,nhde->hde", forward_weight, pieces[0], precision=lax.Precision.HIGHEST
    )
    into_backward = jnp.einsum(
        "nh,nhde->hde", backward_weight, pieces[1], precision=lax.Precision.HIGHEST
    )
    forward_part = jnp.einsum(
        "ihd,hde->ihe",
        rotated_query,
        into_forward.astype(jnp.bfloat16),
        preferred_element_type=jnp.float32,
    )
    backward_part = jnp.einsum(
        "ihd,hde->ihe",
        rotated_query,
        into_backward.astype(jnp.bfloat16),
        preferred_element_type=jnp.float32,
    )
    mixed_heads = (
        local_part
        + jnp.exp(forward_cum).T[:, :, None] * forward_part
        + jnp.exp(backward_cum).T[:, :, None] * backward_part
    )
    scaled = mixed_heads * lax.rsqrt(
        jnp.mean(mixed_heads * mixed_heads, axis=-1, keepdims=True) + EPS
    )
    scaled = scaled * head_gain.reshape(head_count, HEAD_DIM)
    return (
        jax.nn.silu(gate_rows.astype(jnp.float32))
        * scaled.reshape(row_count, head_count * HEAD_DIM)
    ).astype(jnp.bfloat16)


def local(
    tokens,
    norm_gain,
    outer_gate,
    inner_gate,
    conv_input,
    query_proj,
    key_proj,
    value_proj,
    out_gate,
    conv_taps,
    log_decay,
    head_gain,
    conv_output,
    retention_output,
):
    whole = lax.all_gather(tokens, "tp", axis=1, tiled=True)
    wide = whole.astype(jnp.float32)
    normed = (
        wide * lax.rsqrt(jnp.mean(wide * wide, axis=-1, keepdims=True) + EPS) * norm_gain
    ).astype(jnp.bfloat16)
    row_count = normed.shape[0]
    offsets = lax.axis_index("sp") * row_count + lax.iota(jnp.int32, row_count)
    gathered = (
        lax.all_gather(outer_gate, "sp", axis=0, tiled=True),
        lax.all_gather(inner_gate, "sp", axis=0, tiled=True),
        lax.all_gather(conv_input, "sp", axis=0, tiled=True),
        lax.all_gather(query_proj, "sp", axis=0, tiled=True),
        lax.all_gather(key_proj, "sp", axis=0, tiled=True),
        lax.all_gather(value_proj, "sp", axis=0, tiled=True),
        lax.all_gather(out_gate, "sp", axis=0, tiled=True),
        lax.all_gather(conv_output, "sp", axis=1, tiled=True),
        lax.all_gather(retention_output, "sp", axis=1, tiled=True),
    )
    projected = [
        jnp.dot(normed, weight, preferred_element_type=jnp.float32).astype(jnp.bfloat16)
        for weight in gathered[:7]
    ]
    conv_out = conv_branch(projected[0], projected[1], projected[2], conv_taps)
    ret_out = retention_branch(
        projected[3], projected[4], projected[5], projected[6], log_decay, head_gain, offsets
    )
    conv_weight = gathered[7]
    ret_weight = gathered[8]
    return lax.psum_scatter(
        (
            jnp.dot(conv_out, conv_weight, preferred_element_type=jnp.float32)
            + jnp.dot(ret_out, ret_weight, preferred_element_type=jnp.float32)
        ).astype(jnp.bfloat16),
        "tp",
        scatter_dimension=0,
        tiled=True,
    )


def flipped(place, d):
    if d == 0:
        return place
    if d == 1:
        return place + 1 - 2 * lax.rem(place, 2)
    if d == 2:
        return place + 2 - 4 * lax.rem(lax.div(place, 2), 2)
    return 3 - place


LOG2E = 1.4426950408889634
CLASS_A, CLASS_B, CLASS_OUT = 0, 1, 2


def mixer_kernel(
    planes, group,
    tok_ref, key_w, query_w, value_w, gate_w, inner_w, conv_w, outer_w,
    cout_ref, rout_ref, rate_in, gain_in, taps_in, head_gain_in, turn_in, base_in,
    out_ref, gain_ref, taps_ref, head_gain_ref, turn_ref, base_ref,
    xin, x, w, wo, rate_own, rate_pack, rates, cums, wide, ssq_out, ssq_in, cosines, sines, decay,
    ef, eb, kf, kb, rq_buf, v_buf, gate_buf, loc, state_f, state_b, pack_out, pack_in, into,
    acc, edges, parts, feat,
    own_sem, near_send, near_recv, rate_send, rate_recv, ssq_sem,
    tok_send, tok_recv, half_send, half_recv, far_send, far_recv, out_recv,
    wo_send, wo_recv, mate_send, mate_recv, pair_sem, halo_send, halo_recv, pack_send, pack_recv,
    ft_send, ft_recv,
):
    f32, bf16 = jnp.float32, jnp.bfloat16
    own, core = lax.axis_index("sp"), lax.axis_index("tp")
    place, plane = lax.rem(own, group), lax.div(own, group)
    base = plane * group
    length, half = tok_ref.shape
    width = 2 * half
    quarter = half // 2
    rows_in = key_w.shape[0]
    ch = key_w.shape[1] // group
    heads = ch // HEAD_DIM
    all_rows = group * length
    side_rows = cout_ref.shape[0]
    out_cols = cout_ref.shape[1]
    part_cols = group * out_cols
    col_a, col_b = 4 * ch, 3 * ch
    has_up, has_down = plane < planes - 1, plane > 0
    middle = jnp.logical_and(has_up, has_down)
    top = lax.div(plane, planes // 2)
    mesh_id = pl.DeviceIdType.MESH
    chips = [base + flipped(place, d) for d in range(group)]
    partner = (own, 1 - core)
    weights = (key_w, query_w, value_w, gate_w, inner_w, conv_w, outer_w)

    def local_copy(source, target, i):
        return pltpu.make_async_copy(source, target, own_sem.at[i])

    def remote(source, target, send, recv, device):
        return pltpu.make_async_remote_copy(
            src_ref=source, dst_ref=target, send_sem=send, recv_sem=recv,
            device_id=device, device_id_type=mesh_id,
        )

    own_rows = pl.ds(pl.multiple_of(own * rows_in, 128), rows_in)
    own_cols = pl.ds(pl.multiple_of(own * out_cols, 128), out_cols)
    kept = [local_copy(tok_ref, xin, 0), local_copy(rate_in, rate_own, 1)]
    for j, source in enumerate(weights):
        kept.append(
            local_copy(
                source.at[:, pl.ds(pl.multiple_of(place * ch, 128), ch)],
                w.at[own_rows, pl.ds(j * ch, ch)], 2 + j // 4,
            )
        )
    kept.append(local_copy(cout_ref, wo.at[core, pl.ds(0, side_rows), own_cols], 4))
    kept.append(local_copy(rout_ref, wo.at[core, pl.ds(side_rows, side_rows), own_cols], 4))
    place_cols = pl.ds(pl.multiple_of(place * ch, 128), ch)
    small = [
        local_copy(gain_in, gain_ref, 5),
        local_copy(taps_in, taps_ref, 6),
        local_copy(head_gain_in, head_gain_ref, 7),
        local_copy(turn_in, turn_ref, 8),
        local_copy(base_in.at[pl.ds(base, group)], base_ref, 9),
    ]
    for copy in kept + small:
        copy.start()

    def class_cols(kind):
        return pl.ds(0, col_a) if kind == CLASS_A else pl.ds(col_a, col_b)

    def own_here(kind):
        block = wo.at[core, :, own_cols] if kind == CLASS_OUT else w.at[own_rows, class_cols(kind)]
        local_copy(block, block, 2 + kind).wait()

    barrier = pltpu.get_barrier_semaphore()

    def greet(target):
        pl.semaphore_signal(barrier, inc=1, device_id=target, device_id_type=mesh_id)

    for d in range(1, group):
        for c in range(2):
            greet((chips[d], c))
    greet(partner)
    for k in range(1, planes):
        greet((lax.rem(own + k * group, planes * group), core))
    pl.semaphore_wait(barrier, 2 * group + planes - 2)

    def send_near(j, d):
        to = flipped(place, d)
        remote(
            weights[j].at[:, pl.ds(pl.multiple_of(to * ch, 128), ch)],
            w.at[own_rows, pl.ds(j * ch, ch)],
            near_send.at[0], near_recv.at[j // 4, d - 1], (chips[d], core),
        ).start()

    def near_block(kind, d):
        start = pl.multiple_of((base + flipped(place, d)) * rows_in, 128)
        block = w.at[pl.ds(start, rows_in), class_cols(kind)]
        return remote(
            block, block, near_send.at[0], near_recv.at[kind, d - 1], (chips[d], core)
        )

    for d in range(1, group):
        for j in range(4):
            send_near(j, d)

    rate_rows = 2 * heads
    kept[1].wait()
    rate_moves = []
    for d in range(group):
        to = flipped(place, d)
        for way in range(2):
            for h in range(heads):
                row = rate_own[way, pl.ds(heads * to + h, 1), :]
                for part in range(2):
                    rate_pack[d, pl.ds(part * rate_rows + way * heads + h, 1), :] = row[
                        :, part * length // 2 : (part + 1) * length // 2
                    ]
    for d in range(1, group):
        rate_moves.append(
            remote(
                rate_pack.at[d], rates.at[place], rate_send.at[0], rate_recv.at[d - 1],
                (chips[d], core),
            )
        )
    for copy in rate_moves:
        copy.start()
    for d in range(1, group):
        for j in range(4, 7):
            send_near(j, d)

    def far(kind, direction, q, d):
        if kind == CLASS_OUT:
            block = wo.at[
                core, :, pl.ds(pl.multiple_of((q * group + place) * out_cols, 128), out_cols)
            ]
        else:
            start = pl.multiple_of((q * group + flipped(place, d)) * rows_in, 128)
            block = w.at[pl.ds(start, rows_in), class_cols(kind)]
        to = plane + 1 - 2 * direction
        return remote(
            block, block, far_send.at[kind, direction], far_landed(kind, q, d, to),
            (own + group * (1 - 2 * direction), core),
        )

    def far_landed(kind, q, d, at):
        slot = q - (q > at).astype(jnp.int32)
        return out_recv.at[slot] if kind == CLASS_OUT else far_recv.at[kind, slot, d]

    def far_arrived(kind, q, d):
        if kind == CLASS_OUT:
            block = wo.at[
                core, :, pl.ds(pl.multiple_of((q * group + place) * out_cols, 128), out_cols)
            ]
        else:
            start = pl.multiple_of((q * group + flipped(place, d)) * rows_in, 128)
            block = w.at[pl.ds(start, rows_in), class_cols(kind)]
        remote(
            block, block, far_send.at[kind, 0], far_landed(kind, q, d, plane), partner
        ).wait_recv()

    def far_sent(kind, direction, units):
        if kind == CLASS_OUT:
            block, landed = wo.at[core, :, pl.ds(0, units * out_cols)], out_recv.at[0]
        else:
            block = w.at[pl.ds(0, units * group * rows_in), class_cols(kind)]
            landed = far_recv.at[kind, 0, 0]
        remote(block, block, far_send.at[kind, direction], landed, partner).wait_send()

    def places_of(kind):
        return 1 if kind == CLASS_OUT else group

    def own_far(kind, d):
        pl.when(has_up)(lambda: far(kind, 0, plane, d).start())
        pl.when(has_down)(lambda: far(kind, 1, plane, d).start())

    def source_plane(r):
        if r == 0:
            return plane
        if r == 1:
            return plane + 1 - 2 * lax.rem(plane, 2)
        return r + top * (planes - 1 - 2 * r)

    def arrive(kind, r, only=None, blocks=None):
        q = source_plane(r)

        def take():
            for d in range(places_of(kind)) if blocks is None else blocks:
                far_arrived(kind, q, d)
                pl.when(jnp.logical_and(q < plane, has_up))(
                    lambda d=d: far(kind, 0, q, d).start()
                )
                pl.when(jnp.logical_and(q > plane, has_down))(
                    lambda d=d: far(kind, 1, q, d).start()
                )

        if only is None:
            take()
        else:
            pl.when(only)(take)

    ends = jnp.logical_not(middle)

    tile = length // 4
    kept[0].wait()
    own_here(CLASS_A)
    own_far(CLASS_A, 0)
    own_here(CLASS_OUT)
    own_far(CLASS_OUT, 0)

    @pl.loop(0, 4)
    def _(t):
        rows = pl.ds(pl.multiple_of(t * tile, tile), tile)
        value = xin[rows, :].astype(f32)
        value = value * value
        total = value[:, :128]
        for c in range(1, half // 128):
            total = total + value[:, c * 128 : (c + 1) * 128]
        ssq_out[rows, :] = total

    ssq_move = remote(ssq_out, ssq_in, ssq_sem.at[0], ssq_sem.at[1], partner)
    ssq_move.start()
    ssq_move.wait_recv()
    small[0].wait()
    own_half = pl.multiple_of(core * half, 128)

    @pl.loop(0, 4)
    def _(t):
        rows = pl.ds(pl.multiple_of(t * tile, tile), tile)
        total = jnp.sum(ssq_out[rows, :] + ssq_in[rows, :], axis=-1, keepdims=True)
        scale = lax.rsqrt(total / width + EPS)
        value = xin[rows, :].astype(f32) * scale * gain_ref[:, pl.ds(own_half, half)]
        x[pl.ds(pl.multiple_of(place * length + t * tile, tile), tile), pl.ds(own_half, half)] = (
            value.astype(bf16)
        )

    def place_at(d):
        across = lax.rem(lax.rem(place, 2) + lax.rem(d, 2), 2)
        return across + 2 * lax.rem(lax.div(place, 2) + lax.div(d, 2), 2)

    def span_rows(s):
        return pl.ds(pl.multiple_of(s * length, 128), length)

    def piece(d, which):
        return x.at[
            span_rows(flipped(place, d)),
            pl.ds(pl.multiple_of(core * half + which * quarter, 128), quarter),
        ]

    tokens = {}

    def token_landed(which, d):
        return tok_recv.at[4] if d == 3 else tok_recv.at[which * 2 + d - 1]

    def send_piece(which, d_from, hop):
        d_there = d_from + hop
        tokens[(which, d_there)] = remote(
            piece(d_from, which), piece(d_from, which),
            tok_send.at[0], token_landed(which, d_there), (chips[hop], core),
        )
        tokens[(which, d_there)].start()

    def send_half(d):
        block = x.at[span_rows(flipped(place, d)), pl.ds(own_half, half)]
        remote(block, block, half_send.at[0], half_recv.at[d], partner).start()

    send_piece(0, 0, 1)
    send_piece(1, 0, 2)
    send_piece(1, 0, 1)
    send_piece(0, 0, 2)
    send_half(0)

    for d in range(1, group):
        near_block(CLASS_A, d).wait_recv()
        own_far(CLASS_A, d)

    for copy in small[1:]:
        copy.wait()
    for copy in rate_moves:
        copy.wait_recv()
    rates[place] = rate_pack[0]
    for s in range(group):
        for part in range(2):
            cums[s * 8 : s * 8 + rate_rows, part * length // 2 : (part + 1) * length // 2] = rates[
                s, part * rate_rows : (part + 1) * rate_rows, :
            ]
        cums[s * 8 + rate_rows : s * 8 + 8, :] = jnp.zeros((8 - rate_rows, length), f32)
    lanes = lax.broadcasted_iota(jnp.int32, (group * 8, length), 1)
    kinds = lax.rem(lax.broadcasted_iota(jnp.int32, (group * 8, length), 0), 8)
    running = cums[...] * LOG2E
    step = 1
    while step < length:
        ahead = jnp.where(lanes >= step, pltpu.roll(running, step, 1), 0.0)
        behind = jnp.where(lanes < length - step, pltpu.roll(running, length - step, 1), 0.0)
        running = running + jnp.where(kinds < heads, ahead, behind)
        step *= 2
    cums[...] = running
    wide[...] = jnp.zeros_like(wide)
    first_head = lax.broadcasted_iota(jnp.int32, (length, ch), 1) < HEAD_DIM
    lane_in_head = lax.rem(lax.broadcasted_iota(jnp.int32, (length, ch), 1), HEAD_DIM)
    leading = lane_in_head < HEAD_DIM // 2

    @pl.loop(0, group)
    def _(s):
        sums = cums[pl.ds(pl.multiple_of(s * 8, 8), 8), :]
        wide[0:8, :] = sums
        columns = wide[...].T
        cf = [columns[:, h : h + 1] for h in range(heads)]
        rb = [columns[:, heads + h : heads + h + 1] for h in range(heads)]
        cf_wide = jnp.where(first_head, cf[0], cf[1])
        rb_wide = jnp.where(first_head, rb[0], rb[1])
        ef[s] = jnp.exp2(cf_wide)
        eb[s] = jnp.exp2(rb_wide)
        kf[s] = jnp.exp2(cf_wide[length - 1 : length, :] - cf_wide)
        kb[s] = jnp.exp2(rb_wide[0:1, :] - rb_wide)
        row_at = lax.broadcasted_iota(jnp.int32, (length, length), 0)
        col_at = lax.broadcasted_iota(jnp.int32, (length, length), 1)
        for h in range(heads):
            spread = jnp.where(
                col_at <= row_at, cf[h] - sums[h : h + 1, :], rb[h] - sums[heads + h : heads + h + 1, :]
            )
            decay[s, h] = jnp.exp2(spread)
        turn = base_ref[s]
        cos_0, sin_0 = turn[0:1, :], turn[1:2, :]
        cos_i, sin_i = turn_ref[0], turn_ref[1]
        cosines[s] = cos_0 * cos_i - sin_0 * sin_i
        angle_sine = sin_0 * cos_i + cos_0 * sin_i
        sines[s] = jnp.where(leading, -angle_sine, angle_sine)

    def out_piece(r, d, which):
        start = pl.multiple_of((source_plane(r) * group + flipped(place, d)) * out_cols, 128)
        return wo.at[core, pl.ds(which * side_rows, side_rows), pl.ds(start, out_cols)]

    def out_move(r, which, d_there, hop):
        block = out_piece(r, d_there - hop, which)
        return remote(
            block, block, wo_send.at[0], out_sem(r, which, d_there),
            (chips[hop], core),
        )

    def out_sem(r, which, d):
        first = (which, d) == (0, 1)
        return wo_recv.at[r, 0 if first else 1 if (which, d) == (1, 2) else 2]

    def out_landed(r, which, d):
        block = out_piece(r, d, which)
        remote(block, block, wo_send.at[0], out_sem(r, which, d), partner).wait_recv()

    def spread_out(r):
        for which, hop in ((0, 1), (1, 2), (1, 1), (0, 2)):
            out_move(r, which, hop, hop).start()

    def relay_out(r):
        out_landed(r, 0, 1)
        out_move(r, 0, 3, 2).start()
        out_landed(r, 1, 2)
        out_move(r, 1, 3, 1).start()

    def finish_out(r):
        pieces = 1 if r == 1 else 2
        block = wo.at[core, :, pl.ds(0, pieces * out_cols)]
        remote(block, block, wo_send.at[0], wo_recv.at[r, 2], partner).wait_recv()
        if r == 1:
            out_landed(r, 0, 1)
            out_landed(r, 1, 2)

    def part_at(r):
        return pl.ds(pl.multiple_of(source_plane(r) * part_cols, 128), part_cols)

    def out_block(r, d):
        start = pl.multiple_of((source_plane(r) * group + flipped(place, d)) * out_cols, 128)
        return pl.ds(start, out_cols)

    def mate_copy(cols, i):
        block = wo.at[core, :, cols]
        return remote(block, block, mate_send.at[0], mate_recv.at[i], partner)

    def mate_here(cols, i):
        block = wo.at[1 - core, :, cols]
        remote(block, block, mate_send.at[0], mate_recv.at[i], partner).wait_recv()

    def wait_half(d):
        block = x.at[
            span_rows(flipped(place, d)), pl.ds(pl.multiple_of((1 - core) * half, 128), half)
        ]
        remote(block, block, half_send.at[0], half_recv.at[d], partner).wait_recv()

    for d in range(group):
        arrive(CLASS_A, 1, middle, (d,))
        arrive(CLASS_A, 2, middle, (d,))
    arrive(CLASS_OUT, 1, middle)
    for d in range(1, group):
        near_block(CLASS_B, d).wait_recv()
    own_here(CLASS_B)

    @pl.when(ends)
    def _():
        for d in range(group):
            own_far(CLASS_B, d)

    tokens[(0, 1)].wait_recv()
    send_piece(0, 1, 2)
    tokens[(1, 2)].wait_recv()
    send_piece(1, 2, 1)
    spread_out(0)
    arrive(CLASS_OUT, 1, ends)
    spread_out(1)
    arrive(CLASS_A, 3, middle)
    arrive(CLASS_OUT, 2, middle)

    @pl.when(middle)
    def _():
        for d in range(group):
            own_far(CLASS_B, d)

    tokens[(1, 1)].wait_recv()
    send_half(1)
    tokens[(0, 2)].wait_recv()
    send_half(2)
    for r in range(1, planes):
        arrive(CLASS_A, r, ends)
    arrive(CLASS_OUT, 3, middle)
    arrive(CLASS_B, 1, middle)
    wait_half(0)

    same_head = (
        lax.div(lax.broadcasted_iota(jnp.int32, (ch, ch), 0), HEAD_DIM)
        == lax.div(lax.broadcasted_iota(jnp.int32, (ch, ch), 1), HEAD_DIM)
    )

    def one_span(s):
        rows = span_rows(s)
        held = jnp.dot(x[rows, :], w[:, 0:col_a], preferred_element_type=f32)
        cosine, sine = cosines[s], sines[s]

        def turned(value):
            value = value.astype(bf16).astype(f32)
            other = jnp.where(
                leading,
                pltpu.roll(value, ch - HEAD_DIM // 2, 1),
                pltpu.roll(value, HEAD_DIM // 2, 1),
            )
            return value * cosine + other * sine

        rk = (turned(held[:, 0:ch]) * HEAD_DIM ** (-0.5)).astype(bf16).astype(f32)
        rq = turned(held[:, ch : 2 * ch]).astype(bf16)
        value = held[:, 2 * ch : 3 * ch].astype(bf16)
        rq_buf[s] = rq
        v_buf[s] = value
        gate_buf[s] = held[:, 3 * ch : 4 * ch].astype(bf16)
        value_wide = value.astype(f32)
        found = None
        for h in range(heads):
            in_head = first_head if h == 0 else jnp.logical_not(first_head)
            key_head = jnp.where(in_head, rk, 0.0).astype(bf16)
            value_head = jnp.where(in_head, value_wide, 0.0).astype(bf16)
            scores = lax.dot_general(
                rq, key_head, (((1,), (1,)), ((), ())), preferred_element_type=f32
            )
            probs = (scores * decay[s, h]).astype(bf16)
            part = jnp.dot(probs, value_head, preferred_element_type=f32)
            found = part if found is None else found + part
        loc[s] = found
        for table, target in ((kf, state_f), (kb, state_b)):
            keys = (rk * table[s]).astype(bf16)
            state = lax.dot_general(
                keys, value, (((0,), (0,)), ((), ())), preferred_element_type=f32
            )
            target[s] = jnp.where(same_head, state, 0.0)

    halo_rows = 16
    halo_at = (all_rows, all_rows + halo_rows)

    def halo_move(way):
        cols = pl.ds(own_half, half)
        source = x.at[pl.ds((all_rows - halo_rows) * (1 - way), halo_rows), cols]
        return remote(
            source, x.at[pl.ds(halo_at[way], halo_rows), cols],
            halo_send.at[way], halo_recv.at[way], (own + group if way == 0 else own - group, core),
        )

    def halo_pass(way):
        block = x.at[pl.ds(halo_at[way], halo_rows), pl.ds(own_half, half)]
        return remote(block, block, halo_send.at[2 + way], halo_recv.at[2 + way], partner)

    def halo_comes(way):
        return has_down if way == 0 else has_up

    blank = jnp.zeros((halo_rows, width), bf16)

    @pl.when(jnp.logical_not(has_down))
    def _():
        x[pl.ds(all_rows, halo_rows), :] = blank

    @pl.when(jnp.logical_not(has_up))
    def _():
        x[pl.ds(all_rows + halo_rows, halo_rows), :] = blank

    @pl.loop(0, group)
    def _(d):
        @pl.when(d == 1)
        def _():
            last = x.at[
                span_rows(flipped(place, 3)), pl.ds(pl.multiple_of(core * half, 128), half)
            ]
            remote(last, last, tok_send.at[0], token_landed(0, 3), partner).wait_recv()
            send_half(3)
            wait_half(1)

        @pl.when(d == 2)
        def _():
            wait_half(2)

        @pl.when(d == 3)
        def _():
            wait_half(3)
            pl.when(has_up)(lambda: halo_move(0).start())
            pl.when(has_down)(lambda: halo_move(1).start())
            relay_out(0)
            arrive(CLASS_OUT, 2, ends)
            spread_out(2)

        one_span(place_at(d))

    def scan_states(state, table, at, order, target):
        passed, inside, reach = jnp.zeros((ch, ch), f32), {}, {}
        over = jnp.ones((1, ch), f32)
        for s in order:
            inside[s], reach[s] = passed, over
            factor = table[s, at : at + 1, :]
            passed = factor * passed + state[s]
            over = over * factor
        folded = passed[0:HEAD_DIM, :]
        for h in range(1, heads):
            folded = folded + passed[h * HEAD_DIM : (h + 1) * HEAD_DIM, :]
        high = over.astype(bf16).astype(f32)
        coefficient = jnp.where(
            lax.broadcasted_iota(jnp.int32, (16, ch), 0) < 8, high, over - high
        )
        pack_out[target] = jnp.concatenate([folded, coefficient], axis=0).astype(bf16)
        return inside, reach

    ahead_in, ahead_reach = scan_states(state_f, ef, length - 1, range(group), 0)
    back_in, back_reach = scan_states(state_b, eb, 0, range(group)[::-1], 1)

    def pack_move(way, k):
        to = own + k * group if way == 0 else own - k * group
        return remote(
            pack_out.at[way], pack_in.at[way, k - 1],
            pack_send.at[way, k - 1], pack_recv.at[way, k - 1], (to, core),
        )

    def gives(way, k):
        return plane + k < planes if way == 0 else plane - k >= 0

    def takes(way, k):
        return gives(1 - way, k)

    for k in range(1, planes):
        for way in range(2):
            pl.when(gives(way, k))(lambda way=way, k=k: pack_move(way, k).start())
    arrive(CLASS_B, 2, middle)
    arrive(CLASS_B, 3, middle)

    def feature_cols(kind):
        return pl.ds(pl.multiple_of(kind * side_rows + place * ch, 128), ch)

    my_rows = length // 2

    def row_half(c):
        return pl.ds(pl.multiple_of(c * my_rows, 128), my_rows)

    def feature_move(kind, d, s, c):
        sender = ft_send.at[0]
        return remote(
            parts.at[kind, s, row_half(c)], feat.at[core, :, feature_cols(kind)],
            sender, ft_recv.at[kind, d], (base + s, c),
        )

    def feature_mate(kind):
        return remote(
            parts.at[kind, place, row_half(1 - core)], feat.at[core, :, feature_cols(kind)],
            ft_send.at[1], ft_recv.at[kind, 0], partner,
        )

    def own_features(kind):
        feature_mate(kind).start()
        feat[core, :, feature_cols(kind)] = parts[kind, place, row_half(core), :]

    finish_out(0)

    def pair_block(q):
        start = pl.multiple_of((q * group + flipped(place, 3)) * out_cols, 128)
        block = wo.at[core, :, pl.ds(start, out_cols)]
        return remote(
            block, block, pair_sem.at[0], pair_sem.at[1],
            ((plane + 1 - 2 * lax.rem(plane, 2)) * group + place, core),
        )

    pair_block(plane).start()
    mate_copy(part_at(0), 0).start()
    arrive(CLASS_OUT, 3, ends)
    spread_out(3)
    mate_copy(out_block(3, 0), 4).start()
    incoming = []
    for way in range(2):
        into[way] = jnp.zeros((HEAD_DIM, ch), f32)
        into[way + 2] = jnp.ones((HEAD_DIM, ch), f32)
        for k in range(1, planes):
            @pl.when(takes(way, k))
            def _(way=way, k=k):
                pack_move(way, k).wait_recv()
                pack = pack_in[way, k - 1].astype(f32)
                into[way] = into[way] + into[way + 2] * pack[0:HEAD_DIM, :]
                into[way + 2] = into[way + 2] * (
                    pack[HEAD_DIM : HEAD_DIM + 1, :] + pack[HEAD_DIM + 8 : HEAD_DIM + 9, :]
                )
        incoming.append(
            jnp.where(same_head, jnp.concatenate([into[way]] * heads, axis=0), 0.0)
        )
    for s in range(group):
        state_f[s] = ahead_in[s] + ahead_reach[s] * incoming[0]
        state_b[s] = back_in[s] + back_reach[s] * incoming[1]

    @pl.loop(0, group)
    def _(i):
        d = group - 1 - i
        s = place_at(d)
        query = rq_buf[s]
        mix = (
            loc[s]
            + ef[s] * jnp.dot(query, state_f[s].astype(bf16), preferred_element_type=f32)
            + eb[s] * jnp.dot(query, state_b[s].astype(bf16), preferred_element_type=f32)
        )
        squares = mix * mix
        first = jnp.sum(jnp.where(first_head, squares, 0.0), axis=-1, keepdims=True)
        second = jnp.sum(jnp.where(first_head, 0.0, squares), axis=-1, keepdims=True)
        scale = lax.rsqrt(jnp.where(first_head, first, second) / HEAD_DIM + EPS)
        gate = gate_buf[s].astype(f32)
        parts[1, s] = (
            gate / (1.0 + jnp.exp(-gate)) * (mix * scale * head_gain_ref[:, place_cols])
        ).astype(bf16)

        @pl.when(d > 0)
        def _():
            for c in range(2):
                feature_move(1, d, s, c).start()

    own_features(1)

    for way in range(2):
        @pl.when(halo_comes(way))
        def _(way=way):
            halo_move(way).wait_recv()
            halo_pass(way).start()
    relay_out(2)
    arrive(CLASS_B, 1, ends)
    arrive(CLASS_B, 2, ends)
    for way in range(2):
        pl.when(halo_comes(way))(lambda way=way: halo_pass(way).wait_recv())
    depth = group * rows_in
    most = (planes - 1) * depth
    early = pl.multiple_of(top * depth, 128)
    late = pl.multiple_of((1 - top) * most, 128)
    blocks = 5
    block = (all_rows + 2 * halo_rows) // blocks

    @pl.loop(0, blocks)
    def _(t):
        rows = pl.ds(pl.multiple_of(t * block, 16), block)
        acc[rows, :] = jnp.dot(
            x[rows, pl.ds(early, most)], w[pl.ds(early, most), col_a : col_a + col_b],
            preferred_element_type=f32,
        )

    relay_out(3)
    finish_out(1)
    for d in range(group - 1):
        mate_copy(out_block(1, d), 1).start()

    def hand_over(r):
        finish_out(r)
        mate_copy(part_at(r), r + 1).start()

    arrive(CLASS_B, 3, ends)

    spans_at = [s * length - halo_rows for s in range(1, group)] + [all_rows]
    late_w = w[pl.ds(late, depth), col_a : col_a + col_b]
    near_rows = jnp.concatenate(
        [x[at : at + 2 * halo_rows, pl.ds(late, depth)] for at in spans_at], axis=0
    )
    near_sums = jnp.concatenate(
        [acc[at : at + 2 * halo_rows, 0 : 2 * ch] for at in spans_at], axis=0
    )

    def inner_product(held):
        held = held.astype(bf16).astype(f32)
        return (held[:, 0:ch] * held[:, ch : 2 * ch]).astype(bf16).astype(f32)

    edge_values = inner_product(
        near_sums + jnp.dot(near_rows, late_w[:, 0 : 2 * ch], preferred_element_type=f32)
    )
    for s in range(group):
        before = ((s - 1) % group) * 2 * halo_rows + halo_rows - 1
        after = s * 2 * halo_rows + halo_rows
        edges[s, 0:1, :] = edge_values[before : before + 1, :]
        edges[s, 1:2, :] = edge_values[after : after + 1, :]
    row_of = lax.broadcasted_iota(jnp.int32, (length, ch), 0)

    @pl.loop(0, group)
    def _(i):
        d = 3 - 2 * i + 3 * lax.div(i, 2)
        s = place_at(d)
        rows = span_rows(s)
        held = acc[rows, :] + jnp.dot(
            x[rows, pl.ds(late, depth)], w[pl.ds(late, depth), col_a : col_a + col_b],
            preferred_element_type=f32,
        )
        inner = inner_product(held)
        before = jnp.where(row_of == 0, edges[s, 0:1, :], pltpu.roll(inner, 1, 0))
        after = jnp.where(row_of == length - 1, edges[s, 1:2, :], pltpu.roll(inner, length - 1, 0))
        near_sum = (
            taps_ref[0:1, place_cols] * before
            + taps_ref[1:2, place_cols] * inner
            + taps_ref[2:3, place_cols] * after
        )
        parts[0, s] = (held[:, 2 * ch : 3 * ch].astype(bf16).astype(f32) * near_sum).astype(bf16)

        @pl.when(d > 0)
        def _():
            for c in range(2):
                feature_move(0, d, s, c).start()

        pl.when(jnp.logical_and(i == 1, ends))(lambda: hand_over(2))

    own_features(0)

    def features_here(kind, places):
        for d in places:
            rows = my_rows if d == 0 else length
            block = parts.at[0, 0, pl.ds(0, rows)]
            remote(block, block, ft_send.at[0], ft_recv.at[kind, d], partner).wait_recv()

    def product(rows, r):
        total = None
        for c in range(2):
            part = jnp.dot(feat[c, :, rows], wo[c, rows, part_at(r)], preferred_element_type=f32)
            total = part if total is None else total + part
        return total

    def retention_product(r):
        decay[r, 0, 0:my_rows, :] = product(pl.ds(side_rows, side_rows), r)

    pair_rows = 2 * ch
    own_pair = lax.div(place, 2)

    def conv_product(r, pair):
        at = pl.ds(pl.multiple_of(pair * pair_rows, 128), pair_rows)
        return decay[r, 0, 0:my_rows, :] + product(at, r)

    features_here(1, range(group))
    mate_here(part_at(0), 0)
    retention_product(0)
    pl.when(middle)(lambda: hand_over(2))
    finish_out(3)
    for d in range(1, group):
        mate_copy(out_block(3, d), 4).start()
    mate_here(part_at(2), 3)
    retention_product(2)
    pair_block(source_plane(1)).wait_recv()
    mate_copy(out_block(1, 3), 2).start()
    mate_here(part_at(3), 4)
    retention_product(3)
    mate_here(pl.ds(0, (group - 1) * out_cols), 1)
    mate_here(out_block(1, 3), 2)
    retention_product(1)

    for copy in rate_moves:
        copy.wait_send()
    ssq_move.wait_send()

    def sent(block, semaphore, landed):
        remote(block, block, semaphore, landed, partner).wait_send()

    sent(
        x.at[pl.ds(0, (group - 1) * length), pl.ds(0, 2 * quarter)], tok_send.at[0],
        tok_recv.at[0],
    )
    sent(x.at[pl.ds(0, all_rows), pl.ds(0, half)], half_send.at[0], half_recv.at[0])
    sent(
        wo.at[core, :, pl.ds(0, ((group - 1) * planes - 1) * out_cols)], wo_send.at[0],
        wo_recv.at[0, 0],
    )
    pair_block(plane).wait_send()
    sent(
        w.at[pl.ds(0, (group - 1) * rows_in), :], near_send.at[0], near_recv.at[0, 0]
    )
    sent(wo.at[core], mate_send.at[0], mate_recv.at[0])
    pl.when(has_up)(lambda: halo_move(0).wait_send())
    pl.when(has_down)(lambda: halo_move(1).wait_send())
    for way in range(2):
        pl.when(halo_comes(way))(lambda way=way: halo_pass(way).wait_send())
    for k in range(1, planes):
        for way in range(2):
            pl.when(gives(way, k))(lambda way=way, k=k: pack_move(way, k).wait_send())
    for kind in range(3):
        for units in range(1, planes):
            pl.when(plane == units - 1)(functools.partial(far_sent, kind, 0, units))
            pl.when(plane == planes - units)(functools.partial(far_sent, kind, 1, units))

    features_here(0, (2, 3))
    for r in range(planes):
        decay[r, 0, 0:my_rows, :] = conv_product(r, 1 - own_pair)
    features_here(0, (0, 1))
    for r in range(planes):
        out_ref[:, part_at(r)] = conv_product(r, own_pair).astype(bf16)
    sent(parts.at[:, pl.ds(0, group - 1)], ft_send.at[0], ft_recv.at[0, 0])
    sent(parts.at[:, 0, pl.ds(0, my_rows)], ft_send.at[1], ft_recv.at[0, 0])


def turn_tables(spans, length, channels):
    half_dim = HEAD_DIM // 2
    frequency = THETA ** (-2.0 * (np.arange(channels) % half_dim) / HEAD_DIM)
    inner = np.arange(length)[:, None] * frequency
    outer = (np.arange(spans) * length)[:, None] * frequency
    turn = np.stack([np.cos(inner), np.sin(inner)])
    start = np.zeros((spans, 8, channels))
    start[:, 0], start[:, 1] = np.cos(outer), np.sin(outer)
    return turn.astype(np.float32), start.astype(np.float32)


def mixer(planes, group, arrays):
    (
        tokens, norm_gain, outer_gate, inner_gate, conv_input, query_proj, key_proj, value_proj,
        out_gate, conv_taps, log_decay, head_gain, conv_output, retention_output,
    ) = arrays
    f32, bf16 = jnp.float32, jnp.bfloat16
    length, half = tokens.shape
    width = 2 * half
    ch = outer_gate.shape[1] // group
    heads = ch // HEAD_DIM
    rows, side = group * length, conv_output.shape[0]
    turn, start = turn_tables(planes * group, length, ch)
    dma = pltpu.SemaphoreType.DMA
    vmem, held = pl.BlockSpec(memory_space=pltpu.VMEM), pl.BlockSpec(memory_space=pltpu.HBM)
    v = pltpu.VMEM
    result = jax.ShapeDtypeStruct((length // 2, width), bf16)
    table = v((group, length, ch), f32)
    return pl.pallas_call(
        functools.partial(mixer_kernel, planes, group),
        out_shape=result,
        in_specs=[held] * 16,
        out_specs=vmem,
        scratch_shapes=[
            v((1, width), f32), v(conv_taps.shape, f32), v((1, head_gain.shape[0]), f32), v(turn.shape, f32),
            v((group,) + start.shape[1:], f32),
            v((length, half), bf16), v((rows + 32, width), bf16), v((width, 7 * ch), bf16),
            v((2, 2 * side, width), bf16), v(log_decay.shape, f32),
            v((group, 4 * heads, length // 2), f32), v((group, 4 * heads, length // 2), f32),
            v((8 * group, length), f32), v((128, length), f32),
            v((length, 128), f32), v((length, 128), f32),
            table, table, v((group, heads, length, length), f32),
            table, table, table, table,
            v((group, length, ch), bf16), v((group, length, ch), bf16), v((group, length, ch), bf16),
            table, v((group, ch, ch), f32), v((group, ch, ch), f32),
            v((2, HEAD_DIM + 16, ch), bf16), v((2, planes - 1, HEAD_DIM + 16, ch), bf16),
            v((4, HEAD_DIM, ch), f32),
            v((rows + 32, 3 * ch), f32), v((group, 8, ch), f32),
            v((2, group, length, ch), bf16), v((2, length // 2, 2 * side), bf16),
            dma((10,)), dma((1,)), dma((2, group - 1)), dma((1,)), dma((group - 1,)), dma((2,)),
            dma((1,)), dma((5,)), dma((1,)), dma((group,)),
            dma((3, 2)), dma((2, planes - 1, group)), dma((planes - 1,)),
            dma((1,)), dma((planes, 3)), dma((1,)), dma((5,)), dma((2,)), dma((4,)), dma((4,)),
            dma((2, planes - 1)), dma((2, planes - 1)), dma((2,)), dma((2, group)),
        ],
        compiler_params=pltpu.CompilerParams(
            collective_id=0, has_side_effects=True, vmem_limit_bytes=50 * 2**20
        ),
    )(
        *(
            pltpu.with_memory_space_constraint(source, pltpu.HBM)
            for source in (
                tokens, key_proj, query_proj, value_proj, out_gate, inner_gate, conv_input,
                outer_gate, conv_output, retention_output, log_decay, norm_gain.reshape(1, -1),
                conv_taps, head_gain.reshape(1, -1), jnp.asarray(turn), jnp.asarray(start),
            )
        )
    )


LANES = 128

def plan(*arrays):
    spans, cores = lax.axis_size("sp"), lax.axis_size("tp")
    group = arrays[2].shape[1] // LANES
    planes = spans // group
    fits = (
        cores == 2
        and group == 4
        and planes * group == spans
        and planes == 2 * cores
        and arrays[0].shape[1] == 2 * group * arrays[2].shape[0]
    )
    return mixer(planes, group, arrays) if fits else local(*arrays)


def solution(mesh):
    return jax.shard_map(
        plan,
        mesh=mesh,
        in_specs=(
            P("sp", "tp"),
            P(),
            P("sp", "tp"),
            P("sp", "tp"),
            P("sp", "tp"),
            P("sp", "tp"),
            P("sp", "tp"),
            P("sp", "tp"),
            P("sp", "tp"),
            P(None, "tp"),
            P(None, "tp", "sp"),
            P("tp"),
            P("tp", "sp"),
            P("tp", "sp"),
        ),
        out_specs=P(("sp", "tp"), None),
        check_vma=False,
    )
```

```python
import jax
import functools
import jax.numpy as jnp
import numpy as np
from jax import lax
from jax.experimental import pallas as pl
from jax.experimental.pallas import tpu as pltpu
from jax.sharding import PartitionSpec as P

HEAD_DIM = 64


EPS = 1e-06
THETA = 10000.0


def with_halo(shard, sides, width):
    for axis, dim in sides:
        size, length = (lax.axis_size(axis), shard.shape[dim])
        up = [(i, (i + 1) % size) for i in range(size - 1)]
        down = [(j, i) for i, j in up]
        last = lax.slice_in_dim(shard, length - width, length, axis=dim)
        first = lax.slice_in_dim(shard, 0, width, axis=dim)
        before = lax.ppermute(last, axis, up)
        after = lax.ppermute(first, axis, down)
        shard = jnp.concatenate([before, shard, after], axis=dim)
    return shard


def rotate(field_in, position_list):
    half_dim = field_in.shape[-1] // 2
    frequency = jnp.exp(
        -jnp.log(THETA) * jnp.arange(half_dim, dtype=jnp.float32) * (2.0 / field_in.shape[-1])
    )
    angles = position_list.astype(jnp.float32)[:, None, None] * frequency
    cosine = jnp.cos(angles)
    sine_part = jnp.sin(angles)
    leading = field_in[..., :half_dim]
    trailing = field_in[..., half_dim:]
    return jnp.concatenate(
        [leading * cosine - trailing * sine_part, leading * sine_part + trailing * cosine], axis=-1
    )


def conv_branch(outer_rows, inner_rows, conv_values, conv_taps):
    inner_value = (inner_rows.astype(jnp.float32) * conv_values.astype(jnp.float32)).astype(
        jnp.bfloat16
    )
    padded = with_halo(inner_value, (("sp", 0),), 1).astype(jnp.float32)
    convolved = conv_taps[0] * padded[:-2] + conv_taps[1] * padded[1:-1] + conv_taps[2] * padded[2:]
    return (outer_rows.astype(jnp.float32) * convolved).astype(jnp.bfloat16)


def span_parts(query_rows, key_rows, value_rows, log_rates):
    length = query_rows.shape[0]
    forward_cum = jnp.cumsum(log_rates[0], axis=-1)
    backward_cum = jnp.flip(jnp.cumsum(jnp.flip(log_rates[1], -1), axis=-1), -1)
    row_index = lax.broadcasted_iota(jnp.int32, (length, length), 0)
    col_index = lax.broadcasted_iota(jnp.int32, (length, length), 1)
    lower_part = (col_index <= row_index)[None]
    spread = jnp.where(
        lower_part,
        forward_cum[:, :, None] - forward_cum[:, None, :],
        backward_cum[:, :, None] - backward_cum[:, None, :],
    )
    scores = jnp.einsum("ihe,jhe->hij", query_rows, key_rows, preferred_element_type=jnp.float32)
    weighted = (scores * jnp.exp(spread)).astype(jnp.bfloat16)
    local_part = jnp.einsum(
        "hij,jhe->ihe", weighted, value_rows, preferred_element_type=jnp.float32
    )
    key_wide = key_rows.astype(jnp.float32)
    forward_keys = (key_wide * jnp.exp(forward_cum[:, -1:] - forward_cum).T[:, :, None]).astype(
        jnp.bfloat16
    )
    backward_keys = (key_wide * jnp.exp(backward_cum[:, :1] - backward_cum).T[:, :, None]).astype(
        jnp.bfloat16
    )
    forward_state = jnp.einsum(
        "jhd,jhe->hde", forward_keys, value_rows, preferred_element_type=jnp.float32
    )
    backward_state = jnp.einsum(
        "jhd,jhe->hde", backward_keys, value_rows, preferred_element_type=jnp.float32
    )
    return (local_part, forward_cum, backward_cum, forward_state, backward_state)


def retention_branch(query_rows, key_rows, value_rows, gate_rows, log_decay, head_gain, offsets):
    row_count = query_rows.shape[0]
    head_count = query_rows.shape[1] // HEAD_DIM
    shape_heads = (row_count, head_count, HEAD_DIM)
    rotated_query = rotate(query_rows.astype(jnp.float32).reshape(shape_heads), offsets).astype(
        jnp.bfloat16
    )
    rotated_key = (
        rotate(key_rows.astype(jnp.float32).reshape(shape_heads), offsets) * HEAD_DIM ** (-0.5)
    ).astype(jnp.bfloat16)
    local_part, forward_cum, backward_cum, forward_state, backward_state = span_parts(
        rotated_query, rotated_key, value_rows.reshape(shape_heads), log_decay
    )
    forward_total = forward_cum[:, -1]
    backward_total = backward_cum[:, 0]
    totals = lax.all_gather(
        jnp.stack([forward_total, backward_total])[None], "sp", axis=0, tiled=True
    )
    inclusive = jnp.cumsum(totals, axis=0)
    exclusive = inclusive - totals
    own_index = lax.axis_index("sp")
    own_inclusive = lax.dynamic_index_in_dim(inclusive, own_index, 0, keepdims=False)
    own_exclusive = lax.dynamic_index_in_dim(exclusive, own_index, 0, keepdims=False)
    pieces = (
        lax.all_gather(forward_state[None], "sp", axis=0, tiled=True),
        lax.all_gather(backward_state[None], "sp", axis=0, tiled=True),
    )
    piece_count = pieces[0].shape[0]
    span_index = lax.iota(jnp.int32, piece_count)
    forward_weight = jnp.where(
        (span_index < own_index)[:, None],
        jnp.exp(jnp.minimum(own_exclusive[0] - inclusive[:, 0], 0.0)),
        0.0,
    )
    backward_weight = jnp.where(
        (span_index > own_index)[:, None],
        jnp.exp(jnp.minimum(exclusive[:, 1] - own_inclusive[1], 0.0)),
        0.0,
    )
    into_forward = jnp.einsum(
        "nh,nhde->hde", forward_weight, pieces[0], precision=lax.Precision.HIGHEST
    )
    into_backward = jnp.einsum(
        "nh,nhde->hde", backward_weight, pieces[1], precision=lax.Precision.HIGHEST
    )
    forward_part = jnp.einsum(
        "ihd,hde->ihe",
        rotated_query,
        into_forward.astype(jnp.bfloat16),
        preferred_element_type=jnp.float32,
    )
    backward_part = jnp.einsum(
        "ihd,hde->ihe",
        rotated_query,
        into_backward.astype(jnp.bfloat16),
        preferred_element_type=jnp.float32,
    )
    mixed_heads = (
        local_part
        + jnp.exp(forward_cum).T[:, :, None] * forward_part
        + jnp.exp(backward_cum).T[:, :, None] * backward_part
    )
    scaled = mixed_heads * lax.rsqrt(
        jnp.mean(mixed_heads * mixed_heads, axis=-1, keepdims=True) + EPS
    )
    scaled = scaled * head_gain.reshape(head_count, HEAD_DIM)
    return (
        jax.nn.silu(gate_rows.astype(jnp.float32))
        * scaled.reshape(row_count, head_count * HEAD_DIM)
    ).astype(jnp.bfloat16)


def local(
    tokens,
    norm_gain,
    outer_gate,
    inner_gate,
    conv_input,
    query_proj,
    key_proj,
    value_proj,
    out_gate,
    conv_taps,
    log_decay,
    head_gain,
    conv_output,
    retention_output,
):
    whole = lax.all_gather(tokens, "tp", axis=1, tiled=True)
    wide = whole.astype(jnp.float32)
    normed = (
        wide * lax.rsqrt(jnp.mean(wide * wide, axis=-1, keepdims=True) + EPS) * norm_gain
    ).astype(jnp.bfloat16)
    row_count = normed.shape[0]
    offsets = lax.axis_index("sp") * row_count + lax.iota(jnp.int32, row_count)
    gathered = (
        lax.all_gather(outer_gate, "sp", axis=0, tiled=True),
        lax.all_gather(inner_gate, "sp", axis=0, tiled=True),
        lax.all_gather(conv_input, "sp", axis=0, tiled=True),
        lax.all_gather(query_proj, "sp", axis=0, tiled=True),
        lax.all_gather(key_proj, "sp", axis=0, tiled=True),
        lax.all_gather(value_proj, "sp", axis=0, tiled=True),
        lax.all_gather(out_gate, "sp", axis=0, tiled=True),
        lax.all_gather(conv_output, "sp", axis=1, tiled=True),
        lax.all_gather(retention_output, "sp", axis=1, tiled=True),
    )
    projected = [
        jnp.dot(normed, weight, preferred_element_type=jnp.float32).astype(jnp.bfloat16)
        for weight in gathered[:7]
    ]
    conv_out = conv_branch(projected[0], projected[1], projected[2], conv_taps)
    ret_out = retention_branch(
        projected[3], projected[4], projected[5], projected[6], log_decay, head_gain, offsets
    )
    conv_weight = gathered[7]
    ret_weight = gathered[8]
    return lax.psum_scatter(
        (
            jnp.dot(conv_out, conv_weight, preferred_element_type=jnp.float32)
            + jnp.dot(ret_out, ret_weight, preferred_element_type=jnp.float32)
        ).astype(jnp.bfloat16),
        "tp",
        scatter_dimension=0,
        tiled=True,
    )


def flipped(place, d):
    if d == 0:
        return place
    if d == 1:
        return place + 1 - 2 * lax.rem(place, 2)
    if d == 2:
        return place + 2 - 4 * lax.rem(lax.div(place, 2), 2)
    return 3 - place


LOG2E = 1.4426950408889634
CLASS_A, CLASS_B, CLASS_OUT = 0, 1, 2


def mixer_kernel(
    planes, group,
    tok_ref, key_w, query_w, value_w, gate_w, inner_w, conv_w, outer_w,
    cout_ref, rout_ref, rate_in, gain_in, taps_in, head_gain_in, turn_in, base_in,
    out_ref, gain_ref, taps_ref, head_gain_ref, turn_ref, base_ref,
    xin, x, w, wo, rate_own, rate_pack, rates, cums, wide, ssq_out, ssq_in, cosines, sines, decay,
    ef, eb, kf, kb, rq_buf, v_buf, gate_buf, loc, state_f, state_b, pack_out, pack_in, into,
    acc, edges, parts, feat,
    own_sem, near_send, near_recv, rate_send, rate_recv, ssq_sem,
    tok_send, tok_recv, half_send, half_recv, far_send, far_recv, out_recv,
    wo_send, wo_recv, mate_send, mate_recv, pair_sem, halo_send, halo_recv, pack_send, pack_recv,
    ft_send, ft_recv,
):
    f32, bf16 = jnp.float32, jnp.bfloat16
    own, core = lax.axis_index("sp"), lax.axis_index("tp")
    place, plane = lax.rem(own, group), lax.div(own, group)
    base = plane * group
    length, half = tok_ref.shape
    width = 2 * half
    quarter = half // 2
    rows_in = key_w.shape[0]
    ch = key_w.shape[1] // group
    heads = ch // HEAD_DIM
    all_rows = group * length
    side_rows = cout_ref.shape[0]
    out_cols = cout_ref.shape[1]
    part_cols = group * out_cols
    col_a, col_b = 4 * ch, 3 * ch
    has_up, has_down = plane < planes - 1, plane > 0
    middle = jnp.logical_and(has_up, has_down)
    top = lax.div(plane, planes // 2)
    mesh_id = pl.DeviceIdType.MESH
    chips = [base + flipped(place, d) for d in range(group)]
    partner = (own, 1 - core)
    weights = (key_w, query_w, value_w, gate_w, inner_w, conv_w, outer_w)

    def local_copy(source, target, i):
        return pltpu.make_async_copy(source, target, own_sem.at[i])

    def remote(source, target, send, recv, device):
        return pltpu.make_async_remote_copy(
            src_ref=source, dst_ref=target, send_sem=send, recv_sem=recv,
            device_id=device, device_id_type=mesh_id,
        )

    own_rows = pl.ds(pl.multiple_of(own * rows_in, 128), rows_in)
    own_cols = pl.ds(pl.multiple_of(own * out_cols, 128), out_cols)
    kept = [local_copy(tok_ref, xin, 0), local_copy(rate_in, rate_own, 1)]
    for j, source in enumerate(weights):
        kept.append(
            local_copy(
                source.at[:, pl.ds(pl.multiple_of(place * ch, 128), ch)],
                w.at[own_rows, pl.ds(j * ch, ch)], 2 + j // 4,
            )
        )
    kept.append(local_copy(cout_ref, wo.at[core, pl.ds(0, side_rows), own_cols], 4))
    kept.append(local_copy(rout_ref, wo.at[core, pl.ds(side_rows, side_rows), own_cols], 4))
    place_cols = pl.ds(pl.multiple_of(place * ch, 128), ch)
    small = [
        local_copy(gain_in, gain_ref, 5),
        local_copy(taps_in, taps_ref, 6),
        local_copy(head_gain_in, head_gain_ref, 7),
        local_copy(turn_in, turn_ref, 8),
        local_copy(base_in.at[pl.ds(base, group)], base_ref, 9),
    ]
    for copy in kept + small:
        copy.start()

    def class_cols(kind):
        return pl.ds(0, col_a) if kind == CLASS_A else pl.ds(col_a, col_b)

    def own_here(kind):
        block = wo.at[core, :, own_cols] if kind == CLASS_OUT else w.at[own_rows, class_cols(kind)]
        local_copy(block, block, 2 + kind).wait()

    barrier = pltpu.get_barrier_semaphore()

    def greet(target):
        pl.semaphore_signal(barrier, inc=1, device_id=target, device_id_type=mesh_id)

    for d in range(1, group):
        for c in range(2):
            greet((chips[d], c))
    greet(partner)
    for k in range(1, planes):
        greet((lax.rem(own + k * group, planes * group), core))
    pl.semaphore_wait(barrier, 2 * group + planes - 2)

    def send_near(j, d):
        to = flipped(place, d)
        remote(
            weights[j].at[:, pl.ds(pl.multiple_of(to * ch, 128), ch)],
            w.at[own_rows, pl.ds(j * ch, ch)],
            near_send.at[0], near_recv.at[j // 4, d - 1], (chips[d], core),
        ).start()

    def near_block(kind, d):
        start = pl.multiple_of((base + flipped(place, d)) * rows_in, 128)
        block = w.at[pl.ds(start, rows_in), class_cols(kind)]
        return remote(
            block, block, near_send.at[0], near_recv.at[kind, d - 1], (chips[d], core)
        )

    for d in range(1, group):
        for j in range(4):
            send_near(j, d)

    rate_rows = 2 * heads
    kept[1].wait()
    rate_moves = []
    for d in range(group):
        to = flipped(place, d)
        for way in range(2):
            for h in range(heads):
                row = rate_own[way, pl.ds(heads * to + h, 1), :]
                for part in range(2):
                    rate_pack[d, pl.ds(part * rate_rows + way * heads + h, 1), :] = row[
                        :, part * length // 2 : (part + 1) * length // 2
                    ]
    for d in range(1, group):
        rate_moves.append(
            remote(
                rate_pack.at[d], rates.at[place], rate_send.at[0], rate_recv.at[d - 1],
                (chips[d], core),
            )
        )
    for copy in rate_moves:
        copy.start()
    for d in range(1, group):
        for j in range(4, 7):
            send_near(j, d)

    def far(kind, direction, q, d):
        if kind == CLASS_OUT:
            block = wo.at[
                core, :, pl.ds(pl.multiple_of((q * group + place) * out_cols, 128), out_cols)
            ]
        else:
            start = pl.multiple_of((q * group + flipped(place, d)) * rows_in, 128)
            block = w.at[pl.ds(start, rows_in), class_cols(kind)]
        to = plane + 1 - 2 * direction
        return remote(
            block, block, far_send.at[kind, direction], far_landed(kind, q, d, to),
            (own + group * (1 - 2 * direction), core),
        )

    def far_landed(kind, q, d, at):
        slot = q - (q > at).astype(jnp.int32)
        return out_recv.at[slot] if kind == CLASS_OUT else far_recv.at[kind, slot, d]

    def far_arrived(kind, q, d):
        if kind == CLASS_OUT:
            block = wo.at[
                core, :, pl.ds(pl.multiple_of((q * group + place) * out_cols, 128), out_cols)
            ]
        else:
            start = pl.multiple_of((q * group + flipped(place, d)) * rows_in, 128)
            block = w.at[pl.ds(start, rows_in), class_cols(kind)]
        remote(
            block, block, far_send.at[kind, 0], far_landed(kind, q, d, plane), partner
        ).wait_recv()

    def far_sent(kind, direction, units):
        if kind == CLASS_OUT:
            block, landed = wo.at[core, :, pl.ds(0, units * out_cols)], out_recv.at[0]
        else:
            block = w.at[pl.ds(0, units * group * rows_in), class_cols(kind)]
            landed = far_recv.at[kind, 0, 0]
        remote(block, block, far_send.at[kind, direction], landed, partner).wait_send()

    def places_of(kind):
        return 1 if kind == CLASS_OUT else group

    def own_far(kind, d):
        pl.when(has_up)(lambda: far(kind, 0, plane, d).start())
        pl.when(has_down)(lambda: far(kind, 1, plane, d).start())

    def source_plane(r):
        if r == 0:
            return plane
        if r == 1:
            return plane + 1 - 2 * lax.rem(plane, 2)
        return r + top * (planes - 1 - 2 * r)

    def arrive(kind, r, only=None, blocks=None):
        q = source_plane(r)

        def take():
            for d in range(places_of(kind)) if blocks is None else blocks:
                far_arrived(kind, q, d)
                pl.when(jnp.logical_and(q < plane, has_up))(
                    lambda d=d: far(kind, 0, q, d).start()
                )
                pl.when(jnp.logical_and(q > plane, has_down))(
                    lambda d=d: far(kind, 1, q, d).start()
                )

        if only is None:
            take()
        else:
            pl.when(only)(take)

    ends = jnp.logical_not(middle)

    tile = length // 4
    kept[0].wait()
    own_here(CLASS_A)
    own_far(CLASS_A, 0)
    own_here(CLASS_OUT)
    own_far(CLASS_OUT, 0)

    @pl.loop(0, 4)
    def _(t):
        rows = pl.ds(pl.multiple_of(t * tile, tile), tile)
        value = xin[rows, :].astype(f32)
        value = value * value
        total = value[:, :128]
        for c in range(1, half // 128):
            total = total + value[:, c * 128 : (c + 1) * 128]
        ssq_out[rows, :] = total

    ssq_move = remote(ssq_out, ssq_in, ssq_sem.at[0], ssq_sem.at[1], partner)
    ssq_move.start()
    ssq_move.wait_recv()
    small[0].wait()
    own_half = pl.multiple_of(core * half, 128)

    @pl.loop(0, 4)
    def _(t):
        rows = pl.ds(pl.multiple_of(t * tile, tile), tile)
        total = jnp.sum(ssq_out[rows, :] + ssq_in[rows, :], axis=-1, keepdims=True)
        scale = lax.rsqrt(total / width + EPS)
        value = xin[rows, :].astype(f32) * scale * gain_ref[:, pl.ds(own_half, half)]
        x[pl.ds(pl.multiple_of(place * length + t * tile, tile), tile), pl.ds(own_half, half)] = (
            value.astype(bf16)
        )

    def place_at(d):
        across = lax.rem(lax.rem(place, 2) + lax.rem(d, 2), 2)
        return across + 2 * lax.rem(lax.div(place, 2) + lax.div(d, 2), 2)

    def span_rows(s):
        return pl.ds(pl.multiple_of(s * length, 128), length)

    def piece(d, which):
        return x.at[
            span_rows(flipped(place, d)),
            pl.ds(pl.multiple_of(core * half + which * quarter, 128), quarter),
        ]

    tokens = {}

    def token_landed(which, d):
        return tok_recv.at[4] if d == 3 else tok_recv.at[which * 2 + d - 1]

    def send_piece(which, d_from, hop):
        d_there = d_from + hop
        tokens[(which, d_there)] = remote(
            piece(d_from, which), piece(d_from, which),
            tok_send.at[0], token_landed(which, d_there), (chips[hop], core),
        )
        tokens[(which, d_there)].start()

    def send_half(d):
        block = x.at[span_rows(flipped(place, d)), pl.ds(own_half, half)]
        remote(block, block, half_send.at[0], half_recv.at[d], partner).start()

    send_piece(0, 0, 1)
    send_piece(1, 0, 2)
    send_piece(1, 0, 1)
    send_piece(0, 0, 2)
    send_half(0)

    for d in range(1, group):
        near_block(CLASS_A, d).wait_recv()
        own_far(CLASS_A, d)

    for copy in small[1:]:
        copy.wait()
    for copy in rate_moves:
        copy.wait_recv()
    rates[place] = rate_pack[0]
    for s in range(group):
        for part in range(2):
            cums[s * 8 : s * 8 + rate_rows, part * length // 2 : (part + 1) * length // 2] = rates[
                s, part * rate_rows : (part + 1) * rate_rows, :
            ]
        cums[s * 8 + rate_rows : s * 8 + 8, :] = jnp.zeros((8 - rate_rows, length), f32)
    lanes = lax.broadcasted_iota(jnp.int32, (group * 8, length), 1)
    kinds = lax.rem(lax.broadcasted_iota(jnp.int32, (group * 8, length), 0), 8)
    running = cums[...] * LOG2E
    step = 1
    while step < length:
        ahead = jnp.where(lanes >= step, pltpu.roll(running, step, 1), 0.0)
        behind = jnp.where(lanes < length - step, pltpu.roll(running, length - step, 1), 0.0)
        running = running + jnp.where(kinds < heads, ahead, behind)
        step *= 2
    cums[...] = running
    wide[...] = jnp.zeros_like(wide)
    first_head = lax.broadcasted_iota(jnp.int32, (length, ch), 1) < HEAD_DIM
    lane_in_head = lax.rem(lax.broadcasted_iota(jnp.int32, (length, ch), 1), HEAD_DIM)
    leading = lane_in_head < HEAD_DIM // 2

    @pl.loop(0, group)
    def _(s):
        sums = cums[pl.ds(pl.multiple_of(s * 8, 8), 8), :]
        wide[0:8, :] = sums
        columns = wide[...].T
        cf = [columns[:, h : h + 1] for h in range(heads)]
        rb = [columns[:, heads + h : heads + h + 1] for h in range(heads)]
        cf_wide = jnp.where(first_head, cf[0], cf[1])
        rb_wide = jnp.where(first_head, rb[0], rb[1])
        ef[s] = jnp.exp2(cf_wide)
        eb[s] = jnp.exp2(rb_wide)
        kf[s] = jnp.exp2(cf_wide[length - 1 : length, :] - cf_wide)
        kb[s] = jnp.exp2(rb_wide[0:1, :] - rb_wide)
        row_at = lax.broadcasted_iota(jnp.int32, (length, length), 0)
        col_at = lax.broadcasted_iota(jnp.int32, (length, length), 1)
        for h in range(heads):
            spread = jnp.where(
                col_at <= row_at, cf[h] - sums[h : h + 1, :], rb[h] - sums[heads + h : heads + h + 1, :]
            )
            decay[s, h] = jnp.exp2(spread)
        turn = base_ref[s]
        cos_0, sin_0 = turn[0:1, :], turn[1:2, :]
        cos_i, sin_i = turn_ref[0], turn_ref[1]
        cosines[s] = cos_0 * cos_i - sin_0 * sin_i
        angle_sine = sin_0 * cos_i + cos_0 * sin_i
        sines[s] = jnp.where(leading, -angle_sine, angle_sine)

    def out_piece(r, d, which):
        start = pl.multiple_of((source_plane(r) * group + flipped(place, d)) * out_cols, 128)
        return wo.at[core, pl.ds(which * side_rows, side_rows), pl.ds(start, out_cols)]

    def out_move(r, which, d_there, hop):
        block = out_piece(r, d_there - hop, which)
        return remote(
            block, block, wo_send.at[0], out_sem(r, which, d_there),
            (chips[hop], core),
        )

    def out_sem(r, which, d):
        first = (which, d) == (0, 1)
        return wo_recv.at[r, 0 if first else 1 if (which, d) == (1, 2) else 2]

    def out_landed(r, which, d):
        block = out_piece(r, d, which)
        remote(block, block, wo_send.at[0], out_sem(r, which, d), partner).wait_recv()

    def spread_out(r):
        for which, hop in ((0, 1), (1, 2), (1, 1), (0, 2)):
            out_move(r, which, hop, hop).start()

    def relay_out(r):
        out_landed(r, 0, 1)
        out_move(r, 0, 3, 2).start()
        out_landed(r, 1, 2)
        out_move(r, 1, 3, 1).start()

    def finish_out(r):
        pieces = 1 if r == 1 else 2
        block = wo.at[core, :, pl.ds(0, pieces * out_cols)]
        remote(block, block, wo_send.at[0], wo_recv.at[r, 2], partner).wait_recv()
        if r == 1:
            out_landed(r, 0, 1)
            out_landed(r, 1, 2)

    def part_at(r):
        return pl.ds(pl.multiple_of(source_plane(r) * part_cols, 128), part_cols)

    def out_block(r, d):
        start = pl.multiple_of((source_plane(r) * group + flipped(place, d)) * out_cols, 128)
        return pl.ds(start, out_cols)

    def mate_copy(cols, i):
        block = wo.at[core, :, cols]
        return remote(block, block, mate_send.at[0], mate_recv.at[i], partner)

    def mate_here(cols, i):
        block = wo.at[1 - core, :, cols]
        remote(block, block, mate_send.at[0], mate_recv.at[i], partner).wait_recv()

    def wait_half(d):
        block = x.at[
            span_rows(flipped(place, d)), pl.ds(pl.multiple_of((1 - core) * half, 128), half)
        ]
        remote(block, block, half_send.at[0], half_recv.at[d], partner).wait_recv()

    for d in range(group):
        arrive(CLASS_A, 1, middle, (d,))
        arrive(CLASS_A, 2, middle, (d,))
    arrive(CLASS_OUT, 1, middle)
    for d in range(1, group):
        near_block(CLASS_B, d).wait_recv()
    own_here(CLASS_B)

    @pl.when(ends)
    def _():
        for d in range(group):
            own_far(CLASS_B, d)

    tokens[(0, 1)].wait_recv()
    send_piece(0, 1, 2)
    tokens[(1, 2)].wait_recv()
    send_piece(1, 2, 1)
    spread_out(0)
    arrive(CLASS_OUT, 1, ends)
    spread_out(1)
    arrive(CLASS_A, 3, middle)
    arrive(CLASS_OUT, 2, middle)

    @pl.when(middle)
    def _():
        for d in range(group):
            own_far(CLASS_B, d)

    tokens[(1, 1)].wait_recv()
    send_half(1)
    tokens[(0, 2)].wait_recv()
    send_half(2)
    for r in range(1, planes):
        arrive(CLASS_A, r, ends)
    arrive(CLASS_OUT, 3, middle)
    arrive(CLASS_B, 1, middle)
    wait_half(0)

    same_head = (
        lax.div(lax.broadcasted_iota(jnp.int32, (ch, ch), 0), HEAD_DIM)
        == lax.div(lax.broadcasted_iota(jnp.int32, (ch, ch), 1), HEAD_DIM)
    )

    def one_span(s):
        rows = span_rows(s)
        held = jnp.dot(x[rows, :], w[:, 0:col_a], preferred_element_type=f32)
        cosine, sine = cosines[s], sines[s]

        def turned(value):
            value = value.astype(bf16).astype(f32)
            other = jnp.where(
                leading,
                pltpu.roll(value, ch - HEAD_DIM // 2, 1),
                pltpu.roll(value, HEAD_DIM // 2, 1),
            )
            return value * cosine + other * sine

        rk = (turned(held[:, 0:ch]) * HEAD_DIM ** (-0.5)).astype(bf16).astype(f32)
        rq = turned(held[:, ch : 2 * ch]).astype(bf16)
        value = held[:, 2 * ch : 3 * ch].astype(bf16)
        rq_buf[s] = rq
        v_buf[s] = value
        gate_buf[s] = held[:, 3 * ch : 4 * ch].astype(bf16)
        value_wide = value.astype(f32)
        found = None
        for h in range(heads):
            in_head = first_head if h == 0 else jnp.logical_not(first_head)
            key_head = jnp.where(in_head, rk, 0.0).astype(bf16)
            value_head = jnp.where(in_head, value_wide, 0.0).astype(bf16)
            scores = lax.dot_general(
                rq, key_head, (((1,), (1,)), ((), ())), preferred_element_type=f32
            )
            probs = (scores * decay[s, h]).astype(bf16)
            part = jnp.dot(probs, value_head, preferred_element_type=f32)
            found = part if found is None else found + part
        loc[s] = found
        for table, target in ((kf, state_f), (kb, state_b)):
            keys = (rk * table[s]).astype(bf16)
            state = lax.dot_general(
                keys, value, (((0,), (0,)), ((), ())), preferred_element_type=f32
            )
            target[s] = jnp.where(same_head, state, 0.0)

    halo_rows = 16
    halo_at = (all_rows, all_rows + halo_rows)

    def halo_move(way):
        cols = pl.ds(own_half, half)
        source = x.at[pl.ds((all_rows - halo_rows) * (1 - way), halo_rows), cols]
        return remote(
            source, x.at[pl.ds(halo_at[way], halo_rows), cols],
            halo_send.at[way], halo_recv.at[way], (own + group if way == 0 else own - group, core),
        )

    def halo_pass(way):
        block = x.at[pl.ds(halo_at[way], halo_rows), pl.ds(own_half, half)]
        return remote(block, block, halo_send.at[2 + way], halo_recv.at[2 + way], partner)

    def halo_comes(way):
        return has_down if way == 0 else has_up

    blank = jnp.zeros((halo_rows, width), bf16)

    @pl.when(jnp.logical_not(has_down))
    def _():
        x[pl.ds(all_rows, halo_rows), :] = blank

    @pl.when(jnp.logical_not(has_up))
    def _():
        x[pl.ds(all_rows + halo_rows, halo_rows), :] = blank

    @pl.loop(0, group)
    def _(d):
        @pl.when(d == 1)
        def _():
            last = x.at[
                span_rows(flipped(place, 3)), pl.ds(pl.multiple_of(core * half, 128), half)
            ]
            remote(last, last, tok_send.at[0], token_landed(0, 3), partner).wait_recv()
            send_half(3)
            wait_half(1)

        @pl.when(d == 2)
        def _():
            wait_half(2)

        @pl.when(d == 3)
        def _():
            wait_half(3)
            pl.when(has_up)(lambda: halo_move(0).start())
            pl.when(has_down)(lambda: halo_move(1).start())
            relay_out(0)
            arrive(CLASS_OUT, 2, ends)
            spread_out(2)

        one_span(place_at(d))

    def scan_states(state, table, at, order, target):
        passed, inside, reach = jnp.zeros((ch, ch), f32), {}, {}
        over = jnp.ones((1, ch), f32)
        for s in order:
            inside[s], reach[s] = passed, over
            factor = table[s, at : at + 1, :]
            passed = factor * passed + state[s]
            over = over * factor
        folded = passed[0:HEAD_DIM, :]
        for h in range(1, heads):
            folded = folded + passed[h * HEAD_DIM : (h + 1) * HEAD_DIM, :]
        high = over.astype(bf16).astype(f32)
        coefficient = jnp.where(
            lax.broadcasted_iota(jnp.int32, (16, ch), 0) < 8, high, over - high
        )
        pack_out[target] = jnp.concatenate([folded, coefficient], axis=0).astype(bf16)
        return inside, reach

    ahead_in, ahead_reach = scan_states(state_f, ef, length - 1, range(group), 0)
    back_in, back_reach = scan_states(state_b, eb, 0, range(group)[::-1], 1)

    def pack_move(way, k):
        to = own + k * group if way == 0 else own - k * group
        return remote(
            pack_out.at[way], pack_in.at[way, k - 1],
            pack_send.at[way, k - 1], pack_recv.at[way, k - 1], (to, core),
        )

    def gives(way, k):
        return plane + k < planes if way == 0 else plane - k >= 0

    def takes(way, k):
        return gives(1 - way, k)

    for k in range(1, planes):
        for way in range(2):
            pl.when(gives(way, k))(lambda way=way, k=k: pack_move(way, k).start())
    arrive(CLASS_B, 2, middle)
    arrive(CLASS_B, 3, middle)

    def feature_cols(kind):
        return pl.ds(pl.multiple_of(kind * side_rows + place * ch, 128), ch)

    my_rows = length // 2

    def row_half(c):
        return pl.ds(pl.multiple_of(c * my_rows, 128), my_rows)

    def feature_move(kind, d, s, c):
        sender = ft_send.at[0]
        return remote(
            parts.at[kind, s, row_half(c)], feat.at[core, :, feature_cols(kind)],
            sender, ft_recv.at[kind, d], (base + s, c),
        )

    def feature_mate(kind):
        return remote(
            parts.at[kind, place, row_half(1 - core)], feat.at[core, :, feature_cols(kind)],
            ft_send.at[1], ft_recv.at[kind, 0], partner,
        )

    def own_features(kind):
        feature_mate(kind).start()
        feat[core, :, feature_cols(kind)] = parts[kind, place, row_half(core), :]

    finish_out(0)

    def pair_block(q):
        start = pl.multiple_of((q * group + flipped(place, 3)) * out_cols, 128)
        block = wo.at[core, :, pl.ds(start, out_cols)]
        return remote(
            block, block, pair_sem.at[0], pair_sem.at[1],
            ((plane + 1 - 2 * lax.rem(plane, 2)) * group + place, core),
        )

    pair_block(plane).start()
    mate_copy(part_at(0), 0).start()
    arrive(CLASS_OUT, 3, ends)
    spread_out(3)
    mate_copy(out_block(3, 0), 4).start()
    incoming = []
    for way in range(2):
        into[way] = jnp.zeros((HEAD_DIM, ch), f32)
        into[way + 2] = jnp.ones((HEAD_DIM, ch), f32)
        for k in range(1, planes):
            @pl.when(takes(way, k))
            def _(way=way, k=k):
                pack_move(way, k).wait_recv()
                pack = pack_in[way, k - 1].astype(f32)
                into[way] = into[way] + into[way + 2] * pack[0:HEAD_DIM, :]
                into[way + 2] = into[way + 2] * (
                    pack[HEAD_DIM : HEAD_DIM + 1, :] + pack[HEAD_DIM + 8 : HEAD_DIM + 9, :]
                )
        incoming.append(
            jnp.where(same_head, jnp.concatenate([into[way]] * heads, axis=0), 0.0)
        )
    for s in range(group):
        state_f[s] = ahead_in[s] + ahead_reach[s] * incoming[0]
        state_b[s] = back_in[s] + back_reach[s] * incoming[1]

    @pl.loop(0, group)
    def _(i):
        d = group - 1 - i
        s = place_at(d)
        query = rq_buf[s]
        mix = (
            loc[s]
            + ef[s] * jnp.dot(query, state_f[s].astype(bf16), preferred_element_type=f32)
            + eb[s] * jnp.dot(query, state_b[s].astype(bf16), preferred_element_type=f32)
        )
        squares = mix * mix
        first = jnp.sum(jnp.where(first_head, squares, 0.0), axis=-1, keepdims=True)
        second = jnp.sum(jnp.where(first_head, 0.0, squares), axis=-1, keepdims=True)
        scale = lax.rsqrt(jnp.where(first_head, first, second) / HEAD_DIM + EPS)
        gate = gate_buf[s].astype(f32)
        parts[1, s] = (
            gate / (1.0 + jnp.exp(-gate)) * (mix * scale * head_gain_ref[:, place_cols])
        ).astype(bf16)

        @pl.when(d > 0)
        def _():
            for c in range(2):
                feature_move(1, d, s, c).start()

    own_features(1)

    for way in range(2):
        @pl.when(halo_comes(way))
        def _(way=way):
            halo_move(way).wait_recv()
            halo_pass(way).start()
    relay_out(2)
    arrive(CLASS_B, 1, ends)
    arrive(CLASS_B, 2, ends)
    for way in range(2):
        pl.when(halo_comes(way))(lambda way=way: halo_pass(way).wait_recv())
    depth = group * rows_in
    most = (planes - 1) * depth
    early = pl.multiple_of(top * depth, 128)
    late = pl.multiple_of((1 - top) * most, 128)
    blocks = 5
    block = (all_rows + 2 * halo_rows) // blocks

    @pl.loop(0, blocks)
    def _(t):
        rows = pl.ds(pl.multiple_of(t * block, 16), block)
        acc[rows, :] = jnp.dot(
            x[rows, pl.ds(early, most)], w[pl.ds(early, most), col_a : col_a + col_b],
            preferred_element_type=f32,
        )

    relay_out(3)
    finish_out(1)
    for d in range(group - 1):
        mate_copy(out_block(1, d), 1).start()

    def hand_over(r):
        finish_out(r)
        mate_copy(part_at(r), r + 1).start()

    arrive(CLASS_B, 3, ends)

    spans_at = [s * length - halo_rows for s in range(1, group)] + [all_rows]
    late_w = w[pl.ds(late, depth), col_a : col_a + col_b]
    near_rows = jnp.concatenate(
        [x[at : at + 2 * halo_rows, pl.ds(late, depth)] for at in spans_at], axis=0
    )
    near_sums = jnp.concatenate(
        [acc[at : at + 2 * halo_rows, 0 : 2 * ch] for at in spans_at], axis=0
    )

    def inner_product(held):
        held = held.astype(bf16).astype(f32)
        return (held[:, 0:ch] * held[:, ch : 2 * ch]).astype(bf16).astype(f32)

    edge_values = inner_product(
        near_sums + jnp.dot(near_rows, late_w[:, 0 : 2 * ch], preferred_element_type=f32)
    )
    for s in range(group):
        before = ((s - 1) % group) * 2 * halo_rows + halo_rows - 1
        after = s * 2 * halo_rows + halo_rows
        edges[s, 0:1, :] = edge_values[before : before + 1, :]
        edges[s, 1:2, :] = edge_values[after : after + 1, :]
    row_of = lax.broadcasted_iota(jnp.int32, (length, ch), 0)

    @pl.loop(0, group)
    def _(i):
        d = 3 - 2 * i + 3 * lax.div(i, 2)
        s = place_at(d)
        rows = span_rows(s)
        held = acc[rows, :] + jnp.dot(
            x[rows, pl.ds(late, depth)], w[pl.ds(late, depth), col_a : col_a + col_b],
            preferred_element_type=f32,
        )
        inner = inner_product(held)
        before = jnp.where(row_of == 0, edges[s, 0:1, :], pltpu.roll(inner, 1, 0))
        after = jnp.where(row_of == length - 1, edges[s, 1:2, :], pltpu.roll(inner, length - 1, 0))
        near_sum = (
            taps_ref[0:1, place_cols] * before
            + taps_ref[1:2, place_cols] * inner
            + taps_ref[2:3, place_cols] * after
        )
        parts[0, s] = (held[:, 2 * ch : 3 * ch].astype(bf16).astype(f32) * near_sum).astype(bf16)

        @pl.when(d > 0)
        def _():
            for c in range(2):
                feature_move(0, d, s, c).start()

        pl.when(jnp.logical_and(i == 1, ends))(lambda: hand_over(2))

    own_features(0)

    def features_here(kind, places):
        for d in places:
            rows = my_rows if d == 0 else length
            block = parts.at[0, 0, pl.ds(0, rows)]
            remote(block, block, ft_send.at[0], ft_recv.at[kind, d], partner).wait_recv()

    def product(rows, r):
        total = None
        for c in range(2):
            part = jnp.dot(feat[c, :, rows], wo[c, rows, part_at(r)], preferred_element_type=f32)
            total = part if total is None else total + part
        return total

    def retention_product(r):
        decay[r, 0, 0:my_rows, :] = product(pl.ds(side_rows, side_rows), r)

    features_here(1, range(group))
    mate_here(part_at(0), 0)
    retention_product(0)
    pl.when(middle)(lambda: hand_over(2))
    finish_out(3)
    for d in range(1, group):
        mate_copy(out_block(3, d), 4).start()
    mate_here(part_at(2), 3)
    retention_product(2)
    pair_block(source_plane(1)).wait_recv()
    mate_copy(out_block(1, 3), 2).start()
    mate_here(part_at(3), 4)
    retention_product(3)
    mate_here(pl.ds(0, (group - 1) * out_cols), 1)
    mate_here(out_block(1, 3), 2)
    retention_product(1)

    for copy in rate_moves:
        copy.wait_send()
    ssq_move.wait_send()

    def sent(block, semaphore, landed):
        remote(block, block, semaphore, landed, partner).wait_send()

    sent(
        x.at[pl.ds(0, (group - 1) * length), pl.ds(0, 2 * quarter)], tok_send.at[0],
        tok_recv.at[0],
    )
    sent(x.at[pl.ds(0, all_rows), pl.ds(0, half)], half_send.at[0], half_recv.at[0])
    sent(
        wo.at[core, :, pl.ds(0, ((group - 1) * planes - 1) * out_cols)], wo_send.at[0],
        wo_recv.at[0, 0],
    )
    pair_block(plane).wait_send()
    sent(
        w.at[pl.ds(0, (group - 1) * rows_in), :], near_send.at[0], near_recv.at[0, 0]
    )
    sent(wo.at[core], mate_send.at[0], mate_recv.at[0])
    pl.when(has_up)(lambda: halo_move(0).wait_send())
    pl.when(has_down)(lambda: halo_move(1).wait_send())
    for way in range(2):
        pl.when(halo_comes(way))(lambda way=way: halo_pass(way).wait_send())
    for k in range(1, planes):
        for way in range(2):
            pl.when(gives(way, k))(lambda way=way, k=k: pack_move(way, k).wait_send())
    for kind in range(3):
        for units in range(1, planes):
            pl.when(plane == units - 1)(functools.partial(far_sent, kind, 0, units))
            pl.when(plane == planes - units)(functools.partial(far_sent, kind, 1, units))

    features_here(0, (0, 1, 2, 3))
    for r in range(planes):
        out_ref[:, part_at(r)] = (
            decay[r, 0, 0:my_rows, :] + product(pl.ds(0, side_rows), r)
        ).astype(bf16)
    sent(parts.at[:, pl.ds(0, group - 1)], ft_send.at[0], ft_recv.at[0, 0])
    sent(parts.at[:, 0, pl.ds(0, my_rows)], ft_send.at[1], ft_recv.at[0, 0])


def turn_tables(spans, length, channels):
    half_dim = HEAD_DIM // 2
    frequency = THETA ** (-2.0 * (np.arange(channels) % half_dim) / HEAD_DIM)
    inner = np.arange(length)[:, None] * frequency
    outer = (np.arange(spans) * length)[:, None] * frequency
    turn = np.stack([np.cos(inner), np.sin(inner)])
    start = np.zeros((spans, 8, channels))
    start[:, 0], start[:, 1] = np.cos(outer), np.sin(outer)
    return turn.astype(np.float32), start.astype(np.float32)


def mixer(planes, group, arrays):
    (
        tokens, norm_gain, outer_gate, inner_gate, conv_input, query_proj, key_proj, value_proj,
        out_gate, conv_taps, log_decay, head_gain, conv_output, retention_output,
    ) = arrays
    f32, bf16 = jnp.float32, jnp.bfloat16
    length, half = tokens.shape
    width = 2 * half
    ch = outer_gate.shape[1] // group
    heads = ch // HEAD_DIM
    rows, side = group * length, conv_output.shape[0]
    turn, start = turn_tables(planes * group, length, ch)
    dma = pltpu.SemaphoreType.DMA
    vmem, held = pl.BlockSpec(memory_space=pltpu.VMEM), pl.BlockSpec(memory_space=pltpu.HBM)
    v = pltpu.VMEM
    result = jax.ShapeDtypeStruct((length // 2, width), bf16)
    table = v((group, length, ch), f32)
    return pl.pallas_call(
        functools.partial(mixer_kernel, planes, group),
        out_shape=result,
        in_specs=[held] * 16,
        out_specs=vmem,
        scratch_shapes=[
            v((1, width), f32), v(conv_taps.shape, f32), v((1, head_gain.shape[0]), f32), v(turn.shape, f32),
            v((group,) + start.shape[1:], f32),
            v((length, half), bf16), v((rows + 32, width), bf16), v((width, 7 * ch), bf16),
            v((2, 2 * side, width), bf16), v(log_decay.shape, f32),
            v((group, 4 * heads, length // 2), f32), v((group, 4 * heads, length // 2), f32),
            v((8 * group, length), f32), v((128, length), f32),
            v((length, 128), f32), v((length, 128), f32),
            table, table, v((group, heads, length, length), f32),
            table, table, table, table,
            v((group, length, ch), bf16), v((group, length, ch), bf16), v((group, length, ch), bf16),
            table, v((group, ch, ch), f32), v((group, ch, ch), f32),
            v((2, HEAD_DIM + 16, ch), bf16), v((2, planes - 1, HEAD_DIM + 16, ch), bf16),
            v((4, HEAD_DIM, ch), f32),
            v((rows + 32, 3 * ch), f32), v((group, 8, ch), f32),
            v((2, group, length, ch), bf16), v((2, length // 2, 2 * side), bf16),
            dma((10,)), dma((1,)), dma((2, group - 1)), dma((1,)), dma((group - 1,)), dma((2,)),
            dma((1,)), dma((5,)), dma((1,)), dma((group,)),
            dma((3, 2)), dma((2, planes - 1, group)), dma((planes - 1,)),
            dma((1,)), dma((planes, 3)), dma((1,)), dma((5,)), dma((2,)), dma((4,)), dma((4,)),
            dma((2, planes - 1)), dma((2, planes - 1)), dma((2,)), dma((2, group)),
        ],
        compiler_params=pltpu.CompilerParams(
            collective_id=0, has_side_effects=True, vmem_limit_bytes=50 * 2**20
        ),
    )(
        *(
            pltpu.with_memory_space_constraint(source, pltpu.HBM)
            for source in (
                tokens, key_proj, query_proj, value_proj, out_gate, inner_gate, conv_input,
                outer_gate, conv_output, retention_output, log_decay, norm_gain.reshape(1, -1),
                conv_taps, head_gain.reshape(1, -1), jnp.asarray(turn), jnp.asarray(start),
            )
        )
    )


LANES = 128

def plan(*arrays):
    spans, cores = lax.axis_size("sp"), lax.axis_size("tp")
    group = arrays[2].shape[1] // LANES
    planes = spans // group
    fits = (
        cores == 2
        and group == 4
        and planes * group == spans
        and planes == 2 * cores
        and arrays[0].shape[1] == 2 * group * arrays[2].shape[0]
    )
    return mixer(planes, group, arrays) if fits else local(*arrays)


def solution(mesh):
    return jax.shard_map(
        plan,
        mesh=mesh,
        in_specs=(
            P("sp", "tp"),
            P(),
            P("sp", "tp"),
            P("sp", "tp"),
            P("sp", "tp"),
            P("sp", "tp"),
            P("sp", "tp"),
            P("sp", "tp"),
            P("sp", "tp"),
            P(None, "tp"),
            P(None, "tp", "sp"),
            P("tp"),
            P("tp", "sp"),
            P("tp", "sp"),
        ),
        out_specs=P(("sp", "tp"), None),
        check_vma=False,
    )
```
